512 devices in a mesh: ep: 32 (over z, core), tp: 16 (over y, x).
Axes of the slice: x: 4, y: 4, z: 16, core: 2. Of those that a mesh axis runs over, the one named last changes fastest.
Arguments:
- query_rows: bfloat16 [16384, 2048], P('ep', 'tp'), may hold values from -6 to 6
- key_rows: bfloat16 [16384, 2048], P('ep', 'tp'), may hold values from -6 to 6
- value_rows: bfloat16 [16384, 4096], P('ep', 'tp'), may hold values from -6 to 6
- in_gate: float32 [16, 16384], P('tp', 'ep'), may hold values from -120 to 120
- forget_gate: float32 [16, 16384], P('tp', 'ep'), may hold values from -2 to 20
- out_gate: bfloat16 [16384, 4096], P('ep', 'tp'), may hold values from -6 to 6
- head_gain: float32 [4096], P('tp'), may hold values from 0.1 to 1.9
- mix_weight: bfloat16 [4096, 4096], P(None, 'tp'), may hold values from -0.09375 to 0.09375
- expert_input: bfloat16 [8192, 4096], P('ep', 'tp'), may hold values from -30 to 30
- routes: int32 [8192, 2], P('ep'), may hold values from 0 to 31, all different within a row; in each aligned block of 256 rows (0 to 255, 256 to 511, ...) at most 32 rows name the same one
- route_weight: float32 [8192, 2], P('ep'), may hold values from 0.25 to 1.25
- gate_weight: bfloat16 [32, 1024, 4096], P('ep', 'tp'), may hold values from -0.09375 to 0.09375
- up_weight: bfloat16 [32, 1024, 4096], P('ep', 'tp'), may hold values from -0.09375 to 0.09375
- down_weight: bfloat16 [32, 1024, 4096], P('ep', None, 'tp'), may hold values from -0.1875 to 0.1875
Outputs:
- mixer_out: bfloat16 [16384, 4096], P('ep', 'tp')
- expert_out: bfloat16 [8192, 4096], P('ep', 'tp')
The draws below stay inside these ranges and needn't reach their ends.
Inputs may be any that keep to these rules, and one draw needn't show every extreme that they name: `routes`: each row names 2 different experts. In the rows of one device no expert is named by more than 32 rows, and in the rows of some device an expert is named by exactly 32 rows.
All inputs are finite; a program needn't handle non-finite values.
Results may differ from the reference program's by a relative error of at most 0.0057.
Values may be sent and summed in bfloat16 or wider, within the bound.
No kernel may reach another device: no remote copies, remote signals or barrier semaphores. Data moves between devices by JAX's collectives and lax.ppermute only.
A program may use at most 128 MiB of HBM per device.

```python
import math
import jax
import jax.numpy as jnp
import numpy as np
from jax import lax

D = 4096
HEADS = 16
QK = 128
FF = 1024
TOP = 2
BLOCK = 64
ROWS_A = 512
ROWS_B = 256
TOKENS_A = 16384
TOKENS_B = 8192
EXPERTS = 32
CAP = 32
N_EP = 32


def draw_in_gate(key, part):
    base = jnp.clip(jax.random.normal(jax.random.fold_in(key, 11), (HEADS, TOKENS_A), jnp.float32), -4.0, 4.0)
    return base


def draw_forget_gate(key, part):
    slow_share = 0.5
    slow_heads = jax.random.bernoulli(jax.random.fold_in(key, 21), slow_share, (HEADS, 1))
    level = jnp.where(slow_heads, math.log(TOKENS_A) + 0.5, 3.5)
    span_total = TOKENS_A // ROWS_A
    drift = jax.random.uniform(jax.random.fold_in(key, 22), (HEADS, span_total), jnp.float32, -1.0, 1.0)
    noise = 0.7 * jnp.clip(jax.random.normal(jax.random.fold_in(key, 23), (HEADS, TOKENS_A), jnp.float32), -4.0, 4.0)
    return level + jnp.repeat(drift, ROWS_A, axis=1) + noise


def draw_expert_input(key, part):
    row_scale = jnp.exp(jax.random.uniform(jax.random.fold_in(key, 31), (TOKENS_B, 1), jnp.float32, -0.7, 0.7))
    base = jnp.clip(jax.random.normal(jax.random.fold_in(key, 34), (TOKENS_B, D), jnp.float32), -4.0, 4.0)
    return (base * row_scale).astype(jnp.bfloat16)


def steps_of(rng, extent, split, low, high):
    loudness, own = 1.0, jax.random.fold_in(rng, 6)
    for axis_at, shards_of in split:
        steps = jnp.exp(jax.random.uniform(jax.random.fold_in(own, axis_at), (shards_of,), jnp.float32, low / len(split), high / len(split)))
        loudness = loudness * jnp.repeat(steps, extent[axis_at] // shards_of).reshape([-1 if axis == axis_at else 1 for axis in range(len(extent))])
    return loudness


def deal_out(key, own, number, rows, count, top, bound, slope):
    order = jax.random.permutation(key, count)
    packed, usual = load_shares(count, rows * top, bound, slope, True), load_shares(count, rows * top, bound, slope, False)
    places = jnp.arange(count)

    def named(tallies, offset_by):
        used = int((tallies > 0).sum())
        fixed = max(1, used // 4)
        shifted = fixed + (places - fixed + offset_by * (used - fixed)) % max(1, count - fixed)
        return jnp.zeros((count,), jnp.int32).at[order[jnp.where(places < fixed, places, shifted)]].set(jnp.asarray(tallies, jnp.int32))

    tallies = jnp.where(number % 4 == 0, named(packed, number // 4), named(usual, number - number // 4 - 1))
    mixed = jax.random.permutation(jax.random.fold_in(own, 3), count)
    donor, taker = mixed[0:count // 2 * 2:2], mixed[1:count // 2 * 2:2]
    room = jnp.minimum(tallies[donor] - 1, bound - tallies[taker]) // 2
    room = jnp.where((donor == order[0]) | (taker == order[0]) | (tallies[taker] == 0), 0, jnp.maximum(room, 0))
    shifted = jax.random.randint(jax.random.fold_in(own, 4), (count // 2,), 0, 1 << 20) % (room + 1)
    tallies = tallies.at[donor].add(-shifted).at[taker].add(shifted)
    labels = jnp.searchsorted(jnp.cumsum(tallies), jnp.arange(rows * top), side="right").astype(jnp.int32)
    listing = labels.reshape(top, rows).T
    listing = listing[jax.random.permutation(jax.random.fold_in(own, 1), rows)]
    offset_by = jax.random.randint(jax.random.fold_in(own, 2), (rows, 1), 0, top)
    return jnp.take_along_axis(listing, (jnp.arange(top)[None, :] + offset_by) % top, axis=1)


def load_shares(amount, total, bound, lean, full):
    weights = [(1 << 20) // math.isqrt(grade ** lean) + 1 for grade in range(1, amount + 1)]
    largest = bound if full else min(bound, max(-(-total // amount), total * weights[0] // sum(weights)))
    least = 1 if total - largest >= amount - 1 else 0
    given, rest = [largest] + [least] * (amount - 1), total - largest - least * (amount - 1)
    while rest > 0:
        free = [i for i in range(1, amount) if given[i] < largest] or [i for i in range(1, amount) if given[i] < bound]
        mass, remaining = sum([weights[i] for i in free]), rest
        for i in free:
            extra = min(bound - given[i], max(1, remaining * weights[i] // mass), rest)
            given[i] = given[i] + extra
            rest = rest - extra
    return np.array(given)


def centred(key, dims, scale, bound, cuts=(), kind=jnp.bfloat16):
    level = steps_of(key, dims, cuts, -0.22, 0.18) if cuts else 1.0
    entries = jax.random.normal(key, dims, jnp.float32) * scale * level
    return jnp.minimum(jnp.maximum(entries, -bound), bound).astype(kind)


def setup_inputs(seed: int = 0) -> dict:
    key_of = jax.random.split(jax.random.key(seed), 15)
    query_rows = centred(key_of[0], (TOKENS_A, HEADS * QK), 1.0, 6.0, ((0, 32), (1, 16)))
    key_rows = centred(key_of[1], (TOKENS_A, HEADS * QK), 1.0, 6.0, ((0, 32), (1, 16)))
    value_rows = centred(key_of[2], (TOKENS_A, D), 1.0, 6.0, ((0, 32), (1, 16)))
    in_gate = draw_in_gate(jax.random.fold_in(key_of[14], 71), 0)
    forget_gate = draw_forget_gate(jax.random.fold_in(key_of[14], 71), 0)
    out_gate = centred(key_of[5], (TOKENS_A, D), 1.0, 6.0, ((0, 32), (1, 16)))
    head_gain = jnp.clip(1.0 + 0.18 * jax.random.normal(key_of[6], (D,), jnp.float32), 0.1, 1.9)
    mix_weight = centred(key_of[7], (D, D), D ** -0.5, 0.09375, ((1, 16),))
    expert_input = draw_expert_input(jax.random.fold_in(key_of[14], 71), 0)
    routes_keys = jax.random.split(jax.random.fold_in(key_of[9], 1), TOKENS_B // ROWS_B)
    routes_turns = jax.random.permutation(jax.random.fold_in(key_of[9], 3), TOKENS_B // ROWS_B)
    routes = jax.vmap(lambda own, number: deal_out(jax.random.fold_in(key_of[9], 2), own, number, ROWS_B, EXPERTS, TOP, CAP, 1))(routes_keys, routes_turns).reshape((TOKENS_B, TOP))
    route_weight = jnp.clip(0.25 + 1.0 * jax.random.uniform(key_of[10], (TOKENS_B, TOP), jnp.float32) ** steps_of(key_of[10], (TOKENS_B, TOP), ((0, 32),), -0.2, 0.2), 0.25, 1.25)
    gate_weight = centred(key_of[11], (EXPERTS, FF, D), D ** -0.5, 0.09375, ((0, 32), (1, 16)))
    up_weight = centred(key_of[12], (EXPERTS, FF, D), D ** -0.5, 0.09375, ((0, 32), (1, 16)))
    down_weight = centred(key_of[13], (EXPERTS, FF, D), FF ** -0.5, 0.1875, ((0, 32), (2, 16)))
    return dict(query_rows=query_rows, key_rows=key_rows, value_rows=value_rows, in_gate=in_gate, forget_gate=forget_gate, out_gate=out_gate, head_gain=head_gain, mix_weight=mix_weight, expert_input=expert_input, routes=routes, route_weight=route_weight, gate_weight=gate_weight, up_weight=up_weight, down_weight=down_weight)


EPSILON = 1e-06
LOG_FLOOR = -1e+30
HIGHEST_PRECISION = lax.Precision.HIGHEST

def combine(first_part, second_part):
    decay_first, max_first, memory_first, normal_first = first_part
    decay_second, max_second, memory_second, normal_second = second_part
    running_max = jnp.maximum(decay_second + max_first, max_second)
    keep_first = jnp.exp(decay_second + max_first - running_max)
    keep_second = jnp.exp(max_second - running_max)
    memory = keep_first[..., None, None] * memory_first + keep_second[..., None, None] * memory_second
    normalizer = keep_first[..., None] * normal_first + keep_second[..., None] * normal_second
    return (decay_first + decay_second, running_max, memory, normalizer)

def identity_state(head_count, key_width, value_width):
    return (jnp.zeros((head_count,), jnp.float32), jnp.full((head_count,), LOG_FLOOR, jnp.float32), jnp.zeros((head_count, key_width, value_width), jnp.float32), jnp.zeros((head_count, key_width), jnp.float32))

def halfprod(form, left, right):
    return jnp.einsum(form, left.astype(jnp.float32), right.astype(jnp.float32), precision=HIGHEST_PRECISION)

def prepare(query_heads, key_heads, value_heads, in_gate, forget_gate):
    head_count, length, key_width = query_heads.shape
    block_count = length // BLOCK
    query_blocks = query_heads.reshape(head_count, block_count, BLOCK, key_width)
    key_blocks = key_heads.reshape(head_count, block_count, BLOCK, key_width)
    value_blocks = value_heads.reshape(head_count, block_count, BLOCK, value_heads.shape[-1])
    log_input = in_gate.reshape(head_count, block_count, BLOCK)
    cumulative = jnp.cumsum(jax.nn.log_sigmoid(forget_gate).reshape(head_count, block_count, BLOCK), axis=-1)
    block_decay = cumulative[..., -1]
    weight_log = block_decay[..., None] - cumulative + log_input
    block_max = lax.optimization_barrier(jnp.max(weight_log, axis=-1))
    weighted = key_blocks.astype(jnp.float32) * jnp.exp(weight_log - block_max[..., None])[..., None]
    normalizer = lax.optimization_barrier(jnp.sum(weighted, axis=2))
    memory = halfprod('hcsk,hcsv->hckv', weighted.astype(jnp.bfloat16), value_blocks)
    return ((query_blocks, key_blocks, value_blocks, log_input, cumulative), (block_decay, block_max, memory, normalizer))

def prefix(summary, initial):
    leading = jax.tree.map(lambda tensor: jnp.moveaxis(tensor, 1, 0), summary)

    def advance(running, current):
        return (combine(running, current), running)
    final_state, before = lax.scan(advance, initial, leading)
    return (final_state, jax.tree.map(lambda tensor: jnp.moveaxis(tensor, 0, 1), before))

def block_outputs(blocked, before):
    query_blocks, key_blocks, value_blocks, log_input, cumulative = blocked
    prior_max, prior_memory, prior_normal = (before[1], before[2], before[3])
    block_len = cumulative.shape[-1]
    scale = query_blocks.shape[-1] ** (-0.5)
    causal = jnp.tril(jnp.ones((block_len, block_len), dtype=bool))
    log_decay = jnp.where(causal, cumulative[..., :, None] - cumulative[..., None, :] + log_input[..., None, :], -jnp.inf)
    log_inter = cumulative + prior_max[..., None]
    top_value = jnp.maximum(log_inter, lax.optimization_barrier(jnp.max(log_decay, axis=-1)))
    scores = halfprod('hctk,hcsk->hcts', query_blocks, key_blocks) * scale * jnp.exp(log_decay - top_value[..., None])
    carried = jnp.exp(log_inter - top_value) * scale
    query_wide = query_blocks.astype(jnp.float32)
    numerator = carried[..., None] * jnp.einsum('hctk,hckv->hctv', query_wide, prior_memory, precision=HIGHEST_PRECISION) + halfprod('hcts,hcsv->hctv', scores.astype(jnp.bfloat16), value_blocks)
    denominator = carried * jnp.einsum('hctk,hck->hct', query_wide, prior_normal, precision=HIGHEST_PRECISION) + lax.optimization_barrier(jnp.sum(scores, axis=-1))
    return numerator / jnp.maximum(jnp.abs(denominator), jnp.exp(-top_value))[..., None]

def finish(head_values, out_gate, head_gain):
    head_count, block_count, block_len, value_width = head_values.shape
    per_head = jnp.transpose(head_values, (1, 2, 0, 3)).reshape(block_count * block_len, head_count, value_width)
    per_head = per_head * lax.rsqrt(lax.optimization_barrier(jnp.mean(per_head * per_head, axis=-1, keepdims=True)) + EPSILON)
    per_head = per_head.reshape(block_count * block_len, head_count * value_width) * head_gain
    per_head = per_head * jax.nn.sigmoid(out_gate.astype(jnp.float32))
    return per_head.astype(jnp.bfloat16)

def reference(query_rows, key_rows, value_rows, in_gate, forget_gate, out_gate, head_gain, mix_weight, expert_input, routes, route_weight, gate_weight, up_weight, down_weight):
    length = query_rows.shape[0]
    head_count = in_gate.shape[0]
    key_width = query_rows.shape[1] // head_count
    value_width = value_rows.shape[1] // head_count
    query_heads = query_rows.reshape(length, head_count, key_width).transpose(1, 0, 2)
    key_heads = key_rows.reshape(length, head_count, key_width).transpose(1, 0, 2)
    value_heads = value_rows.reshape(length, head_count, value_width).transpose(1, 0, 2)

    def one_head(current):
        query_one, key_one, value_one, input_one, forget_one = current
        blocked, summary = prepare(query_one[None], key_one[None], value_one[None], input_one[None], forget_one[None])
        final_state, before = prefix(summary, identity_state(1, key_width, value_width))
        return block_outputs(blocked, before)[0]
    head_values = lax.map(one_head, (query_heads, key_heads, value_heads, in_gate, forget_gate))
    mixed_heads = finish(head_values, out_gate, head_gain)
    mixer_out = jnp.dot(mixed_heads, mix_weight, preferred_element_type=jnp.float32).astype(jnp.bfloat16)
    squares = lax.optimization_barrier(jnp.sum(jnp.square(expert_input.astype(jnp.float32)), axis=-1))
    inverse_rms = lax.rsqrt(squares / D + EPSILON)
    slot_total = N_EP * CAP

    def one_expert(running, expert):
        matched = routes == expert
        picked = jnp.any(matched, axis=1)
        row_index = jnp.nonzero(picked, size=slot_total, fill_value=0)[0].astype(jnp.int32)
        count = jnp.sum(picked.astype(jnp.int32))
        is_valid = (jnp.arange(slot_total, dtype=jnp.int32) < count).astype(jnp.float32)
        weight = lax.optimization_barrier(jnp.sum(jnp.where(matched, route_weight, 0.0), axis=1))
        chosen = expert_input[row_index]
        row_scale = inverse_rms[row_index][:, None]
        gate_value = jnp.dot(chosen, gate_weight[expert].T, preferred_element_type=jnp.float32) * row_scale
        up_value = jnp.dot(chosen, up_weight[expert].T, preferred_element_type=jnp.float32) * row_scale
        hidden = (jax.nn.silu(gate_value) * up_value).astype(jnp.bfloat16)
        expert_rows = jnp.dot(hidden, down_weight[expert], preferred_element_type=jnp.float32).astype(jnp.bfloat16)
        term = expert_rows.astype(jnp.float32) * (weight[row_index] * is_valid)[:, None]
        return (running.at[row_index].add(term), None)
    total, _ = lax.scan(one_expert, jnp.zeros((TOKENS_B, D), jnp.float32), jnp.arange(EXPERTS, dtype=jnp.int32))
    return (mixer_out, total.astype(jnp.bfloat16))
```

```python
import jax
import jax.numpy as jnp
from jax import lax
from jax.experimental import pallas as pl
from jax.experimental.pallas import tpu as pltpu
from jax.sharding import Mesh
from jax.sharding import PartitionSpec as P

EP = ("z", "c")
TP = ("y", "x")
EPSILON = 1e-06
LOG_FLOOR = -1e30
MASKED = -1e38
HIGHEST = lax.Precision.HIGHEST
F32 = jnp.float32
BF16 = jnp.bfloat16


def dot(a, b):
    return jnp.dot(a, b, preferred_element_type=F32)


def dot_t(a, b):
    return lax.dot_general(a, b, (((1,), (1,)), ((), ())), preferred_element_type=F32)


def iota(shape, dim):
    return lax.broadcasted_iota(jnp.int32, shape, dim)


def call(kernel, out, name, args, scratch=(), grid=None, in_specs=None, out_specs=None):
    vmem = pl.BlockSpec(memory_space=pltpu.VMEM)
    smem = pl.BlockSpec(memory_space=pltpu.SMEM)
    if in_specs is None:
        in_specs = [smem if a.dtype == jnp.int32 and a.ndim == 1 else vmem for a in args]
    kw = {} if grid is None else {"grid": grid}
    if out_specs is None:
        out_specs = jax.tree.map(lambda _: vmem, out)
    return pl.pallas_call(
        kernel,
        out_shape=out,
        in_specs=in_specs,
        out_specs=out_specs,
        scratch_shapes=list(scratch),
        name=name,
        **kw,
    )(*args)


def log_sigmoid(f):
    return jnp.minimum(f, 0.0) - jnp.log1p(jnp.exp(-jnp.abs(f)))


def cumulative_forms(forget_row):
    n = forget_row.shape[1]
    logs = jnp.broadcast_to(log_sigmoid(forget_row), (n, n))
    at_row, at_col = iota((n, n), 0), iota((n, n), 1)
    column = jnp.sum(jnp.where(at_col <= at_row, logs, 0.0), axis=1, keepdims=True)
    own = jnp.sum(jnp.where(at_col == at_row, logs, 0.0), axis=1, keepdims=True)
    row = jnp.sum(jnp.where(at_row <= at_col, own, 0.0), axis=0, keepdims=True)
    return column, row


def summary_kernel(k_ref, v_ref, in_ref, forget_ref, out_ref):
    n = k_ref.shape[0]
    dk = k_ref.shape[1]
    column, _ = cumulative_forms(forget_ref[...])
    diagonal = iota((n, n), 0) == iota((n, n), 1)
    log_in = jnp.sum(
        jnp.where(diagonal, jnp.broadcast_to(in_ref[...], (n, n)), 0.0), axis=1, keepdims=True
    )
    total = column[n - 1 :, :]
    weight_log = total - column + log_in
    top = jnp.max(weight_log, axis=0, keepdims=True)
    weighted = k_ref[...].astype(F32) * jnp.exp(weight_log - top)
    memory = lax.dot_general(
        weighted.astype(BF16), v_ref[...], (((0,), (0,)), ((), ())), preferred_element_type=F32
    )
    normal = jnp.sum(weighted, axis=0, keepdims=True)
    width = out_ref.shape[1]
    out_ref[0:dk, :] = memory
    out_ref[dk : dk + 1, 0:dk] = normal
    out_ref[dk : dk + 1, dk:] = normal
    out_ref[dk + 1 : dk + 2, :] = jnp.broadcast_to(total, (1, width))
    out_ref[dk + 2 : dk + 3, :] = jnp.broadcast_to(top, (1, width))
    out_ref[dk + 3 :, :] = jnp.zeros((out_ref.shape[0] - dk - 3, width), F32)


def parts_of(x, dk):
    return x[0:dk, :], x[dk : dk + 1, :], x[dk + 1 : dk + 2, :], x[dk + 2 : dk + 3, :]


def fold(first, second):
    memory_1, normal_1, decay_1, max_1 = first
    memory_2, normal_2, decay_2, max_2 = second
    top = jnp.maximum(decay_2 + max_1, max_2)
    keep_1 = jnp.exp(decay_2 + max_1 - top)
    keep_2 = jnp.exp(max_2 - top)
    return (
        keep_1 * memory_1 + keep_2 * memory_2,
        keep_1 * normal_1 + keep_2 * normal_2,
        decay_1 + decay_2,
        top,
    )


def split3(x):
    high = x.astype(BF16)
    rest = x - high.astype(F32)
    middle = rest.astype(BF16)
    low = (rest - middle.astype(F32)).astype(BF16)
    return high, middle, low


def chip_kernel(at_ref, mine_ref, other_ref, out_ref):
    dk = 128
    south = at_ref[0] == 0
    mine, other = mine_ref[...], other_ref[...]
    first = parts_of(jnp.where(south, mine, other), dk)
    second = parts_of(jnp.where(south, other, mine), dk)
    memory, normal, decay, top = fold(first, second)
    half = memory.shape[1] // 2
    out_ref[0:dk, :] = jnp.where(south, memory[:, :half], memory[:, half:]).astype(BF16)
    rows = []
    for value in (normal, decay, top):
        rows += [part.astype(F32) for part in split3(value[:, :half])]
    rows.append(jnp.zeros((out_ref.shape[0] - dk - len(rows), half), F32))
    out_ref[dk:, :] = jnp.concatenate(rows, axis=0).astype(BF16)


def prior_kernel(at_ref, all_ref, out_ref):
    dk = 128
    here = at_ref[1]
    half = all_ref.shape[2]
    state = (
        jnp.zeros((dk, half), F32),
        jnp.zeros((1, half), F32),
        jnp.zeros((1, half), F32),
        jnp.full((1, half), LOG_FLOOR, F32),
    )
    for k in range(all_ref.shape[0]):
        item = all_ref[k].astype(F32)
        rows = [
            item[dk + i : dk + i + 1] + item[dk + i + 1 : dk + i + 2] + item[dk + i + 2 : dk + i + 3]
            for i in (0, 3, 6)
        ]
        joined = fold(state, (item[0:dk], *rows))
        state = tuple(jnp.where(k < here, new, old) for new, old in zip(joined, state))
    out_ref[0:dk, :] = state[0]
    out_ref[dk:, :] = jnp.concatenate(
        [state[1], state[2], state[3], jnp.zeros((out_ref.shape[0] - dk - 3, half), F32)], axis=0
    )


def output_kernel(
    at_ref, q_ref, k_ref, v_ref, in_ref, forget_ref, gate_ref, gain_ref,
    prior_ref, prior_other_ref, other_ref, out_ref,
):
    n, dk = q_ref.shape
    scale = dk ** (-0.5)
    south = at_ref[0] == 0
    column, row = cumulative_forms(forget_ref[...])
    left = jnp.where(south, prior_ref[...], prior_other_ref[...])
    right = jnp.where(south, prior_other_ref[...], prior_ref[...])
    before = parts_of(jnp.concatenate([left, right], axis=1), dk)
    joined = fold(before, parts_of(other_ref[...], dk))
    memory, normal, _, top_before = [jnp.where(south, b, j) for b, j in zip(before, joined)]
    normal = normal[:, :dk]
    top_before = top_before[:, 0:1]
    log_in = in_ref[...]
    step = min(n, 128)
    for start in range(0, n, step):
        rows, seen = slice(start, start + step), start + step
        q = q_ref[rows, :]
        at = column[rows, :]
        causal = iota((step, seen), 1) <= iota((step, seen), 0) + start
        log_decay = jnp.where(causal, at - row[:, :seen] + log_in[:, :seen], MASKED)
        log_inter = at + top_before
        top = jnp.maximum(log_inter, jnp.max(log_decay, axis=1, keepdims=True))
        scores = dot_t(q, k_ref[0:seen, :]) * scale * jnp.exp(log_decay - top)
        carried = jnp.exp(log_inter - top) * scale
        wide = q.astype(F32)
        numerator = carried * jnp.dot(
            wide, memory, precision=HIGHEST, preferred_element_type=F32
        ) + dot(scores.astype(BF16), v_ref[0:seen, :])
        denominator = carried * jnp.sum(wide * normal, axis=1, keepdims=True) + jnp.sum(
            scores, axis=1, keepdims=True
        )
        values = numerator / jnp.maximum(jnp.abs(denominator), jnp.exp(-top))
        values = values * lax.rsqrt(jnp.mean(values * values, axis=1, keepdims=True) + EPSILON)
        gate = gate_ref[rows, :].astype(F32)
        values = values * gain_ref[...] * (1.0 / (1.0 + jnp.exp(-gate)))
        mixed = values.astype(BF16)
        for copy in range(out_ref.shape[0]):
            out_ref[copy, rows, :] = mixed


def slot_tables(named, slots_shape, expert_dim, room):
    place = iota(slots_shape, expert_dim)
    return place // room, place % room


def dispatch_kernel(routes_ref, x_ref, out_ref):
    tokens = x_ref.shape[0]
    slots = out_ref.shape[0]
    experts, room = 32, slots // 32
    expert = iota((experts, tokens), 0)
    named = jnp.zeros((experts, tokens), F32)
    for r in range(routes_ref.shape[0]):
        named = named + (routes_ref[r : r + 1, :] == expert).astype(F32)
    earlier = (iota((tokens, tokens), 0) < iota((tokens, tokens), 1)).astype(F32).astype(BF16)
    place = dot(named.astype(BF16), earlier)
    key = jnp.where(named > 0.5, place, -1.0).astype(BF16)
    slot = iota((slots, experts), 0)
    spread = (slot // room == iota((slots, experts), 1)).astype(F32).astype(BF16)
    wanted = (iota((slots, tokens), 0) % room).astype(F32)
    chosen = (dot(spread, key) == wanted).astype(F32).astype(BF16)
    out_ref[...] = dot(chosen, x_ref[...]).astype(BF16)


def collect_kernel(routes_ref, weight_ref, back_ref, out_ref):
    tokens = out_ref.shape[0]
    slots = back_ref.shape[0]
    experts, room = 32, slots // 32
    expert = iota((tokens, experts), 1)
    named = jnp.zeros((tokens, experts), F32)
    weight = jnp.zeros((tokens, experts), F32)
    for r in range(routes_ref.shape[1]):
        hit = routes_ref[:, r : r + 1] == expert
        named = named + hit.astype(F32)
        weight = weight + jnp.where(hit, weight_ref[:, r : r + 1], 0.0)
    earlier = (iota((tokens, tokens), 1) < iota((tokens, tokens), 0)).astype(F32).astype(BF16)
    place = dot(earlier, named.astype(BF16))
    key = jnp.where(named > 0.5, place, -1.0).astype(BF16)
    slot = iota((experts, slots), 1)
    spread = (slot // room == iota((experts, slots), 0)).astype(F32).astype(BF16)
    wanted = (iota((tokens, slots), 1) % room).astype(F32)
    chosen = dot(key, spread) == wanted
    total = jnp.zeros(out_ref.shape, F32)
    for part in split3(weight):
        share = jnp.where(chosen, dot(part, spread), 0.0).astype(BF16)
        total = total + dot(share, back_ref[...])
    out_ref[...] = total.astype(BF16)


def hidden_kernel(
    x_ref, gate_ref, up_ref, w1_ref, w2_ref, w3_ref, out_ref, gate_acc, up_acc, squares
):
    step = pl.program_id(0)
    width = gate_ref.shape[0]

    @pl.when(step == 0)
    def _():
        gate_acc[...] = jnp.zeros_like(gate_acc)
        up_acc[...] = jnp.zeros_like(up_acc)
        squares[...] = jnp.zeros_like(squares)

    far = (w1_ref, w2_ref, w3_ref)
    columns = x_ref.shape[2]
    for i in range(x_ref.shape[0]):
        x = x_ref[i]
        cols = slice(i * columns, (i + 1) * columns)
        gate = jnp.concatenate([gate_ref[:, cols]] + [w[0:width, cols] for w in far], axis=0)
        up = jnp.concatenate([up_ref[:, cols]] + [w[width:, cols] for w in far], axis=0)
        gate_acc[...] += dot_t(x, gate)
        up_acc[...] += dot_t(x, up)
        wide = x.astype(F32)
        squares[...] += wide * wide

    @pl.when(step == pl.num_programs(0) - 1)
    def _():
        mean = jnp.sum(squares[...], axis=1, keepdims=True) * (1.0 / (columns * out_ref.shape[0]))
        inverse = lax.rsqrt(mean + EPSILON)
        gate = gate_acc[...] * inverse
        hidden = gate * (1.0 / (1.0 + jnp.exp(-gate))) * (up_acc[...] * inverse)
        hidden = hidden.astype(BF16)
        for copy in range(out_ref.shape[0]):
            out_ref[copy] = hidden


def down_kernel(h_ref, w_ref, out_ref):
    part = h_ref.shape[2] // 4
    rows = h_ref.shape[1]
    for ys in range(4):
        total = jnp.zeros((rows, w_ref.shape[1]), F32)
        for xs in range(4):
            at = [(((ys + j) % 4) * 4 + xs) * part for j in range(4)]
            weight = jnp.concatenate([w_ref[a : a + part, :] for a in at], axis=0)
            total = total + dot(h_ref[ys * 4 + xs], weight)
        out_ref[ys * rows : (ys + 1) * rows, :] = total.astype(BF16)


def mix_kernel(
    at_ref, h_ref, near_ref, a1_ref, a2_ref, a3_ref, b1_ref, b2_ref, b3_ref, out_ref, acc
):
    step = pl.program_id(0)
    half = h_ref.shape[0] // 2

    @pl.when(step == 0)
    def _():
        acc[...] = jnp.zeros_like(acc)

    c, x = at_ref[0], at_ref[2]
    mine = h_ref[c * half + step]
    theirs = h_ref[(1 - c) * half + step]
    acc[0] += dot(h_ref[step], near_ref[0, 0]) + dot(h_ref[half + step], near_ref[1, 0])
    for k, (a, b) in enumerate(((a1_ref, b1_ref), (a2_ref, b2_ref), (a3_ref, b3_ref))):
        acc[k + 1] += dot(mine, a[...]) + dot(theirs, b[...])

    @pl.when(step == half - 1)
    def _():
        for k in range(4):
            out_ref[lax.rem(x + k, 4)] = acc[k].astype(BF16)


def from_next(x, axis, k):
    n = lax.axis_size(axis)
    return lax.ppermute(x, axis, [((i + k) % n, i) for i in range(n)])


def exchange(x, axis):
    return lax.all_to_all(x, axis, split_axis=0, concat_axis=0, tiled=True)


def body(
    query_rows,
    key_rows,
    value_rows,
    in_gate,
    forget_gate,
    out_gate,
    head_gain,
    mix_weight,
    expert_input,
    routes,
    route_weight,
    gate_weight,
    up_weight,
    down_weight,
):
    sds = jax.ShapeDtypeStruct
    rows_a, dk = query_rows.shape
    dv = value_rows.shape[1]
    tokens, columns = expert_input.shape
    ep, tp = lax.axis_size(EP), lax.axis_size(TP)
    gate_local, up_local, down_local = gate_weight[0], up_weight[0], down_weight[0]
    width = gate_local.shape[0]
    slots = ep * 32
    at = jnp.stack([lax.axis_index("c"), lax.axis_index("z"), lax.axis_index("x")]).astype(
        jnp.int32
    )

    table = call(
        dispatch_kernel, sds((slots, columns), BF16), "dispatch", (routes.T, expert_input)
    )
    arrived = exchange(table.reshape(ep, 32, columns), EP).reshape(4, 1, slots // 4, columns)

    pair = jnp.concatenate([gate_local, up_local], axis=0)
    far = [from_next(pair, "y", k) for k in (1, 2, 3)]
    own_half = lax.dynamic_slice_in_dim(
        mix_weight, at[0] * (mix_weight.shape[0] // 2), mix_weight.shape[0] // 2, 0
    )
    mix_far = [from_next(own_half, "x", k) for k in (1, 2, 3)]
    mix_swap = [from_next(w, "c", 1) for w in mix_far]

    mine = call(
        summary_kernel,
        sds((dk + 8, dv), F32),
        "summary",
        (key_rows, value_rows, in_gate, forget_gate),
    )
    other = from_next(mine, "c", 1)
    packed = call(chip_kernel, sds((dk + 16, dv // 2), BF16), "chip", (at, mine, other))
    chips = lax.all_gather(packed, "z", axis=0)
    prior = call(prior_kernel, sds((dk + 8, dv // 2), F32), "prior", (at, chips))
    prior_other = from_next(prior, "c", 1)
    heads = call(
        output_kernel,
        sds((4, rows_a, dv), BF16),
        "outputs",
        (
            at, query_rows, key_rows, value_rows, in_gate, forget_gate, out_gate,
            head_gain[None, :], prior, prior_other, other,
        ),
    )

    sent = jnp.broadcast_to(arrived, (4, 4, slots // 4, columns)).reshape(tp, slots // 4, columns)
    rows = exchange(sent, TP)
    grid = 8
    per = tp // grid
    weights_spec = lambda r: pl.BlockSpec((r, per * columns), lambda i: (0, i))
    hidden = call(
        hidden_kernel,
        sds((tp, slots // 4, 4 * width), BF16),
        "hidden",
        (rows, gate_local, up_local, *far),
        scratch=[pltpu.VMEM((slots // 4, 4 * width), F32)] * 2
        + [pltpu.VMEM((slots // 4, columns), F32)],
        grid=(grid,),
        in_specs=[
            pl.BlockSpec((per, slots // 4, columns), lambda i: (i, 0, 0)),
            weights_spec(width),
            weights_spec(width),
        ]
        + [weights_spec(2 * width)] * 3,
        out_specs=pl.BlockSpec((tp, slots // 4, 4 * width), lambda i: (0, 0, 0)),
    )
    gathered = exchange(hidden, TP)
    results = call(down_kernel, sds((slots, columns), BF16), "down", (gathered, down_local))
    back = exchange(results.reshape(ep, 32, columns), EP).reshape(slots, columns)

    block = rows_a // 4
    head_rows = exchange(heads.reshape(tp, block, dv), TP)
    half = tp // 2
    weight_block = pl.BlockSpec((dv, columns), lambda i: (i, 0))
    projected = call(
        mix_kernel,
        sds((4, block, columns), BF16),
        "mix",
        (at, head_rows, mix_weight.reshape(2, half, dv, columns), *mix_far, *mix_swap),
        scratch=[pltpu.VMEM((4, block, columns), F32)],
        grid=(half,),
        in_specs=[
            pl.BlockSpec(memory_space=pltpu.SMEM),
            pl.BlockSpec((tp, block, dv), lambda i: (0, 0, 0)),
            pl.BlockSpec((2, 1, dv, columns), lambda i: (0, i, 0, 0)),
        ]
        + [weight_block] * 6,
        out_specs=pl.BlockSpec((4, block, columns), lambda i: (0, 0, 0)),
    )
    mixer_out = exchange(projected, "x").reshape(rows_a, columns)

    expert_out = call(
        collect_kernel, sds((tokens, columns), BF16), "collect", (routes, route_weight, back)
    )
    return (mixer_out, expert_out)


def solution(mesh):
    split = Mesh(mesh.devices.reshape(16, 2, 4, 4), (*EP, *TP))
    in_specs = (
        P(EP, TP),
        P(EP, TP),
        P(EP, TP),
        P(TP, EP),
        P(TP, EP),
        P(EP, TP),
        P(TP),
        P(None, TP),
        P(EP, TP),
        P(EP, None),
        P(EP, None),
        P(EP, TP, None),
        P(EP, TP, None),
        P(EP, None, TP),
    )
    out_specs = (P(EP, TP), P(EP, TP))
    return jax.shard_map(body, mesh=split, in_specs=in_specs, out_specs=out_specs, check_vma=False)
```

```python
import jax
import jax.numpy as jnp
from jax import lax
from jax.experimental import pallas as pl
from jax.experimental.pallas import tpu as pltpu
from jax.sharding import Mesh
from jax.sharding import PartitionSpec as P


EP = ("z", "c")
TP = ("y", "x")
EPSILON = 1e-06
LOG_FLOOR = -1e30
MASKED = -1e38
HIGHEST = lax.Precision.HIGHEST
F32 = jnp.float32
BF16 = jnp.bfloat16


def dot(a, b):
    return jnp.dot(a, b, preferred_element_type=F32)


def dot_t(a, b):
    return lax.dot_general(a, b, (((1,), (1,)), ((), ())), preferred_element_type=F32)


def iota(shape, dim):
    return lax.broadcasted_iota(jnp.int32, shape, dim)


def call(kernel, out, args, scratch=(), grid=None, in_specs=None, out_specs=None):
    vmem = pl.BlockSpec(memory_space=pltpu.VMEM)
    smem = pl.BlockSpec(memory_space=pltpu.SMEM)
    if in_specs is None:
        in_specs = [smem if a.dtype == jnp.int32 and a.ndim == 1 else vmem for a in args]
    kw = {} if grid is None else {"grid": grid}
    if out_specs is None:
        out_specs = jax.tree.map(lambda _: vmem, out)
    return pl.pallas_call(
        kernel,
        out_shape=out,
        in_specs=in_specs,
        out_specs=out_specs,
        scratch_shapes=list(scratch),
        **kw,
    )(*args)


def log_sigmoid(f):
    return jnp.minimum(f, 0.0) - jnp.log1p(jnp.exp(-jnp.abs(f)))


def cumulative_forms(forget_row):
    n = forget_row.shape[1]
    logs = jnp.broadcast_to(log_sigmoid(forget_row), (n, n))
    at_row, at_col = iota((n, n), 0), iota((n, n), 1)
    column = jnp.sum(jnp.where(at_col <= at_row, logs, 0.0), axis=1, keepdims=True)
    own = jnp.sum(jnp.where(at_col == at_row, logs, 0.0), axis=1, keepdims=True)
    row = jnp.sum(jnp.where(at_row <= at_col, own, 0.0), axis=0, keepdims=True)
    return column, row


def summary_kernel(k_ref, v_ref, in_ref, forget_ref, out_ref):
    n = k_ref.shape[0]
    dk = k_ref.shape[1]
    column, _ = cumulative_forms(forget_ref[...])
    diagonal = iota((n, n), 0) == iota((n, n), 1)
    log_in = jnp.sum(
        jnp.where(diagonal, jnp.broadcast_to(in_ref[...], (n, n)), 0.0), axis=1, keepdims=True
    )
    total = column[n - 1 :, :]
    weight_log = total - column + log_in
    top = jnp.max(weight_log, axis=0, keepdims=True)
    weighted = k_ref[...].astype(F32) * jnp.exp(weight_log - top)
    memory = lax.dot_general(
        weighted.astype(BF16), v_ref[...], (((0,), (0,)), ((), ())), preferred_element_type=F32
    )
    normal = jnp.sum(weighted, axis=0, keepdims=True)
    width = out_ref.shape[1]
    out_ref[0:dk, :] = memory
    out_ref[dk : dk + 1, 0:dk] = normal
    out_ref[dk : dk + 1, dk:] = normal
    out_ref[dk + 1 : dk + 2, :] = jnp.broadcast_to(total, (1, width))
    out_ref[dk + 2 : dk + 3, :] = jnp.broadcast_to(top, (1, width))
    out_ref[dk + 3 :, :] = jnp.zeros((out_ref.shape[0] - dk - 3, width), F32)


def parts_of(x, dk):
    return x[0:dk, :], x[dk : dk + 1, :], x[dk + 1 : dk + 2, :], x[dk + 2 : dk + 3, :]


def fold(first, second):
    memory_1, normal_1, decay_1, max_1 = first
    memory_2, normal_2, decay_2, max_2 = second
    top = jnp.maximum(decay_2 + max_1, max_2)
    keep_1 = jnp.exp(decay_2 + max_1 - top)
    keep_2 = jnp.exp(max_2 - top)
    return (
        keep_1 * memory_1 + keep_2 * memory_2,
        keep_1 * normal_1 + keep_2 * normal_2,
        decay_1 + decay_2,
        top,
    )


def split3(x):
    high = x.astype(BF16)
    rest = x - high.astype(F32)
    middle = rest.astype(BF16)
    low = (rest - middle.astype(F32)).astype(BF16)
    return high, middle, low


def pack(out_ref, memory, normal, decay, top):
    dk, width = memory.shape
    out_ref[0:dk, :] = memory.astype(BF16)
    rows = []
    for value in (normal, decay, top):
        rows += [part.astype(F32) for part in split3(value)]
    rows.append(jnp.zeros((out_ref.shape[0] - dk - len(rows), width), F32))
    out_ref[dk:, :] = jnp.concatenate(rows, axis=0).astype(BF16)


def unpack(item, dk):
    item = item.astype(F32)
    rows = [
        item[dk + i : dk + i + 1] + item[dk + i + 1 : dk + i + 2] + item[dk + i + 2 : dk + i + 3]
        for i in (0, 3, 6)
    ]
    return (item[0:dk], *rows)


def first_state(dk, width):
    return (
        jnp.zeros((dk, width), F32),
        jnp.zeros((1, width), F32),
        jnp.zeros((1, width), F32),
        jnp.full((1, width), LOG_FLOOR, F32),
    )


def fold_earlier(all_ref, here, dk):
    state = before = first_state(dk, all_ref.shape[2])
    for k in range(all_ref.shape[0]):
        state = fold(state, unpack(all_ref[k], dk))
        before = tuple(jnp.where(k < here, new, old) for new, old in zip(state, before))
    return before, state


def store_state(out_ref, state):
    memory, normal, decay, top = state
    dk, width = memory.shape
    out_ref[0:dk, :] = memory
    out_ref[dk:, :] = jnp.concatenate(
        [normal, decay, top, jnp.zeros((out_ref.shape[0] - dk - 3, width), F32)], axis=0
    )


def chip_kernel(at_ref, mine_ref, other_ref, packed_ref):
    dk = 128
    south = at_ref[0] == 0
    mine, other = mine_ref[...], other_ref[...]
    first = parts_of(jnp.where(south, mine, other), dk)
    second = parts_of(jnp.where(south, other, mine), dk)
    total = fold(first, second)
    half = mine.shape[1] // 2
    pack(packed_ref, *[jnp.where(south, v[:, :half], v[:, half:]) for v in total])


def prior_kernel(at_ref, all_ref, out_ref):
    before, _ = fold_earlier(all_ref, at_ref[1], 128)
    store_state(out_ref, before)


def output_kernel(
    at_ref, q_ref, k_ref, v_ref, in_ref, forget_ref, gate_ref, gain_ref,
    prior_ref, prior_other_ref, other_ref, out_ref,
):
    n, dk = q_ref.shape
    scale = dk ** (-0.5)
    south = at_ref[0] == 0
    column, row = cumulative_forms(forget_ref[...])
    left = jnp.where(south, prior_ref[...], prior_other_ref[...])
    right = jnp.where(south, prior_other_ref[...], prior_ref[...])
    before = parts_of(jnp.concatenate([left, right], axis=1), dk)
    joined = fold(before, parts_of(other_ref[...], dk))
    memory, normal, _, top_before = [jnp.where(south, b, j) for b, j in zip(before, joined)]
    normal = normal[:, :dk]
    top_before = top_before[:, 0:1]
    log_in = in_ref[...]
    step = n // 4
    for start in range(0, n, step):
        rows, seen = slice(start, start + step), start + step
        q = q_ref[rows, :]
        at = column[rows, :]
        causal = iota((step, seen), 1) <= iota((step, seen), 0) + start
        log_decay = jnp.where(causal, at - row[:, :seen] + log_in[:, :seen], MASKED)
        log_inter = at + top_before
        top = jnp.maximum(log_inter, jnp.max(log_decay, axis=1, keepdims=True))
        scores = dot_t(q, k_ref[0:seen, :]) * scale * jnp.exp(log_decay - top)
        carried = jnp.exp(log_inter - top) * scale
        wide = q.astype(F32)
        numerator = carried * jnp.dot(
            wide, memory, precision=HIGHEST, preferred_element_type=F32
        ) + dot(scores.astype(BF16), v_ref[0:seen, :])
        denominator = carried * jnp.sum(wide * normal, axis=1, keepdims=True) + jnp.sum(
            scores, axis=1, keepdims=True
        )
        values = numerator / jnp.maximum(jnp.abs(denominator), jnp.exp(-top))
        values = values * lax.rsqrt(jnp.mean(values * values, axis=1, keepdims=True) + EPSILON)
        gate = gate_ref[rows, :].astype(F32)
        values = values * gain_ref[...] * (1.0 / (1.0 + jnp.exp(-gate)))
        side, inner = divmod(start, n // 2)
        out_ref[lax.rem(at_ref[2] + side, 2), inner : inner + step, :] = values.astype(BF16)


def dispatch_kernel(routes_ref, x_ref, out_ref):
    tokens = x_ref.shape[0]
    slots = out_ref.shape[0]
    experts, room = 32, slots // 32
    expert = iota((experts, tokens), 0)
    named = jnp.zeros((experts, tokens), F32)
    for r in range(routes_ref.shape[0]):
        named = named + (routes_ref[r : r + 1, :] == expert).astype(F32)
    earlier = (iota((tokens, tokens), 0) < iota((tokens, tokens), 1)).astype(F32).astype(BF16)
    place = dot(named.astype(BF16), earlier)
    key = jnp.where(named > 0.5, place, -1.0).astype(BF16)
    slot = iota((slots, experts), 0)
    spread = (slot // room == iota((slots, experts), 1)).astype(F32).astype(BF16)
    wanted = (iota((slots, tokens), 0) % room).astype(F32)
    chosen = (dot(spread, key) == wanted).astype(F32).astype(BF16)
    out_ref[...] = dot(chosen, x_ref[...]).astype(BF16)


def pair_kernel(gate_ref, up_ref, out_ref):
    width = gate_ref.shape[0]
    out_ref[0:width, :] = gate_ref[...]
    out_ref[width:, :] = up_ref[...]


def collect_kernel(routes_ref, weight_ref, back_ref, out_ref):
    tokens = out_ref.shape[0]
    slots = back_ref.shape[0]
    experts, room = 32, slots // 32
    expert = iota((tokens, experts), 1)
    named = jnp.zeros((tokens, experts), F32)
    weight = jnp.zeros((tokens, experts), F32)
    for r in range(routes_ref.shape[1]):
        hit = routes_ref[:, r : r + 1] == expert
        named = named + hit.astype(F32)
        weight = weight + jnp.where(hit, weight_ref[:, r : r + 1], 0.0)
    earlier = (iota((tokens, tokens), 1) < iota((tokens, tokens), 0)).astype(F32).astype(BF16)
    place = dot(earlier, named.astype(BF16))
    key = jnp.where(named > 0.5, place, -1.0).astype(BF16)
    slot = iota((experts, slots), 1)
    spread = (slot // room == iota((experts, slots), 0)).astype(F32).astype(BF16)
    wanted = (iota((tokens, slots), 1) % room).astype(F32)
    chosen = dot(key, spread) == wanted
    total = jnp.zeros(out_ref.shape, F32)
    for part in split3(weight):
        share = jnp.where(chosen, dot(part, spread), 0.0).astype(BF16)
        total = total + dot(share, back_ref[...])
    out_ref[...] = total.astype(BF16)


def hidden_kernel(
    x_ref, gate_ref, up_ref, w1_ref, w2_ref, w3_ref, out_ref, gate_acc, up_acc, squares
):
    step = pl.program_id(0)
    width = gate_ref.shape[0]
    far = (w1_ref, w2_ref, w3_ref)
    senders, _, columns = x_ref.shape
    x = jnp.concatenate([x_ref[i] for i in range(senders)], axis=1)
    gate = jnp.concatenate([gate_ref[...]] + [w[0:width] for w in far], axis=0)
    up = jnp.concatenate([up_ref[...]] + [w[width:] for w in far], axis=0)
    gate_part, up_part = dot_t(x, gate), dot_t(x, up)
    square = jnp.zeros(squares.shape, F32)
    for i in range(senders):
        wide = x_ref[i].astype(F32)
        square = square + wide * wide

    @pl.when(step == 0)
    def _():
        gate_acc[...] = gate_part
        up_acc[...] = up_part
        squares[...] = square

    @pl.when(step > 0)
    def _():
        gate_acc[...] += gate_part
        up_acc[...] += up_part
        squares[...] += square

    @pl.when(step == pl.num_programs(0) - 1)
    def _():
        total = jnp.sum(squares[...], axis=1, keepdims=True)
        inverse = lax.rsqrt(total * (1.0 / (columns * out_ref.shape[0])) + EPSILON)
        gate = gate_acc[...] * inverse
        hidden = gate * (1.0 / (1.0 + jnp.exp(-gate))) * (up_acc[...] * inverse)
        hidden = hidden.astype(BF16)
        for copy in range(out_ref.shape[0]):
            out_ref[copy] = hidden


def down_kernel(h_ref, w_ref, out_ref):
    part = h_ref.shape[2] // 4
    rows = h_ref.shape[1]
    for ys in range(4):
        total = jnp.zeros((rows, w_ref.shape[1]), F32)
        for xs in range(4):
            at = [(((ys + j) % 4) * 4 + xs) * part for j in range(4)]
            weight = jnp.concatenate([w_ref[a : a + part, :] for a in at], axis=0)
            total = total + dot(h_ref[ys * 4 + xs], weight)
        out_ref[ys * rows : (ys + 1) * rows, :] = total.astype(BF16)


def mix_kernel(
    at_ref, h0_ref, h1_ref, h2_ref, h3_ref, near_ref, a_ref, b_ref, o0_ref, o1_ref, acc, heads
):
    step = pl.program_id(0)
    half = heads.shape[0] // 2
    c, x, y = at_ref[0], at_ref[2], at_ref[3]

    @pl.when(step == 0)
    def _():
        acc[...] = jnp.zeros_like(acc)
        for ky, ref in enumerate((h0_ref, h1_ref, h2_ref, h3_ref)):
            for kx in range(4):
                heads[lax.rem(y + ky, 4) * 4 + lax.rem(x + 4 - kx, 4)] = ref[kx]

    pieces = near_ref.shape[1]
    width = near_ref.shape[2]
    own = jnp.zeros(acc.shape[1:], F32)
    pair = jnp.zeros(acc.shape[1:], F32)
    for i in range(pieces):
        k = step * pieces + i
        rows = slice(i * width, (i + 1) * width)
        own = own + dot(heads[k], near_ref[0, i]) + dot(heads[half + k], near_ref[1, i])
        pair = pair + dot(heads[c * half + k], a_ref[rows, :])
        pair = pair + dot(heads[(1 - c) * half + k], b_ref[rows, :])
    acc[0] += own
    acc[1] += pair

    @pl.when(step == pl.num_programs(0) - 1)
    def _():
        o0_ref[...] = acc[0].astype(BF16)
        o1_ref[...] = acc[1].astype(BF16)


def assemble_kernel(at_ref, own_ref, pair_ref, out_ref):
    block = own_ref.shape[0]
    side = lax.rem(at_ref[2], 2)
    out_ref[pl.ds(pl.multiple_of(side * block, block), block), :] = own_ref[...]
    out_ref[pl.ds(pl.multiple_of((1 - side) * block, block), block), :] = pair_ref[...]


def from_next(x, axis, k):
    n = lax.axis_size(axis)
    return lax.ppermute(x, axis, [((i + k) % n, i) for i in range(n)])


def swapped(x, axis):
    n = lax.axis_size(axis)
    return lax.ppermute(x, axis, [(i ^ 1, i) for i in range(n)])


def exchange(x, axis):
    return lax.all_to_all(x, axis, split_axis=0, concat_axis=0, tiled=True)


def body(
    query_rows,
    key_rows,
    value_rows,
    in_gate,
    forget_gate,
    out_gate,
    head_gain,
    mix_weight,
    expert_input,
    routes,
    route_weight,
    gate_weight,
    up_weight,
    down_weight,
):
    sds = jax.ShapeDtypeStruct
    rows_a, dk = query_rows.shape
    dv = value_rows.shape[1]
    tokens, columns = expert_input.shape
    ep, tp = lax.axis_size(EP), lax.axis_size(TP)
    gate_local, up_local, down_local = gate_weight[0], up_weight[0], down_weight[0]
    width = gate_local.shape[0]
    slots = ep * 32
    at = jnp.stack(
        [lax.axis_index(axis) for axis in ("c", "z", "x", "y")]
    ).astype(jnp.int32)

    table = call(dispatch_kernel, sds((slots, columns), BF16), (routes.T, expert_input))
    arrived = exchange(table.reshape(ep, 32, columns), EP)
    arrived = arrived.reshape(4, 1, slots // 4, columns)

    pair = call(pair_kernel, sds((2 * width, gate_local.shape[1]), BF16), (gate_local, up_local))
    own_half = lax.dynamic_slice_in_dim(
        mix_weight, at[0] * (mix_weight.shape[0] // 2), mix_weight.shape[0] // 2, 0
    )
    far = []
    for k in (1, 2, 3):
        far.append(from_next(pair, "y", k))
    mix_far = swapped(own_half, "x")
    mix_swap = swapped(mix_far, "c")

    mine = call(
        summary_kernel, sds((dk + 8, dv), F32), (key_rows, value_rows, in_gate, forget_gate)
    )
    other = swapped(mine, "c")
    packed = call(chip_kernel, sds((dk + 16, dv // 2), BF16), (at, mine, other))
    chips = lax.all_gather(packed, "z", axis=0)
    prior = call(prior_kernel, sds((dk + 8, dv // 2), F32), (at, chips))
    prior_other = swapped(prior, "c")
    block = rows_a // 2
    heads = call(
        output_kernel,
        sds((2, block, dv), BF16),
        (
            at, query_rows, key_rows, value_rows, in_gate, forget_gate, out_gate,
            head_gain[None, :], prior, prior_other, other,
        ),
    )

    sent = jnp.broadcast_to(arrived, (4, 4, slots // 4, columns)).reshape(tp, slots // 4, columns)
    rows = exchange(sent, TP)
    grid = 2
    per = tp // grid
    weights_spec = lambda r: pl.BlockSpec((r, per * columns), lambda i: (0, i))
    hidden = call(
        hidden_kernel,
        sds((tp, slots // 4, 4 * width), BF16),
        (rows, gate_local, up_local, *far),
        scratch=[pltpu.VMEM((slots // 4, 4 * width), F32)] * 2
        + [pltpu.VMEM((slots // 4, columns), F32)],
        grid=(grid,),
        in_specs=[
            pl.BlockSpec((per, slots // 4, columns), lambda i: (i, 0, 0)),
            weights_spec(width),
            weights_spec(width),
        ]
        + [weights_spec(2 * width)] * 3,
        out_specs=pl.BlockSpec((tp, slots // 4, 4 * width), lambda i: (0, 0, 0)),
    )
    gathered = exchange(hidden, TP)
    results = call(down_kernel, sds((slots, columns), BF16), (gathered, down_local))
    back = exchange(results.reshape(ep, 32, columns), EP).reshape(slots, columns)

    along_x = [heads[0]]
    for k in (1, 2, 3):
        along_x.append(from_next(heads[k % 2], "x", -k))
    along_x = jnp.stack(along_x)
    head_rows = [along_x]
    for k in (1, 2, 3):
        head_rows.append(from_next(along_x, "y", k))
    half = tp // 2
    steps = 2
    pieces = half // steps
    weight_block = pl.BlockSpec((pieces * dv, columns), lambda i: (i, 0))
    projected = call(
        mix_kernel,
        [sds((block, columns), BF16)] * 2,
        (at, *head_rows, mix_weight.reshape(2, half, dv, columns), mix_far, mix_swap),
        scratch=[pltpu.VMEM((2, block, columns), F32), pltpu.VMEM((tp, block, dv), BF16)],
        grid=(steps,),
        in_specs=[pl.BlockSpec(memory_space=pltpu.SMEM)]
        + [pl.BlockSpec((4, block, dv), lambda i: (0, 0, 0))] * 4
        + [pl.BlockSpec((2, pieces, dv, columns), lambda i: (0, i, 0, 0))]
        + [weight_block] * 2,
        out_specs=[pl.BlockSpec((block, columns), lambda i: (0, 0))] * 2,
    )
    from_pair = swapped(projected[1], "x")
    mixer_out = call(assemble_kernel, sds((rows_a, columns), BF16), (at, projected[0], from_pair))

    expert_out = call(collect_kernel, sds((tokens, columns), BF16), (routes, route_weight, back))
    return (mixer_out, expert_out)


def solution(mesh):
    split = Mesh(mesh.devices.reshape(16, 2, 4, 4), (*EP, *TP))
    in_specs = (
        P(EP, TP),
        P(EP, TP),
        P(EP, TP),
        P(TP, EP),
        P(TP, EP),
        P(EP, TP),
        P(TP),
        P(None, TP),
        P(EP, TP),
        P(EP, None),
        P(EP, None),
        P(EP, TP, None),
        P(EP, TP, None),
        P(EP, None, TP),
    )
    out_specs = (P(EP, TP), P(EP, TP))

    return jax.shard_map(body, mesh=split, in_specs=in_specs, out_specs=out_specs, check_vma=False)
```

```python
import functools

import jax
import jax.numpy as jnp
from jax import lax
from jax.experimental import pallas as pl
from jax.experimental.pallas import tpu as pltpu
from jax.sharding import Mesh
from jax.sharding import PartitionSpec as P


EP = ("z", "c")
TP = ("y", "x")
EPSILON = 1e-06
LOG_FLOOR = -1e30
MASKED = -1e38
HIGHEST = lax.Precision.HIGHEST
F32 = jnp.float32
BF16 = jnp.bfloat16


def dot(a, b):
    return jnp.dot(a, b, preferred_element_type=F32)


def dot_t(a, b):
    return lax.dot_general(a, b, (((1,), (1,)), ((), ())), preferred_element_type=F32)


def iota(shape, dim):
    return lax.broadcasted_iota(jnp.int32, shape, dim)


def call(kernel, out, args, scratch=(), grid=None, in_specs=None, out_specs=None, near=()):
    args = [
        pltpu.with_memory_space_constraint(a, pltpu.VMEM) if i in near else a
        for i, a in enumerate(args)
    ]
    vmem = pl.BlockSpec(memory_space=pltpu.VMEM)
    smem = pl.BlockSpec(memory_space=pltpu.SMEM)
    if in_specs is None:
        in_specs = [smem if a.dtype == jnp.int32 and a.ndim == 1 else vmem for a in args]
    kw = {} if grid is None else {"grid": grid}
    if out_specs is None:
        out_specs = jax.tree.map(lambda _: vmem, out)
    return pl.pallas_call(
        kernel,
        out_shape=out,
        in_specs=in_specs,
        out_specs=out_specs,
        scratch_shapes=list(scratch),
        compiler_params=pltpu.CompilerParams(vmem_limit_bytes=57 << 20),
        **kw,
    )(*args)


def log_sigmoid(f):
    return jnp.minimum(f, 0.0) - jnp.log1p(jnp.exp(-jnp.abs(f)))


def cumulative_forms(forget_row):
    n = forget_row.shape[1]
    logs = jnp.broadcast_to(log_sigmoid(forget_row), (n, n))
    at_row, at_col = iota((n, n), 0), iota((n, n), 1)
    column = jnp.sum(jnp.where(at_col <= at_row, logs, 0.0), axis=1, keepdims=True)
    own = jnp.sum(jnp.where(at_col == at_row, logs, 0.0), axis=1, keepdims=True)
    row = jnp.sum(jnp.where(at_row <= at_col, own, 0.0), axis=0, keepdims=True)
    return column, row


def summary_kernel(k_ref, v_ref, in_ref, forget_ref, out_ref):
    n = k_ref.shape[0]
    dk = k_ref.shape[1]
    column, _ = cumulative_forms(forget_ref[...])
    diagonal = iota((n, n), 0) == iota((n, n), 1)
    log_in = jnp.sum(
        jnp.where(diagonal, jnp.broadcast_to(in_ref[...], (n, n)), 0.0), axis=1, keepdims=True
    )
    total = column[n - 1 :, :]
    weight_log = total - column + log_in
    top = jnp.max(weight_log, axis=0, keepdims=True)
    weighted = k_ref[...].astype(F32) * jnp.exp(weight_log - top)
    memory = lax.dot_general(
        weighted.astype(BF16), v_ref[...], (((0,), (0,)), ((), ())), preferred_element_type=F32
    )
    normal = jnp.sum(weighted, axis=0, keepdims=True)
    width = out_ref.shape[1]
    out_ref[0:dk, :] = memory
    out_ref[dk : dk + 1, 0:dk] = normal
    out_ref[dk : dk + 1, dk:] = normal
    out_ref[dk + 1 : dk + 2, :] = jnp.broadcast_to(total, (1, width))
    out_ref[dk + 2 : dk + 3, :] = jnp.broadcast_to(top, (1, width))
    out_ref[dk + 3 :, :] = jnp.zeros((out_ref.shape[0] - dk - 3, width), F32)


def parts_of(x, dk):
    return x[0:dk, :], x[dk : dk + 1, :], x[dk + 1 : dk + 2, :], x[dk + 2 : dk + 3, :]


def fold(first, second):
    memory_1, normal_1, decay_1, max_1 = first
    memory_2, normal_2, decay_2, max_2 = second
    top = jnp.maximum(decay_2 + max_1, max_2)
    keep_1 = jnp.exp(decay_2 + max_1 - top)
    keep_2 = jnp.exp(max_2 - top)
    return (
        keep_1 * memory_1 + keep_2 * memory_2,
        keep_1 * normal_1 + keep_2 * normal_2,
        decay_1 + decay_2,
        top,
    )


def split3(x):
    high = x.astype(BF16)
    rest = x - high.astype(F32)
    middle = rest.astype(BF16)
    low = (rest - middle.astype(F32)).astype(BF16)
    return high, middle, low


def pack(out_ref, memory, normal, decay, top):
    dk, width = memory.shape
    out_ref[0:dk, :] = memory.astype(BF16)
    rows = []
    for value in (normal, decay, top):
        rows += [part.astype(F32) for part in split3(value)]
    rows.append(jnp.zeros((out_ref.shape[0] - dk - len(rows), width), F32))
    out_ref[dk:, :] = jnp.concatenate(rows, axis=0).astype(BF16)


def unpack(item, dk):
    item = item.astype(F32)
    rows = [
        item[dk + i : dk + i + 1] + item[dk + i + 1 : dk + i + 2] + item[dk + i + 2 : dk + i + 3]
        for i in (0, 3, 6)
    ]
    return (item[0:dk], *rows)


def first_state(dk, width):
    return (
        jnp.zeros((dk, width), F32),
        jnp.zeros((1, width), F32),
        jnp.zeros((1, width), F32),
        jnp.full((1, width), LOG_FLOOR, F32),
    )


def store_state(out_ref, state):
    memory, normal, decay, top = state
    dk, width = memory.shape
    out_ref[0:dk, :] = memory
    out_ref[dk:, :] = jnp.concatenate(
        [normal, decay, top, jnp.zeros((out_ref.shape[0] - dk - 3, width), F32)], axis=0
    )


def chip_kernel(at_ref, mine_ref, other_ref, total_ref, packed_ref):
    dk = 128
    south = at_ref[0] == 0
    mine, other = mine_ref[...], other_ref[...]
    first = parts_of(jnp.where(south, mine, other), dk)
    second = parts_of(jnp.where(south, other, mine), dk)
    total = fold(first, second)
    half = mine.shape[1] // 2
    total = [jnp.where(south, v[:, :half], v[:, half:]) for v in total]
    store_state(total_ref, total)
    pack(packed_ref, *total)


def step_kernel(reach, first, last, at_ref, came_ref, *refs):
    dk = 128
    valid = at_ref[1] >= reach
    came = unpack(came_ref[...], dk)
    if first:
        before = first_state(dk, came_ref.shape[1])
    else:
        before, refs = parts_of(refs[0][...], dk), refs[1:]
    joined = fold(came, before)
    if not last:
        total = parts_of(refs[0][...], dk)
        more = fold(came, total)
        total = [jnp.where(valid, new, old) for new, old in zip(more, total)]
        store_state(refs[1], total)
        pack(refs[3], *total)
    store_state(refs[0 if last else 2], [jnp.where(valid, n, o) for n, o in zip(joined, before)])


def output_kernel(
    at_ref, q_ref, k_ref, v_ref, in_ref, forget_ref, gate_ref, gain_ref,
    prior_ref, prior_other_ref, other_ref, out_ref,
):
    n, dk = q_ref.shape
    scale = dk ** (-0.5)
    south = at_ref[0] == 0
    column, row = cumulative_forms(forget_ref[...])
    left = jnp.where(south, prior_ref[...], prior_other_ref[...])
    right = jnp.where(south, prior_other_ref[...], prior_ref[...])
    before = parts_of(jnp.concatenate([left, right], axis=1), dk)
    joined = fold(before, parts_of(other_ref[...], dk))
    memory, normal, _, top_before = [jnp.where(south, b, j) for b, j in zip(before, joined)]
    normal = normal[:, :dk]
    top_before = top_before[:, 0:1]
    log_in = in_ref[...]
    step = n // 4
    for start in range(0, n, step):
        rows, seen = slice(start, start + step), start + step
        q = q_ref[rows, :]
        at = column[rows, :]
        causal = iota((step, seen), 1) <= iota((step, seen), 0) + start
        log_decay = jnp.where(causal, at - row[:, :seen] + log_in[:, :seen], MASKED)
        log_inter = at + top_before
        top = jnp.maximum(log_inter, jnp.max(log_decay, axis=1, keepdims=True))
        scores = dot_t(q, k_ref[0:seen, :]) * scale * jnp.exp(log_decay - top)
        carried = jnp.exp(log_inter - top) * scale
        wide = q.astype(F32)
        numerator = carried * jnp.dot(
            wide, memory, precision=HIGHEST, preferred_element_type=F32
        ) + dot(scores.astype(BF16), v_ref[0:seen, :])
        denominator = carried * jnp.sum(wide * normal, axis=1, keepdims=True) + jnp.sum(
            scores, axis=1, keepdims=True
        )
        values = numerator / jnp.maximum(jnp.abs(denominator), jnp.exp(-top))
        values = values * lax.rsqrt(jnp.mean(values * values, axis=1, keepdims=True) + EPSILON)
        gate = gate_ref[rows, :].astype(F32)
        values = values * gain_ref[...] * (1.0 / (1.0 + jnp.exp(-gate)))
        side, inner = divmod(start, n // 2)
        out_ref[lax.rem(at_ref[2] + side, 2), inner : inner + step, :] = values.astype(BF16)


def dispatch_kernel(routes_ref, x_ref, out_ref):
    tokens = x_ref.shape[0]
    slots = out_ref.shape[0]
    experts, room = 32, slots // 32
    expert = iota((experts, tokens), 0)
    named = jnp.zeros((experts, tokens), F32)
    for r in range(routes_ref.shape[0]):
        named = named + (routes_ref[r : r + 1, :] == expert).astype(F32)
    earlier = (iota((tokens, tokens), 0) < iota((tokens, tokens), 1)).astype(F32).astype(BF16)
    place = dot(named.astype(BF16), earlier)
    key = jnp.where(named > 0.5, place, -1.0).astype(BF16)
    slot = iota((slots, experts), 0)
    spread = (slot // room == iota((slots, experts), 1)).astype(F32).astype(BF16)
    wanted = (iota((slots, tokens), 0) % room).astype(F32)
    chosen = (dot(spread, key) == wanted).astype(F32).astype(BF16)
    out_ref[...] = dot(chosen, x_ref[...]).astype(BF16)


def pair_kernel(gate_ref, up_ref, out_ref):
    width = gate_ref.shape[0]
    out_ref[0:width, :] = gate_ref[...]
    out_ref[width:, :] = up_ref[...]


def plan_kernel(routes_ref, weight_ref, high_ref, low_ref):
    tokens, slots = high_ref.shape
    experts, room = 32, slots // 32
    expert = iota((tokens, experts), 1)
    named = jnp.zeros((tokens, experts), F32)
    weight = jnp.zeros((tokens, experts), F32)
    for r in range(routes_ref.shape[1]):
        hit = routes_ref[:, r : r + 1] == expert
        named = named + hit.astype(F32)
        weight = weight + jnp.where(hit, weight_ref[:, r : r + 1], 0.0)
    earlier = (iota((tokens, tokens), 1) < iota((tokens, tokens), 0)).astype(F32).astype(BF16)
    place = dot(earlier, named.astype(BF16))
    key = jnp.where(named > 0.5, place, -1.0).astype(BF16)
    slot = iota((experts, slots), 1)
    spread = (slot // room == iota((experts, slots), 0)).astype(F32).astype(BF16)
    wanted = (iota((tokens, slots), 1) % room).astype(F32)
    chosen = dot(key, spread) == wanted
    high, low, _ = split3(weight)
    high_ref[...] = jnp.where(chosen, dot(high, spread), 0.0).astype(BF16)
    low_ref[...] = jnp.where(chosen, dot(low, spread), 0.0).astype(BF16)


def collect_kernel(high_ref, low_ref, back_ref, out_ref):
    back = back_ref[...]
    out_ref[...] = (dot(high_ref[...], back) + dot(low_ref[...], back)).astype(BF16)


def hidden_kernel(
    x_ref, gate_ref, up_ref, w1_ref, w2_ref, w3_ref, out_ref, gate_acc, up_acc, squares
):
    step = pl.program_id(0)
    width = gate_ref.shape[0]
    far = (w1_ref, w2_ref, w3_ref)
    _, _, columns = x_ref.shape
    senders = gate_ref.shape[1] // columns
    pieces = [x_ref[step * senders + i] for i in range(senders)]
    x = jnp.concatenate(pieces, axis=1)
    gate = jnp.concatenate([gate_ref[...]] + [w[0:width] for w in far], axis=0)
    up = jnp.concatenate([up_ref[...]] + [w[width:] for w in far], axis=0)
    gate_part, up_part = dot_t(x, gate), dot_t(x, up)
    square = jnp.zeros(squares.shape, F32)
    for piece in pieces:
        wide = piece.astype(F32)
        square = square + wide * wide

    @pl.when(step == 0)
    def _():
        gate_acc[...] = gate_part
        up_acc[...] = up_part
        squares[...] = square

    @pl.when(step > 0)
    def _():
        gate_acc[...] += gate_part
        up_acc[...] += up_part
        squares[...] += square

    @pl.when(step == pl.num_programs(0) - 1)
    def _():
        total = jnp.sum(squares[...], axis=1, keepdims=True)
        inverse = lax.rsqrt(total * (1.0 / (columns * out_ref.shape[0])) + EPSILON)
        gate = gate_acc[...] * inverse
        hidden = gate * (1.0 / (1.0 + jnp.exp(-gate))) * (up_acc[...] * inverse)
        hidden = hidden.astype(BF16)
        for copy in range(out_ref.shape[0]):
            out_ref[copy] = hidden


def down_kernel(h_ref, w_ref, out_ref):
    part = h_ref.shape[2] // 4
    rows = h_ref.shape[1]
    for ys in range(4):
        total = jnp.zeros((rows, w_ref.shape[1]), F32)
        for xs in range(4):
            at = [(((ys + j) % 4) * 4 + xs) * part for j in range(4)]
            weight = jnp.concatenate([w_ref[a : a + part, :] for a in at], axis=0)
            total = total + dot(h_ref[ys * 4 + xs], weight)
        out_ref[ys * rows : (ys + 1) * rows, :] = total.astype(BF16)


def mix_kernel(
    at_ref, h0_ref, h1_ref, h2_ref, h3_ref, near_ref, a_ref, b_ref, o0_ref, o1_ref, acc, heads
):
    step = pl.program_id(0)
    half = heads.shape[0] // 2
    c, x, y = at_ref[0], at_ref[2], at_ref[3]

    @pl.when(step == 0)
    def _():
        acc[...] = jnp.zeros_like(acc)
        for ky, ref in enumerate((h0_ref, h1_ref, h2_ref, h3_ref)):
            for kx in range(4):
                heads[lax.rem(y + ky, 4) * 4 + lax.rem(x + 4 - kx, 4)] = ref[kx]

    pieces = near_ref.shape[1]
    width = near_ref.shape[2]
    own = jnp.zeros(acc.shape[1:], F32)
    pair = jnp.zeros(acc.shape[1:], F32)
    for i in range(pieces):
        k = step * pieces + i
        rows = slice(i * width, (i + 1) * width)
        own = own + dot(heads[k], near_ref[0, i]) + dot(heads[half + k], near_ref[1, i])
        pair = pair + dot(heads[c * half + k], a_ref[rows, :])
        pair = pair + dot(heads[(1 - c) * half + k], b_ref[rows, :])
    acc[0] += own
    acc[1] += pair

    @pl.when(step == pl.num_programs(0) - 1)
    def _():
        o0_ref[...] = acc[0].astype(BF16)
        o1_ref[...] = acc[1].astype(BF16)


def assemble_kernel(at_ref, own_ref, pair_ref, out_ref):
    block = own_ref.shape[0]
    side = lax.rem(at_ref[2], 2)
    out_ref[pl.ds(pl.multiple_of(side * block, block), block), :] = own_ref[...]
    out_ref[pl.ds(pl.multiple_of((1 - side) * block, block), block), :] = pair_ref[...]


def from_next(x, axis, k):
    n = lax.axis_size(axis)
    return lax.ppermute(x, axis, [((i + k) % n, i) for i in range(n)])


def swapped(x, axis):
    n = lax.axis_size(axis)
    return lax.ppermute(x, axis, [(i ^ 1, i) for i in range(n)])


def exchange(x, axis):
    return lax.all_to_all(x, axis, split_axis=0, concat_axis=0, tiled=True)


def body(
    query_rows,
    key_rows,
    value_rows,
    in_gate,
    forget_gate,
    out_gate,
    head_gain,
    mix_weight,
    expert_input,
    routes,
    route_weight,
    gate_weight,
    up_weight,
    down_weight,
):
    sds = jax.ShapeDtypeStruct
    rows_a, dk = query_rows.shape
    dv = value_rows.shape[1]
    tokens, columns = expert_input.shape
    ep, tp = lax.axis_size(EP), lax.axis_size(TP)
    gate_local, up_local, down_local = gate_weight[0], up_weight[0], down_weight[0]
    width = gate_local.shape[0]
    slots = ep * 32
    at = jnp.stack(
        [lax.axis_index(axis) for axis in ("c", "z", "x", "y")]
    ).astype(jnp.int32)

    table = call(dispatch_kernel, pltpu.VMEM((slots, columns), BF16), (routes.T, expert_input))
    arrived = exchange(table.reshape(ep, 32, columns), EP)
    arrived = arrived.reshape(4, 1, slots // 4, columns)

    pair = call(pair_kernel, sds((2 * width, gate_local.shape[1]), BF16), (gate_local, up_local))
    own_half = lax.dynamic_slice_in_dim(
        mix_weight, at[0] * (mix_weight.shape[0] // 2), mix_weight.shape[0] // 2, 0
    )
    far = []
    for k in (1, 2, 3):
        far.append(from_next(pair, "y", k))
    mix_far = swapped(own_half, "x")
    mix_swap = swapped(mix_far, "c")

    mine = call(
        summary_kernel, sds((dk + 8, dv), F32), (key_rows, value_rows, in_gate, forget_gate)
    )
    other = swapped(mine, "c")
    state, lines = sds((dk + 8, dv // 2), F32), sds((dk + 16, dv // 2), BF16)
    total, packed = call(chip_kernel, [state, lines], (at, mine, other), near=(2,))
    before, reach, chips = (), 1, lax.axis_size("z")
    while reach < chips:
        came = lax.ppermute(packed, "z", [(i, i + reach) for i in range(chips - reach)])
        last = 2 * reach == chips
        result = call(
            functools.partial(step_kernel, reach, reach == 1, last),
            [state] if last else [state, state, lines],
            (at, came, *before) + (() if last else (total,)),
            near=(1,),
        )
        if last:
            (prior,) = result
        else:
            total, before, packed = result[0], result[1:2], result[2]
        reach *= 2
    prior_other = swapped(prior, "c")
    block = rows_a // 2
    heads = call(
        output_kernel,
        sds((2, block, dv), BF16),
        (
            at, query_rows, key_rows, value_rows, in_gate, forget_gate, out_gate,
            head_gain[None, :], prior, prior_other, other,
        ),
        near=(9, 10),
    )

    sent = jnp.broadcast_to(arrived, (4, 4, slots // 4, columns)).reshape(tp, slots // 4, columns)
    rows = exchange(sent, TP)
    grid = 2
    per = tp // grid
    weights_spec = lambda r: pl.BlockSpec((r, per * columns), lambda i: (0, i))
    hidden = call(
        hidden_kernel,
        sds((tp, slots // 4, 4 * width), BF16),
        (rows, gate_local, up_local, *far),
        scratch=[pltpu.VMEM((slots // 4, 4 * width), F32)] * 2
        + [pltpu.VMEM((slots // 4, columns), F32)],
        grid=(grid,),
        in_specs=[
            pl.BlockSpec(memory_space=pltpu.VMEM),
            weights_spec(width),
            weights_spec(width),
        ]
        + [weights_spec(2 * width)] * 3,
        out_specs=pl.BlockSpec(memory_space=pltpu.VMEM),
        near=(0,),
    )
    gathered = exchange(hidden, TP)
    results = call(down_kernel, pltpu.VMEM((slots, columns), BF16), (gathered, down_local), near=(0,))
    back = exchange(results.reshape(ep, 32, columns), EP).reshape(slots, columns)

    along_x = [heads[0]]
    for k in (1, 2, 3):
        along_x.append(from_next(heads[k % 2], "x", -k))
    along_x = jnp.stack(along_x)
    head_rows = [along_x]
    for k in (1, 2, 3):
        head_rows.append(from_next(along_x, "y", k))
    half = tp // 2
    steps = 2
    pieces = half // steps
    weight_block = pl.BlockSpec((pieces * dv, columns), lambda i: (i, 0))
    projected = call(
        mix_kernel,
        [sds((block, columns), BF16)] * 2,
        (at, *head_rows, mix_weight.reshape(2, half, dv, columns), mix_far, mix_swap),
        scratch=[pltpu.VMEM((2, block, columns), F32), pltpu.VMEM((tp, block, dv), BF16)],
        grid=(steps,),
        in_specs=[pl.BlockSpec(memory_space=pltpu.SMEM)]
        + [pl.BlockSpec(memory_space=pltpu.VMEM)] * 4
        + [pl.BlockSpec((2, pieces, dv, columns), lambda i: (0, i, 0, 0))]
        + [weight_block] * 2,
        out_specs=[pl.BlockSpec((block, columns), lambda i: (0, 0))] * 2,
        near=(1, 2, 3, 4),
    )
    from_pair = swapped(projected[1], "x")
    mixer_out = call(
        assemble_kernel, sds((rows_a, columns), BF16), (at, projected[0], from_pair), near=(2,)
    )

    share = [pltpu.VMEM((tokens, slots), BF16)] * 2
    plan = call(plan_kernel, share, (routes, route_weight))
    expert_out = call(collect_kernel, sds((tokens, columns), BF16), (*plan, back), near=(0, 1, 2))
    return (mixer_out, expert_out)


def solution(mesh):
    split = Mesh(mesh.devices.reshape(16, 2, 4, 4), (*EP, *TP))
    in_specs = (
        P(EP, TP),
        P(EP, TP),
        P(EP, TP),
        P(TP, EP),
        P(TP, EP),
        P(EP, TP),
        P(TP),
        P(None, TP),
        P(EP, TP),
        P(EP, None),
        P(EP, None),
        P(EP, TP, None),
        P(EP, TP, None),
        P(EP, None, TP),
    )
    out_specs = (P(EP, TP), P(EP, TP))

    return jax.shard_map(body, mesh=split, in_specs=in_specs, out_specs=out_specs, check_vma=False)
```

```python
import functools

import jax
import jax.numpy as jnp
from jax import lax
from jax.experimental import pallas as pl
from jax.experimental.pallas import tpu as pltpu
from jax.sharding import Mesh
from jax.sharding import PartitionSpec as P


EP = ("z", "c")
TP = ("y", "x")
EPSILON = 1e-06
LOG_FLOOR = -1e30
MASKED = -1e38
HIGHEST = lax.Precision.HIGHEST
F32 = jnp.float32
BF16 = jnp.bfloat16


def dot(a, b):
    return jnp.dot(a, b, preferred_element_type=F32)


def dot_t(a, b):
    return lax.dot_general(a, b, (((1,), (1,)), ((), ())), preferred_element_type=F32)


def iota(shape, dim):
    return lax.broadcasted_iota(jnp.int32, shape, dim)


def call(kernel, out, args, scratch=(), grid=None, in_specs=None, out_specs=None, near=()):
    args = [
        pltpu.with_memory_space_constraint(a, pltpu.VMEM) if i in near else a
        for i, a in enumerate(args)
    ]
    vmem = pl.BlockSpec(memory_space=pltpu.VMEM)
    smem = pl.BlockSpec(memory_space=pltpu.SMEM)
    if in_specs is None:
        in_specs = [smem if a.dtype == jnp.int32 and a.ndim == 1 else vmem for a in args]
    kw = {} if grid is None else {"grid": grid}
    if out_specs is None:
        out_specs = jax.tree.map(lambda _: vmem, out)
    return pl.pallas_call(
        kernel,
        out_shape=out,
        in_specs=in_specs,
        out_specs=out_specs,
        scratch_shapes=list(scratch),
        compiler_params=pltpu.CompilerParams(vmem_limit_bytes=57 << 20),
        **kw,
    )(*args)


def log_sigmoid(f):
    return jnp.minimum(f, 0.0) - jnp.log1p(jnp.exp(-jnp.abs(f)))


def cumulative_forms(forget_row):
    n = forget_row.shape[1]
    logs = jnp.broadcast_to(log_sigmoid(forget_row), (n, n))
    at_row, at_col = iota((n, n), 0), iota((n, n), 1)
    column = jnp.sum(jnp.where(at_col <= at_row, logs, 0.0), axis=1, keepdims=True)
    own = jnp.sum(jnp.where(at_col == at_row, logs, 0.0), axis=1, keepdims=True)
    row = jnp.sum(jnp.where(at_row <= at_col, own, 0.0), axis=0, keepdims=True)
    return column, row


def summary_kernel(k_ref, v_ref, in_ref, forget_ref, out_ref):
    n = k_ref.shape[0]
    dk = k_ref.shape[1]
    column, _ = cumulative_forms(forget_ref[...])
    diagonal = iota((n, n), 0) == iota((n, n), 1)
    log_in = jnp.sum(
        jnp.where(diagonal, jnp.broadcast_to(in_ref[...], (n, n)), 0.0), axis=1, keepdims=True
    )
    total = column[n - 1 :, :]
    weight_log = total - column + log_in
    top = jnp.max(weight_log, axis=0, keepdims=True)
    weighted = k_ref[...].astype(F32) * jnp.exp(weight_log - top)
    memory = lax.dot_general(
        weighted.astype(BF16), v_ref[...], (((0,), (0,)), ((), ())), preferred_element_type=F32
    )
    normal = jnp.sum(weighted, axis=0, keepdims=True)
    width = out_ref.shape[1]
    out_ref[0:dk, :] = memory
    out_ref[dk : dk + 1, 0:dk] = normal
    out_ref[dk : dk + 1, dk:] = normal
    out_ref[dk + 1 : dk + 2, :] = jnp.broadcast_to(total, (1, width))
    out_ref[dk + 2 : dk + 3, :] = jnp.broadcast_to(top, (1, width))
    out_ref[dk + 3 :, :] = jnp.zeros((out_ref.shape[0] - dk - 3, width), F32)


def parts_of(x, dk):
    return x[0:dk, :], x[dk : dk + 1, :], x[dk + 1 : dk + 2, :], x[dk + 2 : dk + 3, :]


def fold(first, second):
    memory_1, normal_1, decay_1, max_1 = first
    memory_2, normal_2, decay_2, max_2 = second
    top = jnp.maximum(decay_2 + max_1, max_2)
    keep_1 = jnp.exp(decay_2 + max_1 - top)
    keep_2 = jnp.exp(max_2 - top)
    return (
        keep_1 * memory_1 + keep_2 * memory_2,
        keep_1 * normal_1 + keep_2 * normal_2,
        decay_1 + decay_2,
        top,
    )


def split3(x):
    high = x.astype(BF16)
    rest = x - high.astype(F32)
    middle = rest.astype(BF16)
    low = (rest - middle.astype(F32)).astype(BF16)
    return high, middle, low


def pack(out_ref, memory, normal, decay, top):
    dk, width = memory.shape
    out_ref[0:dk, :] = memory.astype(BF16)
    rows = []
    for value in (normal, decay, top):
        rows += [part.astype(F32) for part in split3(value)]
    rows.append(jnp.zeros((out_ref.shape[0] - dk - len(rows), width), F32))
    out_ref[dk:, :] = jnp.concatenate(rows, axis=0).astype(BF16)


def unpack(item, dk):
    item = item.astype(F32)
    rows = [
        item[dk + i : dk + i + 1] + item[dk + i + 1 : dk + i + 2] + item[dk + i + 2 : dk + i + 3]
        for i in (0, 3, 6)
    ]
    return (item[0:dk], *rows)


def first_state(dk, width):
    return (
        jnp.zeros((dk, width), F32),
        jnp.zeros((1, width), F32),
        jnp.zeros((1, width), F32),
        jnp.full((1, width), LOG_FLOOR, F32),
    )


def store_state(out_ref, state):
    memory, normal, decay, top = state
    dk, width = memory.shape
    out_ref[0:dk, :] = memory
    out_ref[dk:, :] = jnp.concatenate(
        [normal, decay, top, jnp.zeros((out_ref.shape[0] - dk - 3, width), F32)], axis=0
    )


def chip_kernel(at_ref, mine_ref, other_ref, total_ref, packed_ref):
    dk = 128
    south = at_ref[0] == 0
    mine, other = mine_ref[...], other_ref[...]
    first = parts_of(jnp.where(south, mine, other), dk)
    second = parts_of(jnp.where(south, other, mine), dk)
    total = fold(first, second)
    half = mine.shape[1] // 2
    total = [jnp.where(south, v[:, :half], v[:, half:]) for v in total]
    store_state(total_ref, total)
    pack(packed_ref, *total)


def step_kernel(reach, first, last, at_ref, came_ref, *refs):
    dk = 128
    valid = at_ref[1] >= reach
    came = unpack(came_ref[...], dk)
    if first:
        before = first_state(dk, came_ref.shape[1])
    else:
        before, refs = parts_of(refs[0][...], dk), refs[1:]
    joined = fold(came, before)
    if not last:
        total = parts_of(refs[0][...], dk)
        more = fold(came, total)
        total = [jnp.where(valid, new, old) for new, old in zip(more, total)]
        store_state(refs[1], total)
        pack(refs[3], *total)
    store_state(refs[0 if last else 2], [jnp.where(valid, n, o) for n, o in zip(joined, before)])


def output_kernel(
    at_ref, q_ref, k_ref, v_ref, in_ref, forget_ref, gate_ref, gain_ref,
    prior_ref, prior_other_ref, other_ref, out_ref,
):
    n, dk = q_ref.shape
    scale = dk ** (-0.5)
    south = at_ref[0] == 0
    column, row = cumulative_forms(forget_ref[...])
    left = jnp.where(south, prior_ref[...], prior_other_ref[...])
    right = jnp.where(south, prior_other_ref[...], prior_ref[...])
    before = parts_of(jnp.concatenate([left, right], axis=1), dk)
    joined = fold(before, parts_of(other_ref[...], dk))
    memory, normal, _, top_before = [jnp.where(south, b, j) for b, j in zip(before, joined)]
    normal = normal[:, :dk]
    top_before = top_before[:, 0:1]
    log_in = in_ref[...]
    step = n // 4
    for start in range(0, n, step):
        rows, seen = slice(start, start + step), start + step
        q = q_ref[rows, :]
        at = column[rows, :]
        causal = iota((step, seen), 1) <= iota((step, seen), 0) + start
        log_decay = jnp.where(causal, at - row[:, :seen] + log_in[:, :seen], MASKED)
        log_inter = at + top_before
        top = jnp.maximum(log_inter, jnp.max(log_decay, axis=1, keepdims=True))
        scores = dot_t(q, k_ref[0:seen, :]) * scale * jnp.exp(log_decay - top)
        carried = jnp.exp(log_inter - top) * scale
        wide = q.astype(F32)
        numerator = carried * jnp.dot(
            wide, memory, precision=HIGHEST, preferred_element_type=F32
        ) + dot(scores.astype(BF16), v_ref[0:seen, :])
        denominator = carried * jnp.sum(wide * normal, axis=1, keepdims=True) + jnp.sum(
            scores, axis=1, keepdims=True
        )
        values = numerator / jnp.maximum(jnp.abs(denominator), jnp.exp(-top))
        values = values * lax.rsqrt(jnp.mean(values * values, axis=1, keepdims=True) + EPSILON)
        gate = gate_ref[rows, :].astype(F32)
        values = values * gain_ref[...] * (1.0 / (1.0 + jnp.exp(-gate)))
        side, inner = divmod(start, n // 2)
        out_ref[lax.rem(at_ref[2] + side, 2), inner : inner + step, :] = values.astype(BF16)


def dispatch_kernel(routes_ref, x_ref, out_ref):
    tokens = x_ref.shape[0]
    slots = out_ref.shape[0]
    experts, room = 32, slots // 32
    expert = iota((experts, tokens), 0)
    named = jnp.zeros((experts, tokens), F32)
    for r in range(routes_ref.shape[0]):
        named = named + (routes_ref[r : r + 1, :] == expert).astype(F32)
    earlier = (iota((tokens, tokens), 0) < iota((tokens, tokens), 1)).astype(F32).astype(BF16)
    place = dot(named.astype(BF16), earlier)
    key = jnp.where(named > 0.5, place, -1.0).astype(BF16)
    slot = iota((slots, experts), 0)
    spread = (slot // room == iota((slots, experts), 1)).astype(F32).astype(BF16)
    wanted = (iota((slots, tokens), 0) % room).astype(F32)
    chosen = (dot(spread, key) == wanted).astype(F32).astype(BF16)
    out_ref[...] = dot(chosen, x_ref[...]).astype(BF16)


def plan_kernel(routes_ref, weight_ref, high_ref, low_ref):
    tokens, slots = high_ref.shape
    experts, room = 32, slots // 32
    expert = iota((tokens, experts), 1)
    named = jnp.zeros((tokens, experts), F32)
    weight = jnp.zeros((tokens, experts), F32)
    for r in range(routes_ref.shape[1]):
        hit = routes_ref[:, r : r + 1] == expert
        named = named + hit.astype(F32)
        weight = weight + jnp.where(hit, weight_ref[:, r : r + 1], 0.0)
    earlier = (iota((tokens, tokens), 1) < iota((tokens, tokens), 0)).astype(F32).astype(BF16)
    place = dot(earlier, named.astype(BF16))
    key = jnp.where(named > 0.5, place, -1.0).astype(BF16)
    slot = iota((experts, slots), 1)
    spread = (slot // room == iota((experts, slots), 0)).astype(F32).astype(BF16)
    wanted = (iota((tokens, slots), 1) % room).astype(F32)
    chosen = dot(key, spread) == wanted
    high, low, _ = split3(weight)
    high_ref[...] = jnp.where(chosen, dot(high, spread), 0.0).astype(BF16)
    low_ref[...] = jnp.where(chosen, dot(low, spread), 0.0).astype(BF16)


def collect_kernel(high_ref, low_ref, back_ref, out_ref):
    back = back_ref[...]
    out_ref[...] = (dot(high_ref[...], back) + dot(low_ref[...], back)).astype(BF16)


def hidden_kernel(
    x_ref, g0_ref, g1_ref, g2_ref, g3_ref, u0_ref, u1_ref, u2_ref, u3_ref,
    out_ref, gate_acc, up_acc, squares,
):
    step = pl.program_id(0)
    _, _, columns = x_ref.shape
    senders = g0_ref.shape[1] // columns
    pieces = [x_ref[step * senders + i] for i in range(senders)]
    x = jnp.concatenate(pieces, axis=1)
    gate = jnp.concatenate([w[...] for w in (g0_ref, g1_ref, g2_ref, g3_ref)], axis=0)
    up = jnp.concatenate([w[...] for w in (u0_ref, u1_ref, u2_ref, u3_ref)], axis=0)
    gate_part, up_part = dot_t(x, gate), dot_t(x, up)
    square = jnp.zeros(squares.shape, F32)
    for piece in pieces:
        wide = piece.astype(F32)
        square = square + wide * wide

    @pl.when(step == 0)
    def _():
        gate_acc[...] = gate_part
        up_acc[...] = up_part
        squares[...] = square

    @pl.when(step > 0)
    def _():
        gate_acc[...] += gate_part
        up_acc[...] += up_part
        squares[...] += square

    @pl.when(step == pl.num_programs(0) - 1)
    def _():
        total = jnp.sum(squares[...], axis=1, keepdims=True)
        inverse = lax.rsqrt(total * (1.0 / (columns * out_ref.shape[0])) + EPSILON)
        gate = gate_acc[...] * inverse
        hidden = gate * (1.0 / (1.0 + jnp.exp(-gate))) * (up_acc[...] * inverse)
        hidden = hidden.astype(BF16)
        for copy in range(out_ref.shape[0]):
            out_ref[copy] = hidden


def down_kernel(h_ref, w_ref, out_ref):
    part = h_ref.shape[2] // 4
    rows = h_ref.shape[1]
    for ys in range(4):
        total = jnp.zeros((rows, w_ref.shape[1]), F32)
        for xs in range(4):
            at = [(((ys + j) % 4) * 4 + xs) * part for j in range(4)]
            weight = jnp.concatenate([w_ref[a : a + part, :] for a in at], axis=0)
            total = total + dot(h_ref[ys * 4 + xs], weight)
        out_ref[ys * rows : (ys + 1) * rows, :] = total.astype(BF16)


def mix_kernel(
    at_ref, h0_ref, h1_ref, h2_ref, h3_ref, near_ref, a_ref, b_ref, o0_ref, o1_ref, acc, heads
):
    step = pl.program_id(0)
    half = heads.shape[0] // 2
    c, x, y = at_ref[0], at_ref[2], at_ref[3]

    @pl.when(step == 0)
    def _():
        acc[...] = jnp.zeros_like(acc)
        for ky, ref in enumerate((h0_ref, h1_ref, h2_ref, h3_ref)):
            for kx in range(4):
                heads[lax.rem(y + ky, 4) * 4 + lax.rem(x + 4 - kx, 4)] = ref[kx]

    pieces = near_ref.shape[1]
    width = near_ref.shape[2]
    own = jnp.zeros(acc.shape[1:], F32)
    pair = jnp.zeros(acc.shape[1:], F32)
    for i in range(pieces):
        k = step * pieces + i
        rows = slice(i * width, (i + 1) * width)
        own = own + dot(heads[k], near_ref[0, i]) + dot(heads[half + k], near_ref[1, i])
        pair = pair + dot(heads[c * half + k], a_ref[rows, :])
        pair = pair + dot(heads[(1 - c) * half + k], b_ref[rows, :])
    acc[0] += own
    acc[1] += pair

    @pl.when(step == pl.num_programs(0) - 1)
    def _():
        o0_ref[...] = acc[0].astype(BF16)
        o1_ref[...] = acc[1].astype(BF16)


def assemble_kernel(at_ref, own_ref, pair_ref, out_ref):
    block = own_ref.shape[0]
    side = lax.rem(at_ref[2], 2)
    out_ref[pl.ds(pl.multiple_of(side * block, block), block), :] = own_ref[...]
    out_ref[pl.ds(pl.multiple_of((1 - side) * block, block), block), :] = pair_ref[...]


def from_next(x, axis, k):
    n = lax.axis_size(axis)
    return lax.ppermute(x, axis, [((i + k) % n, i) for i in range(n)])


def swapped(x, axis):
    n = lax.axis_size(axis)
    return lax.ppermute(x, axis, [(i ^ 1, i) for i in range(n)])


def exchange(x, axis):
    return lax.all_to_all(x, axis, split_axis=0, concat_axis=0, tiled=True)


def body(
    query_rows,
    key_rows,
    value_rows,
    in_gate,
    forget_gate,
    out_gate,
    head_gain,
    mix_weight,
    expert_input,
    routes,
    route_weight,
    gate_weight,
    up_weight,
    down_weight,
):
    sds = jax.ShapeDtypeStruct
    rows_a, dk = query_rows.shape
    dv = value_rows.shape[1]
    tokens, columns = expert_input.shape
    ep, tp = lax.axis_size(EP), lax.axis_size(TP)
    gate_local, up_local, down_local = gate_weight[0], up_weight[0], down_weight[0]
    width = gate_local.shape[0]
    slots = ep * 32
    at = jnp.stack(
        [lax.axis_index(axis) for axis in ("c", "z", "x", "y")]
    ).astype(jnp.int32)

    table = call(dispatch_kernel, pltpu.VMEM((slots, columns), BF16), (routes.T, expert_input))
    arrived = exchange(table.reshape(ep, 32, columns), EP)
    arrived = arrived.reshape(4, 1, slots // 4, columns)

    own_half = lax.dynamic_slice_in_dim(
        mix_weight, at[0] * (mix_weight.shape[0] // 2), mix_weight.shape[0] // 2, 0
    )
    gate_1 = from_next(gate_local, "y", 1)
    up_3 = from_next(up_local, "y", 3)
    gate_3 = from_next(gate_local, "y", 3)
    up_1 = from_next(up_local, "y", 1)
    gate_2 = from_next(gate_1, "y", 1)
    up_2 = from_next(up_3, "y", 3)
    mix_far = swapped(own_half, "x")
    mix_swap = swapped(mix_far, "c")

    mine = call(
        summary_kernel, sds((dk + 8, dv), F32), (key_rows, value_rows, in_gate, forget_gate)
    )
    other = swapped(mine, "c")
    state, lines = sds((dk + 8, dv // 2), F32), sds((dk + 16, dv // 2), BF16)
    total, packed = call(chip_kernel, [state, lines], (at, mine, other), near=(2,))
    before, reach, chips = (), 1, lax.axis_size("z")
    while reach < chips:
        came = lax.ppermute(packed, "z", [(i, i + reach) for i in range(chips - reach)])
        last = 2 * reach == chips
        result = call(
            functools.partial(step_kernel, reach, reach == 1, last),
            [state] if last else [state, state, lines],
            (at, came, *before) + (() if last else (total,)),
            near=(1,),
        )
        if last:
            (prior,) = result
        else:
            total, before, packed = result[0], result[1:2], result[2]
        reach *= 2
    prior_other = swapped(prior, "c")
    block = rows_a // 2
    heads = call(
        output_kernel,
        sds((2, block, dv), BF16),
        (
            at, query_rows, key_rows, value_rows, in_gate, forget_gate, out_gate,
            head_gain[None, :], prior, prior_other, other,
        ),
        near=(9, 10),
    )

    sent = jnp.broadcast_to(arrived, (4, 4, slots // 4, columns)).reshape(tp, slots // 4, columns)
    rows = exchange(sent, TP)
    grid = 2
    per = tp // grid
    weights_spec = lambda r: pl.BlockSpec((r, per * columns), lambda i: (0, i))
    hidden = call(
        hidden_kernel,
        sds((tp, slots // 4, 4 * width), BF16),
        (rows, gate_local, gate_1, gate_2, gate_3, up_local, up_1, up_2, up_3),
        scratch=[pltpu.VMEM((slots // 4, 4 * width), F32)] * 2
        + [pltpu.VMEM((slots // 4, columns), F32)],
        grid=(grid,),
        in_specs=[
            pl.BlockSpec(memory_space=pltpu.VMEM),
        ]
        + [weights_spec(width)] * 8,
        out_specs=pl.BlockSpec(memory_space=pltpu.VMEM),
        near=(0,),
    )
    gathered = exchange(hidden, TP)
    results = call(down_kernel, pltpu.VMEM((slots, columns), BF16), (gathered, down_local), near=(0,))
    back = exchange(results.reshape(ep, 32, columns), EP).reshape(slots, columns)

    along_x = [heads[0]]
    for k in (1, 2, 3):
        along_x.append(from_next(heads[k % 2], "x", -k))
    along_x = jnp.stack(along_x)
    head_rows = [along_x]
    for k in (1, 2, 3):
        head_rows.append(from_next(along_x, "y", k))
    half = tp // 2
    steps = 2
    pieces = half // steps
    weight_block = pl.BlockSpec((pieces * dv, columns), lambda i: (i, 0))
    projected = call(
        mix_kernel,
        [sds((block, columns), BF16)] * 2,
        (at, *head_rows, mix_weight.reshape(2, half, dv, columns), mix_far, mix_swap),
        scratch=[pltpu.VMEM((2, block, columns), F32), pltpu.VMEM((tp, block, dv), BF16)],
        grid=(steps,),
        in_specs=[pl.BlockSpec(memory_space=pltpu.SMEM)]
        + [pl.BlockSpec(memory_space=pltpu.VMEM)] * 4
        + [pl.BlockSpec((2, pieces, dv, columns), lambda i: (0, i, 0, 0))]
        + [weight_block] * 2,
        out_specs=[pl.BlockSpec((block, columns), lambda i: (0, 0))] * 2,
        near=(1, 2, 3, 4),
    )
    from_pair = swapped(projected[1], "x")
    mixer_out = call(
        assemble_kernel, sds((rows_a, columns), BF16), (at, projected[0], from_pair), near=(2,)
    )

    share = [pltpu.VMEM((tokens, slots), BF16)] * 2
    plan = call(plan_kernel, share, (routes, route_weight))
    expert_out = call(collect_kernel, sds((tokens, columns), BF16), (*plan, back), near=(0, 1, 2))
    return (mixer_out, expert_out)


def solution(mesh):
    split = Mesh(mesh.devices.reshape(16, 2, 4, 4), (*EP, *TP))
    in_specs = (
        P(EP, TP),
        P(EP, TP),
        P(EP, TP),
        P(TP, EP),
        P(TP, EP),
        P(EP, TP),
        P(TP),
        P(None, TP),
        P(EP, TP),
        P(EP, None),
        P(EP, None),
        P(EP, TP, None),
        P(EP, TP, None),
        P(EP, None, TP),
    )
    out_specs = (P(EP, TP), P(EP, TP))

    return jax.shard_map(body, mesh=split, in_specs=in_specs, out_specs=out_specs, check_vma=False)
```

```python
import jax
import jax.numpy as jnp
from jax import lax
from jax.experimental import pallas as pl
from jax.experimental.pallas import tpu as pltpu
from jax.sharding import Mesh
from jax.sharding import PartitionSpec as P


EP = ("z", "c")
TP = ("y", "x")
EPSILON = 1e-06
LOG_FLOOR = -1e30
MASKED = -1e38
HIGHEST = lax.Precision.HIGHEST
F32 = jnp.float32
BF16 = jnp.bfloat16


def dot(a, b):
    return jnp.dot(a, b, preferred_element_type=F32)


def dot_t(a, b):
    return lax.dot_general(a, b, (((1,), (1,)), ((), ())), preferred_element_type=F32)


def iota(shape, dim):
    return lax.broadcasted_iota(jnp.int32, shape, dim)


def call(kernel, out, args, scratch=(), grid=None, in_specs=None, out_specs=None, near=()):
    args = [
        pltpu.with_memory_space_constraint(a, pltpu.VMEM) if i in near else a
        for i, a in enumerate(args)
    ]
    vmem = pl.BlockSpec(memory_space=pltpu.VMEM)
    smem = pl.BlockSpec(memory_space=pltpu.SMEM)
    if in_specs is None:
        in_specs = [smem if a.dtype == jnp.int32 and a.ndim == 1 else vmem for a in args]
    kw = {} if grid is None else {"grid": grid}
    if out_specs is None:
        out_specs = jax.tree.map(lambda _: vmem, out)
    return pl.pallas_call(
        kernel,
        out_shape=out,
        in_specs=in_specs,
        out_specs=out_specs,
        scratch_shapes=list(scratch),
        compiler_params=pltpu.CompilerParams(vmem_limit_bytes=57 << 20),
        **kw,
    )(*args)


def log_sigmoid(f):
    return jnp.minimum(f, 0.0) - jnp.log1p(jnp.exp(-jnp.abs(f)))


def cumulative_forms(forget_row):
    n = forget_row.shape[1]
    logs = jnp.broadcast_to(log_sigmoid(forget_row), (n, n))
    at_row, at_col = iota((n, n), 0), iota((n, n), 1)
    column = jnp.sum(jnp.where(at_col <= at_row, logs, 0.0), axis=1, keepdims=True)
    own = jnp.sum(jnp.where(at_col == at_row, logs, 0.0), axis=1, keepdims=True)
    row = jnp.sum(jnp.where(at_row <= at_col, own, 0.0), axis=0, keepdims=True)
    return column, row


def summary_kernel(k_ref, v_ref, in_ref, forget_ref, out_ref):
    n = k_ref.shape[0]
    dk = k_ref.shape[1]
    column, _ = cumulative_forms(forget_ref[...])
    diagonal = iota((n, n), 0) == iota((n, n), 1)
    log_in = jnp.sum(
        jnp.where(diagonal, jnp.broadcast_to(in_ref[...], (n, n)), 0.0), axis=1, keepdims=True
    )
    total = column[n - 1 :, :]
    weight_log = total - column + log_in
    top = jnp.max(weight_log, axis=0, keepdims=True)
    weighted = k_ref[...].astype(F32) * jnp.exp(weight_log - top)
    memory = lax.dot_general(
        weighted.astype(BF16), v_ref[...], (((0,), (0,)), ((), ())), preferred_element_type=F32
    )
    normal = jnp.sum(weighted, axis=0, keepdims=True)
    width = out_ref.shape[1]
    normal = jnp.concatenate([normal] * (width // dk), axis=1)
    pack(
        out_ref,
        memory,
        normal,
        jnp.broadcast_to(total, (1, width)),
        jnp.broadcast_to(top, (1, width)),
    )


def fold(first, second):
    memory_1, normal_1, decay_1, max_1 = first
    memory_2, normal_2, decay_2, max_2 = second
    top = jnp.maximum(decay_2 + max_1, max_2)
    keep_1 = jnp.exp(decay_2 + max_1 - top)
    keep_2 = jnp.exp(max_2 - top)
    return (
        keep_1 * memory_1 + keep_2 * memory_2,
        keep_1 * normal_1 + keep_2 * normal_2,
        decay_1 + decay_2,
        top,
    )


def split3(x):
    high = x.astype(BF16)
    rest = x - high.astype(F32)
    middle = rest.astype(BF16)
    low = (rest - middle.astype(F32)).astype(BF16)
    return high, middle, low


def pack(out_ref, memory, normal, decay, top):
    dk, width = memory.shape
    out_ref[0:dk, :] = memory.astype(BF16)
    rows = []
    for value in (normal, decay, top):
        rows += [part.astype(F32) for part in split3(value)]
    rows.append(jnp.zeros((out_ref.shape[0] - dk - len(rows), width), F32))
    out_ref[dk:, :] = jnp.concatenate(rows, axis=0).astype(BF16)


def unpack(item, dk):
    item = item.astype(F32)
    rows = [
        item[dk + i : dk + i + 1] + item[dk + i + 1 : dk + i + 2] + item[dk + i + 2 : dk + i + 3]
        for i in (0, 3, 6)
    ]
    return (item[0:dk], *rows)


def first_state(dk, width):
    return (
        jnp.zeros((dk, width), F32),
        jnp.zeros((1, width), F32),
        jnp.zeros((1, width), F32),
        jnp.full((1, width), LOG_FLOOR, F32),
    )


def output_kernel(
    at_ref, q_ref, k_ref, v_ref, in_ref, forget_ref, gate_ref, gain_ref, all_ref, out_ref
):
    n, dk = q_ref.shape
    scale = dk ** (-0.5)
    column, row = cumulative_forms(forget_ref[...])
    memory, normal, _, top_before = lax.fori_loop(
        0,
        at_ref[0],
        lambda k, state: fold(state, unpack(all_ref[k], dk)),
        first_state(dk, all_ref.shape[2]),
    )
    normal = normal[:, :dk]
    top_before = top_before[:, 0:1]
    log_in = in_ref[...]
    step = n // 4
    for start in range(0, n, step):
        rows, seen = slice(start, start + step), start + step
        q = q_ref[rows, :]
        at = column[rows, :]
        causal = iota((step, seen), 1) <= iota((step, seen), 0) + start
        log_decay = jnp.where(causal, at - row[:, :seen] + log_in[:, :seen], MASKED)
        log_inter = at + top_before
        top = jnp.maximum(log_inter, jnp.max(log_decay, axis=1, keepdims=True))
        scores = dot_t(q, k_ref[0:seen, :]) * scale * jnp.exp(log_decay - top)
        carried = jnp.exp(log_inter - top) * scale
        wide = q.astype(F32)
        numerator = carried * jnp.dot(
            wide, memory, precision=HIGHEST, preferred_element_type=F32
        ) + dot(scores.astype(BF16), v_ref[0:seen, :])
        denominator = carried * jnp.sum(wide * normal, axis=1, keepdims=True) + jnp.sum(
            scores, axis=1, keepdims=True
        )
        values = numerator / jnp.maximum(jnp.abs(denominator), jnp.exp(-top))
        values = values * lax.rsqrt(jnp.mean(values * values, axis=1, keepdims=True) + EPSILON)
        gate = gate_ref[rows, :].astype(F32)
        values = values * gain_ref[...] * (1.0 / (1.0 + jnp.exp(-gate)))
        out_ref[rows, :] = values.astype(BF16)


def dispatch_kernel(routes_ref, x_ref, out_ref):
    tokens = x_ref.shape[0]
    slots = out_ref.shape[0]
    experts, room = 32, slots // 32
    expert = iota((experts, tokens), 0)
    named = jnp.zeros((experts, tokens), F32)
    for r in range(routes_ref.shape[0]):
        named = named + (routes_ref[r : r + 1, :] == expert).astype(F32)
    earlier = (iota((tokens, tokens), 0) < iota((tokens, tokens), 1)).astype(F32).astype(BF16)
    place = dot(named.astype(BF16), earlier)
    key = jnp.where(named > 0.5, place, -1.0).astype(BF16)
    slot = iota((slots, experts), 0)
    spread = (slot // room == iota((slots, experts), 1)).astype(F32).astype(BF16)
    wanted = (iota((slots, tokens), 0) % room).astype(F32)
    chosen = (dot(spread, key) == wanted).astype(F32).astype(BF16)
    out_ref[...] = dot(chosen, x_ref[...]).astype(BF16)


def plan_kernel(routes_ref, weight_ref, high_ref, low_ref):
    tokens, slots = high_ref.shape
    experts, room = 32, slots // 32
    expert = iota((tokens, experts), 1)
    named = jnp.zeros((tokens, experts), F32)
    weight = jnp.zeros((tokens, experts), F32)
    for r in range(routes_ref.shape[1]):
        hit = routes_ref[:, r : r + 1] == expert
        named = named + hit.astype(F32)
        weight = weight + jnp.where(hit, weight_ref[:, r : r + 1], 0.0)
    earlier = (iota((tokens, tokens), 1) < iota((tokens, tokens), 0)).astype(F32).astype(BF16)
    place = dot(earlier, named.astype(BF16))
    key = jnp.where(named > 0.5, place, -1.0).astype(BF16)
    slot = iota((experts, slots), 1)
    spread = (slot // room == iota((experts, slots), 0)).astype(F32).astype(BF16)
    wanted = (iota((tokens, slots), 1) % room).astype(F32)
    chosen = dot(key, spread) == wanted
    high, low, _ = split3(weight)
    high_ref[...] = jnp.where(chosen, dot(high, spread), 0.0).astype(BF16)
    low_ref[...] = jnp.where(chosen, dot(low, spread), 0.0).astype(BF16)


def collect_kernel(high_ref, low_ref, back_ref, out_ref):
    back = back_ref[...]
    out_ref[...] = (dot(high_ref[...], back) + dot(low_ref[...], back)).astype(BF16)


def hidden_kernel(
    x_ref, g0_ref, g1_ref, g2_ref, g3_ref, u0_ref, u1_ref, u2_ref, u3_ref,
    out_ref, gate_acc, up_acc, squares,
):
    step = pl.program_id(0)
    _, _, columns = x_ref.shape
    senders = g0_ref.shape[1] // columns
    pieces = [x_ref[step * senders + i] for i in range(senders)]
    x = jnp.concatenate(pieces, axis=1)
    gate = jnp.concatenate([w[...] for w in (g0_ref, g1_ref, g2_ref, g3_ref)], axis=0)
    up = jnp.concatenate([w[...] for w in (u0_ref, u1_ref, u2_ref, u3_ref)], axis=0)
    gate_part, up_part = dot_t(x, gate), dot_t(x, up)
    square = jnp.zeros(squares.shape, F32)
    for piece in pieces:
        wide = piece.astype(F32)
        square = square + wide * wide

    @pl.when(step == 0)
    def _():
        gate_acc[...] = gate_part
        up_acc[...] = up_part
        squares[...] = square

    @pl.when(step > 0)
    def _():
        gate_acc[...] += gate_part
        up_acc[...] += up_part
        squares[...] += square

    @pl.when(step == pl.num_programs(0) - 1)
    def _():
        total = jnp.sum(squares[...], axis=1, keepdims=True)
        inverse = lax.rsqrt(total * (1.0 / (columns * out_ref.shape[0])) + EPSILON)
        gate = gate_acc[...] * inverse
        hidden = gate * (1.0 / (1.0 + jnp.exp(-gate))) * (up_acc[...] * inverse)
        hidden = hidden.astype(BF16)
        for copy in range(out_ref.shape[0]):
            out_ref[copy] = hidden


def down_kernel(h_ref, w_ref, out_ref):
    part = h_ref.shape[2] // 4
    rows = h_ref.shape[1]
    for ys in range(4):
        total = jnp.zeros((rows, w_ref.shape[1]), F32)
        for xs in range(4):
            at = [(((ys + j) % 4) * 4 + xs) * part for j in range(4)]
            weight = jnp.concatenate([w_ref[a : a + part, :] for a in at], axis=0)
            total = total + dot(h_ref[ys * 4 + xs], weight)
        out_ref[ys * rows : (ys + 1) * rows, :] = total.astype(BF16)


def mix_kernel(h_ref, w_ref, out_ref, acc):
    step = pl.program_id(0)
    width = h_ref.shape[2]
    total = jnp.zeros(acc.shape, F32)
    for i in range(h_ref.shape[0]):
        total = total + dot(h_ref[i], w_ref[i * width : (i + 1) * width, :])

    @pl.when(step == 0)
    def _():
        acc[...] = total

    @pl.when(step > 0)
    def _():
        acc[...] += total

    @pl.when(step == pl.num_programs(0) - 1)
    def _():
        out_ref[...] = acc[...].astype(BF16)


def from_next(x, axis, k):
    n = lax.axis_size(axis)
    return lax.ppermute(x, axis, [((i + k) % n, i) for i in range(n)])


def exchange(x, axis):
    return lax.all_to_all(x, axis, split_axis=0, concat_axis=0, tiled=True)


def body(
    query_rows,
    key_rows,
    value_rows,
    in_gate,
    forget_gate,
    out_gate,
    head_gain,
    mix_weight,
    expert_input,
    routes,
    route_weight,
    gate_weight,
    up_weight,
    down_weight,
):
    sds = jax.ShapeDtypeStruct
    rows_a, dk = query_rows.shape
    dv = value_rows.shape[1]
    tokens, columns = expert_input.shape
    ep, tp = lax.axis_size(EP), lax.axis_size(TP)
    gate_local, up_local, down_local = gate_weight[0], up_weight[0], down_weight[0]
    width = gate_local.shape[0]
    slots = ep * 32
    at = lax.axis_index(EP).astype(jnp.int32)[None]

    table = call(dispatch_kernel, pltpu.VMEM((slots, columns), BF16), (routes.T, expert_input))
    arrived = exchange(table.reshape(ep, 32, columns), EP)
    arrived = arrived.reshape(4, 1, slots // 4, columns)

    gate_1 = from_next(gate_local, "y", 1)
    up_3 = from_next(up_local, "y", 3)
    gate_3 = from_next(gate_local, "y", 3)
    up_1 = from_next(up_local, "y", 1)
    gate_2 = from_next(gate_1, "y", 1)
    up_2 = from_next(up_3, "y", 3)
    mine = call(
        summary_kernel, sds((dk + 16, dv), BF16), (key_rows, value_rows, in_gate, forget_gate)
    )
    states = lax.all_gather(mine, EP, axis=0)
    heads = call(
        output_kernel,
        sds((rows_a, dv), BF16),
        (
            at, query_rows, key_rows, value_rows, in_gate, forget_gate, out_gate,
            head_gain[None, :], states,
        ),
    )

    sent = jnp.broadcast_to(arrived, (4, 4, slots // 4, columns)).reshape(tp, slots // 4, columns)
    rows = exchange(sent, TP)
    grid = 2
    per = tp // grid
    weights_spec = lambda r: pl.BlockSpec((r, per * columns), lambda i: (0, i))
    hidden = call(
        hidden_kernel,
        sds((tp, slots // 4, 4 * width), BF16),
        (rows, gate_local, gate_1, gate_2, gate_3, up_local, up_1, up_2, up_3),
        scratch=[pltpu.VMEM((slots // 4, 4 * width), F32)] * 2
        + [pltpu.VMEM((slots // 4, columns), F32)],
        grid=(grid,),
        in_specs=[
            pl.BlockSpec(memory_space=pltpu.VMEM),
        ]
        + [weights_spec(width)] * 8,
        out_specs=pl.BlockSpec(memory_space=pltpu.VMEM),
        near=(0,),
    )
    gathered = exchange(hidden, TP)
    results = call(down_kernel, pltpu.VMEM((slots, columns), BF16), (gathered, down_local), near=(0,))
    back = exchange(results.reshape(ep, 32, columns), EP).reshape(slots, columns)

    all_heads = lax.all_gather(heads, TP, axis=0)
    steps = 2
    mixer_out = call(
        mix_kernel,
        sds((rows_a, columns), BF16),
        (all_heads, mix_weight),
        scratch=[pltpu.VMEM((rows_a, columns), F32)],
        grid=(steps,),
        in_specs=[
            pl.BlockSpec((tp // steps, rows_a, dv), lambda i: (i, 0, 0)),
            pl.BlockSpec((tp * dv // steps, columns), lambda i: (i, 0)),
        ],
        out_specs=pl.BlockSpec((rows_a, columns), lambda i: (0, 0)),
    )

    share = [pltpu.VMEM((tokens, slots), BF16)] * 2
    plan = call(plan_kernel, share, (routes, route_weight))
    expert_out = call(collect_kernel, sds((tokens, columns), BF16), (*plan, back), near=(0, 1, 2))
    return (mixer_out, expert_out)


def solution(mesh):
    split = Mesh(mesh.devices.reshape(16, 2, 4, 4), (*EP, *TP))
    in_specs = (
        P(EP, TP),
        P(EP, TP),
        P(EP, TP),
        P(TP, EP),
        P(TP, EP),
        P(EP, TP),
        P(TP),
        P(None, TP),
        P(EP, TP),
        P(EP, None),
        P(EP, None),
        P(EP, TP, None),
        P(EP, TP, None),
        P(EP, None, TP),
    )
    out_specs = (P(EP, TP), P(EP, TP))

    return jax.shard_map(body, mesh=split, in_specs=in_specs, out_specs=out_specs, check_vma=False)
```

```python
import jax
import jax.numpy as jnp
from jax import lax
from jax.experimental import pallas as pl
from jax.experimental.pallas import tpu as pltpu
from jax.sharding import Mesh
from jax.sharding import PartitionSpec as P


EP = ("z", "c")
TP = ("y", "x")
EPSILON = 1e-06
LOG_FLOOR = -1e30
MASKED = -1e38
HIGHEST = lax.Precision.HIGHEST
F32 = jnp.float32
BF16 = jnp.bfloat16


def dot(a, b):
    return jnp.dot(a, b, preferred_element_type=F32)


def dot_t(a, b):
    return lax.dot_general(a, b, (((1,), (1,)), ((), ())), preferred_element_type=F32)


def iota(shape, dim):
    return lax.broadcasted_iota(jnp.int32, shape, dim)


def call(kernel, out, args, scratch=(), grid=None, in_specs=None, out_specs=None, near=()):
    args = [
        pltpu.with_memory_space_constraint(a, pltpu.VMEM) if i in near else a
        for i, a in enumerate(args)
    ]
    vmem = pl.BlockSpec(memory_space=pltpu.VMEM)
    smem = pl.BlockSpec(memory_space=pltpu.SMEM)
    if in_specs is None:
        in_specs = [smem if a.dtype == jnp.int32 and a.ndim == 1 else vmem for a in args]
    kw = {} if grid is None else {"grid": grid}
    if out_specs is None:
        out_specs = jax.tree.map(lambda _: vmem, out)
    return pl.pallas_call(
        kernel,
        out_shape=out,
        in_specs=in_specs,
        out_specs=out_specs,
        scratch_shapes=list(scratch),
        compiler_params=pltpu.CompilerParams(vmem_limit_bytes=57 << 20),
        **kw,
    )(*args)


def log_sigmoid(f):
    return jnp.minimum(f, 0.0) - jnp.log1p(jnp.exp(-jnp.abs(f)))


def cumulative_forms(forget_row):
    n = forget_row.shape[1]
    logs = jnp.broadcast_to(log_sigmoid(forget_row), (n, n))
    at_row, at_col = iota((n, n), 0), iota((n, n), 1)
    column = jnp.sum(jnp.where(at_col <= at_row, logs, 0.0), axis=1, keepdims=True)
    own = jnp.sum(jnp.where(at_col == at_row, logs, 0.0), axis=1, keepdims=True)
    row = jnp.sum(jnp.where(at_row <= at_col, own, 0.0), axis=0, keepdims=True)
    return column, row


def summary_kernel(k_ref, v_ref, in_ref, forget_ref, out_ref):
    n = k_ref.shape[0]
    dk = k_ref.shape[1]
    column, _ = cumulative_forms(forget_ref[...])
    diagonal = iota((n, n), 0) == iota((n, n), 1)
    log_in = jnp.sum(
        jnp.where(diagonal, jnp.broadcast_to(in_ref[...], (n, n)), 0.0), axis=1, keepdims=True
    )
    total = column[n - 1 :, :]
    weight_log = total - column + log_in
    top = jnp.max(weight_log, axis=0, keepdims=True)
    weighted = k_ref[...].astype(F32) * jnp.exp(weight_log - top)
    memory = lax.dot_general(
        weighted.astype(BF16), v_ref[...], (((0,), (0,)), ((), ())), preferred_element_type=F32
    )
    normal = jnp.sum(weighted, axis=0, keepdims=True)
    width = out_ref.shape[1]
    out_ref[0:dk, :] = memory
    rows = [
        jnp.concatenate([normal] * (width // dk), axis=1),
        jnp.broadcast_to(total, (1, width)),
        jnp.broadcast_to(top, (1, width)),
        jnp.zeros((out_ref.shape[0] - dk - 3, width), F32),
    ]
    out_ref[dk:, :] = jnp.concatenate(rows, axis=0)


def parts_of(x, dk):
    return x[0:dk, :], x[dk : dk + 1, :], x[dk + 1 : dk + 2, :], x[dk + 2 : dk + 3, :]


def fold(first, second):
    memory_1, normal_1, decay_1, max_1 = first
    memory_2, normal_2, decay_2, max_2 = second
    top = jnp.maximum(decay_2 + max_1, max_2)
    keep_1 = jnp.exp(decay_2 + max_1 - top)
    keep_2 = jnp.exp(max_2 - top)
    return (
        keep_1 * memory_1 + keep_2 * memory_2,
        keep_1 * normal_1 + keep_2 * normal_2,
        decay_1 + decay_2,
        top,
    )


def split3(x):
    high = x.astype(BF16)
    rest = x - high.astype(F32)
    middle = rest.astype(BF16)
    low = (rest - middle.astype(F32)).astype(BF16)
    return high, middle, low


def pack(out_ref, memory, normal, decay, top):
    dk, width = memory.shape
    out_ref[0:dk, :] = memory.astype(BF16)
    rows = []
    for value in (normal, decay, top):
        rows += [part.astype(F32) for part in split3(value)]
    rows.append(jnp.zeros((out_ref.shape[0] - dk - len(rows), width), F32))
    out_ref[dk:, :] = jnp.concatenate(rows, axis=0).astype(BF16)


def unpack(item, dk):
    item = item.astype(F32)
    rows = [
        item[dk + i : dk + i + 1] + item[dk + i + 1 : dk + i + 2] + item[dk + i + 2 : dk + i + 3]
        for i in (0, 3, 6)
    ]
    return (item[0:dk], *rows)


def first_state(dk, width):
    return (
        jnp.zeros((dk, width), F32),
        jnp.zeros((1, width), F32),
        jnp.zeros((1, width), F32),
        jnp.full((1, width), LOG_FLOOR, F32),
    )


def chip_kernel(at_ref, mine_ref, other_ref, out_ref):
    first_here = at_ref[1] == 0
    mine, other = mine_ref[...], other_ref[...]
    first = parts_of(jnp.where(first_here, mine, other), 128)
    second = parts_of(jnp.where(first_here, other, mine), 128)
    pack(out_ref, *fold(first, second))


def output_kernel(
    at_ref, q_ref, k_ref, v_ref, in_ref, forget_ref, gate_ref, gain_ref, all_ref, other_ref,
    out_ref,
):
    n, dk = q_ref.shape
    scale = dk ** (-0.5)
    column, row = cumulative_forms(forget_ref[...])
    before = lax.fori_loop(
        0,
        at_ref[0],
        lambda k, state: fold(state, unpack(all_ref[k], dk)),
        first_state(dk, all_ref.shape[2]),
    )
    joined = fold(before, parts_of(other_ref[...], dk))
    memory, normal, _, top_before = [
        jnp.where(at_ref[1] == 0, alone, both) for alone, both in zip(before, joined)
    ]
    normal = normal[:, :dk]
    top_before = top_before[:, 0:1]
    log_in = in_ref[...]
    step = n // 4
    for start in range(0, n, step):
        rows, seen = slice(start, start + step), start + step
        q = q_ref[rows, :]
        at = column[rows, :]
        causal = iota((step, seen), 1) <= iota((step, seen), 0) + start
        log_decay = jnp.where(causal, at - row[:, :seen] + log_in[:, :seen], MASKED)
        log_inter = at + top_before
        top = jnp.maximum(log_inter, jnp.max(log_decay, axis=1, keepdims=True))
        scores = dot_t(q, k_ref[0:seen, :]) * scale * jnp.exp(log_decay - top)
        carried = jnp.exp(log_inter - top) * scale
        wide = q.astype(F32)
        numerator = carried * jnp.dot(
            wide, memory, precision=HIGHEST, preferred_element_type=F32
        ) + dot(scores.astype(BF16), v_ref[0:seen, :])
        denominator = carried * jnp.sum(wide * normal, axis=1, keepdims=True) + jnp.sum(
            scores, axis=1, keepdims=True
        )
        values = numerator / jnp.maximum(jnp.abs(denominator), jnp.exp(-top))
        values = values * lax.rsqrt(jnp.mean(values * values, axis=1, keepdims=True) + EPSILON)
        gate = gate_ref[rows, :].astype(F32)
        values = values * gain_ref[...] * (1.0 / (1.0 + jnp.exp(-gate)))
        out_ref[rows, :] = values.astype(BF16)


def dispatch_kernel(routes_ref, x_ref, out_ref):
    tokens = x_ref.shape[0]
    slots = out_ref.shape[0]
    experts, room = 32, slots // 32
    expert = iota((experts, tokens), 0)
    named = jnp.zeros((experts, tokens), F32)
    for r in range(routes_ref.shape[0]):
        named = named + (routes_ref[r : r + 1, :] == expert).astype(F32)
    earlier = (iota((tokens, tokens), 0) < iota((tokens, tokens), 1)).astype(F32).astype(BF16)
    place = dot(named.astype(BF16), earlier)
    key = jnp.where(named > 0.5, place, -1.0).astype(BF16)
    slot = iota((slots, experts), 0)
    spread = (slot // room == iota((slots, experts), 1)).astype(F32).astype(BF16)
    wanted = (iota((slots, tokens), 0) % room).astype(F32)
    chosen = (dot(spread, key) == wanted).astype(F32).astype(BF16)
    out_ref[...] = dot(chosen, x_ref[...]).astype(BF16)


def plan_kernel(routes_ref, weight_ref, high_ref, low_ref):
    tokens, slots = high_ref.shape
    experts, room = 32, slots // 32
    expert = iota((tokens, experts), 1)
    named = jnp.zeros((tokens, experts), F32)
    weight = jnp.zeros((tokens, experts), F32)
    for r in range(routes_ref.shape[1]):
        hit = routes_ref[:, r : r + 1] == expert
        named = named + hit.astype(F32)
        weight = weight + jnp.where(hit, weight_ref[:, r : r + 1], 0.0)
    earlier = (iota((tokens, tokens), 1) < iota((tokens, tokens), 0)).astype(F32).astype(BF16)
    place = dot(earlier, named.astype(BF16))
    key = jnp.where(named > 0.5, place, -1.0).astype(BF16)
    slot = iota((experts, slots), 1)
    spread = (slot // room == iota((experts, slots), 0)).astype(F32).astype(BF16)
    wanted = (iota((tokens, slots), 1) % room).astype(F32)
    chosen = dot(key, spread) == wanted
    high, low, _ = split3(weight)
    high_ref[...] = jnp.where(chosen, dot(high, spread), 0.0).astype(BF16)
    low_ref[...] = jnp.where(chosen, dot(low, spread), 0.0).astype(BF16)


def collect_kernel(high_ref, low_ref, back_ref, out_ref):
    back = back_ref[...]
    out_ref[...] = (dot(high_ref[...], back) + dot(low_ref[...], back)).astype(BF16)


def hidden_kernel(
    x_ref, g0_ref, g1_ref, g2_ref, g3_ref, u0_ref, u1_ref, u2_ref, u3_ref,
    out_ref, gate_acc, up_acc, squares,
):
    step = pl.program_id(0)
    _, _, columns = x_ref.shape
    senders = g0_ref.shape[1] // columns
    pieces = [x_ref[step * senders + i] for i in range(senders)]
    x = jnp.concatenate(pieces, axis=1)
    gate = jnp.concatenate([w[...] for w in (g0_ref, g1_ref, g2_ref, g3_ref)], axis=0)
    up = jnp.concatenate([w[...] for w in (u0_ref, u1_ref, u2_ref, u3_ref)], axis=0)
    gate_part, up_part = dot_t(x, gate), dot_t(x, up)
    square = jnp.zeros(squares.shape, F32)
    for piece in pieces:
        wide = piece.astype(F32)
        square = square + wide * wide

    @pl.when(step == 0)
    def _():
        gate_acc[...] = gate_part
        up_acc[...] = up_part
        squares[...] = square

    @pl.when(step > 0)
    def _():
        gate_acc[...] += gate_part
        up_acc[...] += up_part
        squares[...] += square

    @pl.when(step == pl.num_programs(0) - 1)
    def _():
        total = jnp.sum(squares[...], axis=1, keepdims=True)
        inverse = lax.rsqrt(total * (1.0 / (columns * x_ref.shape[0])) + EPSILON)
        gate = gate_acc[...] * inverse
        hidden = gate * (1.0 / (1.0 + jnp.exp(-gate))) * (up_acc[...] * inverse)
        hidden = hidden.astype(BF16)
        for copy in range(out_ref.shape[0]):
            out_ref[copy] = hidden


def down_kernel(at_ref, h_ref, w0_ref, w1_ref, w2_ref, w3_ref, out_ref):
    part = h_ref.shape[2] // 4
    y = at_ref[2]
    hidden = jnp.concatenate([h_ref[xs] for xs in range(4)], axis=1)
    for k, w_ref in enumerate((w0_ref, w1_ref, w2_ref, w3_ref)):
        weight = []
        for xs in range(4):
            for j in range(4):
                start = (lax.rem(y + j, 4) * 4 + xs) * part
                weight.append(w_ref[pl.ds(pl.multiple_of(start, part), part), :])
        out_ref[lax.rem(y + k, 4)] = dot(hidden, jnp.concatenate(weight, axis=0)).astype(BF16)


def mix_kernel(h_ref, w_ref, out_ref, acc):
    step = pl.program_id(0)
    width = h_ref.shape[2]
    total = jnp.zeros(acc.shape, F32)
    for i in range(h_ref.shape[0]):
        total = total + dot(h_ref[i], w_ref[i * width : (i + 1) * width, :])

    @pl.when(step == 0)
    def _():
        acc[...] = total

    @pl.when(step > 0)
    def _():
        acc[...] += total

    @pl.when(step == pl.num_programs(0) - 1)
    def _():
        out_ref[...] = acc[...].astype(BF16)


def from_next(x, axis, k):
    n = lax.axis_size(axis)
    return lax.ppermute(x, axis, [((i + k) % n, i) for i in range(n)])


def exchange(x, axis):
    return lax.all_to_all(x, axis, split_axis=0, concat_axis=0, tiled=True)


def body(
    query_rows,
    key_rows,
    value_rows,
    in_gate,
    forget_gate,
    out_gate,
    head_gain,
    mix_weight,
    expert_input,
    routes,
    route_weight,
    gate_weight,
    up_weight,
    down_weight,
):
    sds = jax.ShapeDtypeStruct
    rows_a, dk = query_rows.shape
    dv = value_rows.shape[1]
    tokens, columns = expert_input.shape
    ep, tp = lax.axis_size(EP), lax.axis_size(TP)
    gate_local, up_local, down_local = gate_weight[0], up_weight[0], down_weight[0]
    width = gate_local.shape[0]
    slots = ep * 32
    at = jnp.stack([lax.axis_index(axis) for axis in ("z", "c", "y")]).astype(jnp.int32)

    table = call(dispatch_kernel, pltpu.VMEM((slots, columns), BF16), (routes.T, expert_input))
    arrived = exchange(table.reshape(ep, 32, columns), EP)
    arrived = arrived.reshape(4, 1, slots // 4, columns)

    gate_1 = from_next(gate_local, "y", 1)
    up_3 = from_next(up_local, "y", 3)
    gate_3 = from_next(gate_local, "y", 3)
    up_1 = from_next(up_local, "y", 1)
    gate_2 = from_next(gate_1, "y", 1)
    up_2 = from_next(up_3, "y", 3)
    down_far = []
    for k in (1, 3, 2):
        down_far.append(from_next(down_local, "y", k))
    down_1, down_3, down_2 = down_far

    mine = call(
        summary_kernel, sds((dk + 8, dv), F32), (key_rows, value_rows, in_gate, forget_gate)
    )
    other = lax.ppermute(mine, "c", [(0, 1), (1, 0)])
    chip = call(chip_kernel, sds((dk + 16, dv), BF16), (at, mine, other), near=(2,))
    states = lax.all_gather(chip, "z", axis=0)
    heads = call(
        output_kernel,
        sds((rows_a, dv), BF16),
        (
            at, query_rows, key_rows, value_rows, in_gate, forget_gate, out_gate,
            head_gain[None, :], states, other,
        ),
        near=(9,),
    )

    sent = jnp.broadcast_to(arrived, (4, 4, slots // 4, columns)).reshape(tp, slots // 4, columns)
    rows = exchange(sent, TP)
    grid = 2
    per = tp // grid
    weights_spec = lambda r: pl.BlockSpec((r, per * columns), lambda i: (0, i))
    hidden = call(
        hidden_kernel,
        sds((4, slots // 4, 4 * width), BF16),
        (rows, gate_local, gate_1, gate_2, gate_3, up_local, up_1, up_2, up_3),
        scratch=[pltpu.VMEM((slots // 4, 4 * width), F32)] * 2
        + [pltpu.VMEM((slots // 4, columns), F32)],
        grid=(grid,),
        in_specs=[
            pl.BlockSpec(memory_space=pltpu.VMEM),
        ]
        + [weights_spec(width)] * 8,
        out_specs=pl.BlockSpec(memory_space=pltpu.VMEM),
        near=(0,),
    )
    gathered = exchange(hidden, "x")
    results = call(
        down_kernel,
        pltpu.VMEM((4, slots // 4, columns), BF16),
        (at, gathered, down_local, down_1, down_2, down_3),
        near=(1,),
    )
    results = exchange(results, "y")
    back = exchange(results.reshape(ep, 32, columns), EP).reshape(slots, columns)

    all_heads = lax.all_gather(heads, TP, axis=0)
    steps = 2
    mixer_out = call(
        mix_kernel,
        sds((rows_a, columns), BF16),
        (all_heads, mix_weight),
        scratch=[pltpu.VMEM((rows_a, columns), F32)],
        grid=(steps,),
        in_specs=[
            pl.BlockSpec((tp // steps, rows_a, dv), lambda i: (i, 0, 0)),
            pl.BlockSpec((tp * dv // steps, columns), lambda i: (i, 0)),
        ],
        out_specs=pl.BlockSpec((rows_a, columns), lambda i: (0, 0)),
    )

    share = [pltpu.VMEM((tokens, slots), BF16)] * 2
    plan = call(plan_kernel, share, (routes, route_weight))
    expert_out = call(collect_kernel, sds((tokens, columns), BF16), (*plan, back), near=(0, 1, 2))
    return (mixer_out, expert_out)


def solution(mesh):
    split = Mesh(mesh.devices.reshape(16, 2, 4, 4), (*EP, *TP))
    in_specs = (
        P(EP, TP),
        P(EP, TP),
        P(EP, TP),
        P(TP, EP),
        P(TP, EP),
        P(EP, TP),
        P(TP),
        P(None, TP),
        P(EP, TP),
        P(EP, None),
        P(EP, None),
        P(EP, TP, None),
        P(EP, TP, None),
        P(EP, None, TP),
    )
    out_specs = (P(EP, TP), P(EP, TP))

    return jax.shard_map(body, mesh=split, in_specs=in_specs, out_specs=out_specs, check_vma=False)
```

```python
import jax
import jax.numpy as jnp
from jax import lax
from jax.experimental import pallas as pl
from jax.experimental.pallas import tpu as pltpu
from jax.sharding import Mesh
from jax.sharding import PartitionSpec as P


EP = ("z", "c")
TP = ("y", "x")
EPSILON = 1e-06
LOG_FLOOR = -1e30
MASKED = -1e38
HIGHEST = lax.Precision.HIGHEST
F32 = jnp.float32
BF16 = jnp.bfloat16


def dot(a, b):
    return jnp.dot(a, b, preferred_element_type=F32)


def dot_t(a, b):
    return lax.dot_general(a, b, (((1,), (1,)), ((), ())), preferred_element_type=F32)


def iota(shape, dim):
    return lax.broadcasted_iota(jnp.int32, shape, dim)


def call(kernel, out, args, scratch=(), grid=None, in_specs=None, out_specs=None, near=()):
    args = [
        pltpu.with_memory_space_constraint(a, pltpu.VMEM) if i in near else a
        for i, a in enumerate(args)
    ]
    vmem = pl.BlockSpec(memory_space=pltpu.VMEM)
    smem = pl.BlockSpec(memory_space=pltpu.SMEM)
    if in_specs is None:
        in_specs = [smem if a.dtype == jnp.int32 and a.ndim == 1 else vmem for a in args]
    kw = {} if grid is None else {"grid": grid}
    if out_specs is None:
        out_specs = jax.tree.map(lambda _: vmem, out)
    return pl.pallas_call(
        kernel,
        out_shape=out,
        in_specs=in_specs,
        out_specs=out_specs,
        scratch_shapes=list(scratch),
        compiler_params=pltpu.CompilerParams(vmem_limit_bytes=57 << 20),
        **kw,
    )(*args)


def log_sigmoid(f):
    return jnp.minimum(f, 0.0) - jnp.log1p(jnp.exp(-jnp.abs(f)))


def cumulative_forms(forget_row):
    n = forget_row.shape[1]
    logs = jnp.broadcast_to(log_sigmoid(forget_row), (n, n))
    at_row, at_col = iota((n, n), 0), iota((n, n), 1)
    column = jnp.sum(jnp.where(at_col <= at_row, logs, 0.0), axis=1, keepdims=True)
    own = jnp.sum(jnp.where(at_col == at_row, logs, 0.0), axis=1, keepdims=True)
    row = jnp.sum(jnp.where(at_row <= at_col, own, 0.0), axis=0, keepdims=True)
    return column, row


def summary_kernel(k_ref, v_ref, in_ref, forget_ref, out_ref):
    n = k_ref.shape[0]
    dk = k_ref.shape[1]
    column, _ = cumulative_forms(forget_ref[...])
    diagonal = iota((n, n), 0) == iota((n, n), 1)
    log_in = jnp.sum(
        jnp.where(diagonal, jnp.broadcast_to(in_ref[...], (n, n)), 0.0), axis=1, keepdims=True
    )
    total = column[n - 1 :, :]
    weight_log = total - column + log_in
    top = jnp.max(weight_log, axis=0, keepdims=True)
    weighted = k_ref[...].astype(F32) * jnp.exp(weight_log - top)
    memory = lax.dot_general(
        weighted.astype(BF16), v_ref[...], (((0,), (0,)), ((), ())), preferred_element_type=F32
    )
    normal = jnp.sum(weighted, axis=0, keepdims=True)
    width = out_ref.shape[1]
    normal = jnp.concatenate([normal] * (width // dk), axis=1)
    pack(
        out_ref,
        memory,
        normal,
        jnp.broadcast_to(total, (1, width)),
        jnp.broadcast_to(top, (1, width)),
    )


def fold(first, second):
    memory_1, normal_1, decay_1, max_1 = first
    memory_2, normal_2, decay_2, max_2 = second
    top = jnp.maximum(decay_2 + max_1, max_2)
    keep_1 = jnp.exp(decay_2 + max_1 - top)
    keep_2 = jnp.exp(max_2 - top)
    return (
        keep_1 * memory_1 + keep_2 * memory_2,
        keep_1 * normal_1 + keep_2 * normal_2,
        decay_1 + decay_2,
        top,
    )


def split3(x):
    high = x.astype(BF16)
    rest = x - high.astype(F32)
    middle = rest.astype(BF16)
    low = (rest - middle.astype(F32)).astype(BF16)
    return high, middle, low


def pack(out_ref, memory, normal, decay, top):
    dk, width = memory.shape
    out_ref[0:dk, :] = memory.astype(BF16)
    rows = []
    for value in (normal, decay, top):
        rows += [part.astype(F32) for part in split3(value)]
    rows.append(jnp.zeros((out_ref.shape[0] - dk - len(rows), width), F32))
    out_ref[dk:, :] = jnp.concatenate(rows, axis=0).astype(BF16)


def unpack(item, dk):
    item = item.astype(F32)
    rows = [
        item[dk + i : dk + i + 1] + item[dk + i + 1 : dk + i + 2] + item[dk + i + 2 : dk + i + 3]
        for i in (0, 3, 6)
    ]
    return (item[0:dk], *rows)


def first_state(dk, width):
    return (
        jnp.zeros((dk, width), F32),
        jnp.zeros((1, width), F32),
        jnp.zeros((1, width), F32),
        jnp.full((1, width), LOG_FLOOR, F32),
    )


def output_kernel(
    at_ref, q_ref, k_ref, v_ref, in_ref, forget_ref, gate_ref, gain_ref, all_ref, out_ref
):
    n, dk = q_ref.shape
    scale = dk ** (-0.5)
    column, row = cumulative_forms(forget_ref[...])
    memory, normal, _, top_before = lax.fori_loop(
        0,
        at_ref[0],
        lambda k, state: fold(state, unpack(all_ref[k], dk)),
        first_state(dk, all_ref.shape[2]),
    )
    normal = normal[:, :dk]
    top_before = top_before[:, 0:1]
    log_in = in_ref[...]
    step = n // 4
    for start in range(0, n, step):
        rows, seen = slice(start, start + step), start + step
        q = q_ref[rows, :]
        at = column[rows, :]
        causal = iota((step, seen), 1) <= iota((step, seen), 0) + start
        log_decay = jnp.where(causal, at - row[:, :seen] + log_in[:, :seen], MASKED)
        log_inter = at + top_before
        top = jnp.maximum(log_inter, jnp.max(log_decay, axis=1, keepdims=True))
        scores = dot_t(q, k_ref[0:seen, :]) * scale * jnp.exp(log_decay - top)
        carried = jnp.exp(log_inter - top) * scale
        wide = q.astype(F32)
        numerator = carried * jnp.dot(
            wide, memory, precision=HIGHEST, preferred_element_type=F32
        ) + dot(scores.astype(BF16), v_ref[0:seen, :])
        denominator = carried * jnp.sum(wide * normal, axis=1, keepdims=True) + jnp.sum(
            scores, axis=1, keepdims=True
        )
        values = numerator / jnp.maximum(jnp.abs(denominator), jnp.exp(-top))
        values = values * lax.rsqrt(jnp.mean(values * values, axis=1, keepdims=True) + EPSILON)
        gate = gate_ref[rows, :].astype(F32)
        values = values * gain_ref[...] * (1.0 / (1.0 + jnp.exp(-gate)))
        out_ref[rows, :] = values.astype(BF16)


def dispatch_kernel(routes_ref, x_ref, out_ref):
    tokens = x_ref.shape[0]
    slots = out_ref.shape[0]
    experts, room = 32, slots // 32
    expert = iota((experts, tokens), 0)
    named = jnp.zeros((experts, tokens), F32)
    for r in range(routes_ref.shape[0]):
        named = named + (routes_ref[r : r + 1, :] == expert).astype(F32)
    earlier = (iota((tokens, tokens), 0) < iota((tokens, tokens), 1)).astype(F32).astype(BF16)
    place = dot(named.astype(BF16), earlier)
    key = jnp.where(named > 0.5, place, -1.0).astype(BF16)
    slot = iota((slots, experts), 0)
    spread = (slot // room == iota((slots, experts), 1)).astype(F32).astype(BF16)
    wanted = (iota((slots, tokens), 0) % room).astype(F32)
    chosen = (dot(spread, key) == wanted).astype(F32).astype(BF16)
    out_ref[...] = dot(chosen, x_ref[...]).astype(BF16)


def plan_kernel(routes_ref, weight_ref, high_ref, low_ref):
    tokens, slots = high_ref.shape
    experts, room = 32, slots // 32
    expert = iota((tokens, experts), 1)
    named = jnp.zeros((tokens, experts), F32)
    weight = jnp.zeros((tokens, experts), F32)
    for r in range(routes_ref.shape[1]):
        hit = routes_ref[:, r : r + 1] == expert
        named = named + hit.astype(F32)
        weight = weight + jnp.where(hit, weight_ref[:, r : r + 1], 0.0)
    earlier = (iota((tokens, tokens), 1) < iota((tokens, tokens), 0)).astype(F32).astype(BF16)
    place = dot(earlier, named.astype(BF16))
    key = jnp.where(named > 0.5, place, -1.0).astype(BF16)
    slot = iota((experts, slots), 1)
    spread = (slot // room == iota((experts, slots), 0)).astype(F32).astype(BF16)
    wanted = (iota((tokens, slots), 1) % room).astype(F32)
    chosen = dot(key, spread) == wanted
    high, low, _ = split3(weight)
    high_ref[...] = jnp.where(chosen, dot(high, spread), 0.0).astype(BF16)
    low_ref[...] = jnp.where(chosen, dot(low, spread), 0.0).astype(BF16)


def collect_kernel(high_ref, low_ref, back_ref, out_ref):
    back = back_ref[...]
    out_ref[...] = (dot(high_ref[...], back) + dot(low_ref[...], back)).astype(BF16)


def hidden_kernel(
    x_ref, g0_ref, g1_ref, g2_ref, g3_ref, u0_ref, u1_ref, u2_ref, u3_ref,
    out_ref, gate_acc, up_acc, squares,
):
    step = pl.program_id(0)
    _, _, columns = x_ref.shape
    senders = g0_ref.shape[1] // columns
    pieces = [x_ref[step * senders + i] for i in range(senders)]
    x = jnp.concatenate(pieces, axis=1)
    gate = jnp.concatenate([w[...] for w in (g0_ref, g1_ref, g2_ref, g3_ref)], axis=0)
    up = jnp.concatenate([w[...] for w in (u0_ref, u1_ref, u2_ref, u3_ref)], axis=0)
    gate_part, up_part = dot_t(x, gate), dot_t(x, up)
    square = jnp.zeros(squares.shape, F32)
    for piece in pieces:
        wide = piece.astype(F32)
        square = square + wide * wide

    @pl.when(step == 0)
    def _():
        gate_acc[...] = gate_part
        up_acc[...] = up_part
        squares[...] = square

    @pl.when(step > 0)
    def _():
        gate_acc[...] += gate_part
        up_acc[...] += up_part
        squares[...] += square

    @pl.when(step == pl.num_programs(0) - 1)
    def _():
        total = jnp.sum(squares[...], axis=1, keepdims=True)
        inverse = lax.rsqrt(total * (1.0 / (columns * x_ref.shape[0])) + EPSILON)
        gate = gate_acc[...] * inverse
        hidden = gate * (1.0 / (1.0 + jnp.exp(-gate))) * (up_acc[...] * inverse)
        hidden = hidden.astype(BF16)
        for copy in range(out_ref.shape[0]):
            out_ref[copy] = hidden


def down_kernel(at_ref, h_ref, w0_ref, w1_ref, w2_ref, w3_ref, out_ref):
    part = h_ref.shape[2] // 4
    y = at_ref[1]
    hidden = jnp.concatenate([h_ref[xs] for xs in range(4)], axis=1)
    for k, w_ref in enumerate((w0_ref, w1_ref, w2_ref, w3_ref)):
        weight = []
        for xs in range(4):
            for j in range(4):
                start = (lax.rem(y + j, 4) * 4 + xs) * part
                weight.append(w_ref[pl.ds(pl.multiple_of(start, part), part), :])
        out_ref[lax.rem(y + k, 4)] = dot(hidden, jnp.concatenate(weight, axis=0)).astype(BF16)


def mix_kernel(h_ref, w_ref, out_ref, acc):
    step = pl.program_id(0)
    width = h_ref.shape[2]
    total = jnp.zeros(acc.shape, F32)
    for i in range(h_ref.shape[0]):
        total = total + dot(h_ref[i], w_ref[i * width : (i + 1) * width, :])

    @pl.when(step == 0)
    def _():
        acc[...] = total

    @pl.when(step > 0)
    def _():
        acc[...] += total

    @pl.when(step == pl.num_programs(0) - 1)
    def _():
        out_ref[...] = acc[...].astype(BF16)


def from_next(x, axis, k):
    n = lax.axis_size(axis)
    return lax.ppermute(x, axis, [((i + k) % n, i) for i in range(n)])


def exchange(x, axis):
    return lax.all_to_all(x, axis, split_axis=0, concat_axis=0, tiled=True)


def body(
    query_rows,
    key_rows,
    value_rows,
    in_gate,
    forget_gate,
    out_gate,
    head_gain,
    mix_weight,
    expert_input,
    routes,
    route_weight,
    gate_weight,
    up_weight,
    down_weight,
):
    sds = jax.ShapeDtypeStruct
    rows_a, dk = query_rows.shape
    dv = value_rows.shape[1]
    tokens, columns = expert_input.shape
    ep, tp = lax.axis_size(EP), lax.axis_size(TP)
    gate_local, up_local, down_local = gate_weight[0], up_weight[0], down_weight[0]
    width = gate_local.shape[0]
    slots = ep * 32
    at = jnp.stack([lax.axis_index(EP), lax.axis_index("y")]).astype(jnp.int32)

    mine = call(
        summary_kernel, sds((dk + 16, dv), BF16), (key_rows, value_rows, in_gate, forget_gate)
    )
    states = lax.all_gather(mine, EP, axis=0)
    table = call(dispatch_kernel, pltpu.VMEM((slots, columns), BF16), (routes.T, expert_input))
    arrived = exchange(table.reshape(ep, 32, columns), EP)
    arrived = arrived.reshape(4, 1, slots // 4, columns)

    gate_1 = from_next(gate_local, "y", 1)
    up_3 = from_next(up_local, "y", 3)
    gate_3 = from_next(gate_local, "y", 3)
    up_1 = from_next(up_local, "y", 1)
    gate_2 = from_next(gate_1, "y", 1)
    up_2 = from_next(up_3, "y", 3)
    down_far = []
    for k in (1, 3, 2):
        down_far.append(from_next(down_local, "y", k))
    down_1, down_3, down_2 = down_far

    heads = call(
        output_kernel,
        sds((rows_a, dv), BF16),
        (
            at, query_rows, key_rows, value_rows, in_gate, forget_gate, out_gate,
            head_gain[None, :], states,
        ),
    )

    sent = jnp.broadcast_to(arrived, (4, 4, slots // 4, columns)).reshape(tp, slots // 4, columns)
    rows = exchange(sent, TP)
    grid = 2
    per = tp // grid
    weights_spec = lambda r: pl.BlockSpec((r, per * columns), lambda i: (0, i))
    hidden = call(
        hidden_kernel,
        sds((4, slots // 4, 4 * width), BF16),
        (rows, gate_local, gate_1, gate_2, gate_3, up_local, up_1, up_2, up_3),
        scratch=[pltpu.VMEM((slots // 4, 4 * width), F32)] * 2
        + [pltpu.VMEM((slots // 4, columns), F32)],
        grid=(grid,),
        in_specs=[
            pl.BlockSpec(memory_space=pltpu.VMEM),
        ]
        + [weights_spec(width)] * 8,
        out_specs=pl.BlockSpec(memory_space=pltpu.VMEM),
        near=(0,),
    )
    gathered = exchange(hidden, "x")
    results = call(
        down_kernel,
        pltpu.VMEM((4, slots // 4, columns), BF16),
        (at, gathered, down_local, down_1, down_2, down_3),
        near=(1,),
    )
    results = exchange(results, "y")
    back = exchange(results.reshape(ep, 32, columns), EP).reshape(slots, columns)

    all_heads = lax.all_gather(heads, TP, axis=0)
    steps = 2
    mixer_out = call(
        mix_kernel,
        sds((rows_a, columns), BF16),
        (all_heads, mix_weight),
        scratch=[pltpu.VMEM((rows_a, columns), F32)],
        grid=(steps,),
        in_specs=[
            pl.BlockSpec((tp // steps, rows_a, dv), lambda i: (i, 0, 0)),
            pl.BlockSpec((tp * dv // steps, columns), lambda i: (i, 0)),
        ],
        out_specs=pl.BlockSpec((rows_a, columns), lambda i: (0, 0)),
    )

    share = [pltpu.VMEM((tokens, slots), BF16)] * 2
    plan = call(plan_kernel, share, (routes, route_weight))
    expert_out = call(collect_kernel, sds((tokens, columns), BF16), (*plan, back), near=(0, 1, 2))
    return (mixer_out, expert_out)


def solution(mesh):
    split = Mesh(mesh.devices.reshape(16, 2, 4, 4), (*EP, *TP))
    in_specs = (
        P(EP, TP),
        P(EP, TP),
        P(EP, TP),
        P(TP, EP),
        P(TP, EP),
        P(EP, TP),
        P(TP),
        P(None, TP),
        P(EP, TP),
        P(EP, None),
        P(EP, None),
        P(EP, TP, None),
        P(EP, TP, None),
        P(EP, None, TP),
    )
    out_specs = (P(EP, TP), P(EP, TP))

    return jax.shard_map(body, mesh=split, in_specs=in_specs, out_specs=out_specs, check_vma=False)
```

```python
import jax
import jax.numpy as jnp
from jax import lax
from jax.experimental import pallas as pl
from jax.experimental.pallas import tpu as pltpu
from jax.sharding import Mesh
from jax.sharding import PartitionSpec as P


EP = ("z", "c")
TP = ("y", "x")
EPSILON = 1e-06
LOG_FLOOR = -1e30
MASKED = -1e38
HIGHEST = lax.Precision.HIGHEST
F32 = jnp.float32
BF16 = jnp.bfloat16


def dot(a, b):
    return jnp.dot(a, b, preferred_element_type=F32)


def dot_t(a, b):
    return lax.dot_general(a, b, (((1,), (1,)), ((), ())), preferred_element_type=F32)


def iota(shape, dim):
    return lax.broadcasted_iota(jnp.int32, shape, dim)


def call(kernel, out, args, scratch=(), grid=None, in_specs=None, out_specs=None, near=()):
    args = [
        pltpu.with_memory_space_constraint(a, pltpu.VMEM) if i in near else a
        for i, a in enumerate(args)
    ]
    vmem = pl.BlockSpec(memory_space=pltpu.VMEM)
    smem = pl.BlockSpec(memory_space=pltpu.SMEM)
    if in_specs is None:
        in_specs = [smem if a.dtype == jnp.int32 and a.ndim == 1 else vmem for a in args]
    kw = {} if grid is None else {"grid": grid}
    if out_specs is None:
        out_specs = jax.tree.map(lambda _: vmem, out)
    return pl.pallas_call(
        kernel,
        out_shape=out,
        in_specs=in_specs,
        out_specs=out_specs,
        scratch_shapes=list(scratch),
        compiler_params=pltpu.CompilerParams(vmem_limit_bytes=57 << 20),
        **kw,
    )(*args)


def log_sigmoid(f):
    return jnp.minimum(f, 0.0) - jnp.log1p(jnp.exp(-jnp.abs(f)))


def cumulative_forms(forget_row):
    n = forget_row.shape[1]
    logs = jnp.broadcast_to(log_sigmoid(forget_row), (n, n))
    at_row, at_col = iota((n, n), 0), iota((n, n), 1)
    column = jnp.sum(jnp.where(at_col <= at_row, logs, 0.0), axis=1, keepdims=True)
    own = jnp.sum(jnp.where(at_col == at_row, logs, 0.0), axis=1, keepdims=True)
    row = jnp.sum(jnp.where(at_row <= at_col, own, 0.0), axis=0, keepdims=True)
    return column, row


def summary_kernel(k_ref, v_ref, in_ref, forget_ref, out_ref):
    n = k_ref.shape[0]
    dk = k_ref.shape[1]
    column, _ = cumulative_forms(forget_ref[...])
    diagonal = iota((n, n), 0) == iota((n, n), 1)
    log_in = jnp.sum(
        jnp.where(diagonal, jnp.broadcast_to(in_ref[...], (n, n)), 0.0), axis=1, keepdims=True
    )
    total = column[n - 1 :, :]
    weight_log = total - column + log_in
    top = jnp.max(weight_log, axis=0, keepdims=True)
    weighted = k_ref[...].astype(F32) * jnp.exp(weight_log - top)
    memory = lax.dot_general(
        weighted.astype(BF16), v_ref[...], (((0,), (0,)), ((), ())), preferred_element_type=F32
    )
    normal = jnp.sum(weighted, axis=0, keepdims=True)
    width = out_ref.shape[1]
    normal = jnp.concatenate([normal] * (width // dk), axis=1)
    pack(
        out_ref,
        memory,
        normal,
        jnp.broadcast_to(total, (1, width)),
        jnp.broadcast_to(top, (1, width)),
    )


def fold(first, second):
    memory_1, normal_1, decay_1, max_1 = first
    memory_2, normal_2, decay_2, max_2 = second
    top = jnp.maximum(decay_2 + max_1, max_2)
    keep_1 = jnp.exp(decay_2 + max_1 - top)
    keep_2 = jnp.exp(max_2 - top)
    return (
        keep_1 * memory_1 + keep_2 * memory_2,
        keep_1 * normal_1 + keep_2 * normal_2,
        decay_1 + decay_2,
        top,
    )


def split3(x):
    high = x.astype(BF16)
    rest = x - high.astype(F32)
    middle = rest.astype(BF16)
    low = (rest - middle.astype(F32)).astype(BF16)
    return high, middle, low


def pack(out_ref, memory, normal, decay, top):
    dk, width = memory.shape
    out_ref[0:dk, :] = memory.astype(BF16)
    rows = []
    for value in (normal, decay, top):
        rows += [part.astype(F32) for part in split3(value)]
    rows.append(jnp.zeros((out_ref.shape[0] - dk - len(rows), width), F32))
    out_ref[dk:, :] = jnp.concatenate(rows, axis=0).astype(BF16)


def unpack(item, dk):
    item = item.astype(F32)
    rows = [
        item[dk + i : dk + i + 1] + item[dk + i + 1 : dk + i + 2] + item[dk + i + 2 : dk + i + 3]
        for i in (0, 3, 6)
    ]
    return (item[0:dk], *rows)


def first_state(dk, width):
    return (
        jnp.zeros((dk, width), F32),
        jnp.zeros((1, width), F32),
        jnp.zeros((1, width), F32),
        jnp.full((1, width), LOG_FLOOR, F32),
    )


def output_kernel(
    at_ref, q_ref, k_ref, v_ref, in_ref, forget_ref, gate_ref, gain_ref, all_ref, out_ref
):
    n, dk = q_ref.shape
    scale = dk ** (-0.5)
    column, row = cumulative_forms(forget_ref[...])
    memory, normal, _, top_before = lax.fori_loop(
        0,
        at_ref[0],
        lambda k, state: fold(state, unpack(all_ref[k], dk)),
        first_state(dk, all_ref.shape[2]),
    )
    normal = normal[:, :dk]
    top_before = top_before[:, 0:1]
    log_in = in_ref[...]
    step = n // 4
    for start in range(0, n, step):
        rows, seen = slice(start, start + step), start + step
        q = q_ref[rows, :]
        at = column[rows, :]
        causal = iota((step, seen), 1) <= iota((step, seen), 0) + start
        log_decay = jnp.where(causal, at - row[:, :seen] + log_in[:, :seen], MASKED)
        log_inter = at + top_before
        top = jnp.maximum(log_inter, jnp.max(log_decay, axis=1, keepdims=True))
        scores = dot_t(q, k_ref[0:seen, :]) * scale * jnp.exp(log_decay - top)
        carried = jnp.exp(log_inter - top) * scale
        wide = q.astype(F32)
        numerator = carried * jnp.dot(
            wide, memory, precision=HIGHEST, preferred_element_type=F32
        ) + dot(scores.astype(BF16), v_ref[0:seen, :])
        denominator = carried * jnp.sum(wide * normal, axis=1, keepdims=True) + jnp.sum(
            scores, axis=1, keepdims=True
        )
        values = numerator / jnp.maximum(jnp.abs(denominator), jnp.exp(-top))
        values = values * lax.rsqrt(jnp.mean(values * values, axis=1, keepdims=True) + EPSILON)
        gate = gate_ref[rows, :].astype(F32)
        values = values * gain_ref[...] * (1.0 / (1.0 + jnp.exp(-gate)))
        out_ref[rows, :] = values.astype(BF16)


def dispatch_kernel(routes_ref, x_ref, out_ref):
    tokens = x_ref.shape[0]
    slots = out_ref.shape[0]
    experts, room = 32, slots // 32
    expert = iota((experts, tokens), 0)
    named = jnp.zeros((experts, tokens), F32)
    for r in range(routes_ref.shape[0]):
        named = named + (routes_ref[r : r + 1, :] == expert).astype(F32)
    earlier = (iota((tokens, tokens), 0) < iota((tokens, tokens), 1)).astype(F32).astype(BF16)
    place = dot(named.astype(BF16), earlier)
    key = jnp.where(named > 0.5, place, -1.0).astype(BF16)
    slot = iota((slots, experts), 0)
    spread = (slot // room == iota((slots, experts), 1)).astype(F32).astype(BF16)
    wanted = (iota((slots, tokens), 0) % room).astype(F32)
    chosen = (dot(spread, key) == wanted).astype(F32).astype(BF16)
    out_ref[...] = dot(chosen, x_ref[...]).astype(BF16)


def plan_kernel(routes_ref, weight_ref, high_ref, low_ref):
    tokens, slots = high_ref.shape
    experts, room = 32, slots // 32
    expert = iota((tokens, experts), 1)
    named = jnp.zeros((tokens, experts), F32)
    weight = jnp.zeros((tokens, experts), F32)
    for r in range(routes_ref.shape[1]):
        hit = routes_ref[:, r : r + 1] == expert
        named = named + hit.astype(F32)
        weight = weight + jnp.where(hit, weight_ref[:, r : r + 1], 0.0)
    earlier = (iota((tokens, tokens), 1) < iota((tokens, tokens), 0)).astype(F32).astype(BF16)
    place = dot(earlier, named.astype(BF16))
    key = jnp.where(named > 0.5, place, -1.0).astype(BF16)
    slot = iota((experts, slots), 1)
    spread = (slot // room == iota((experts, slots), 0)).astype(F32).astype(BF16)
    wanted = (iota((tokens, slots), 1) % room).astype(F32)
    chosen = dot(key, spread) == wanted
    high, low, _ = split3(weight)
    high_ref[...] = jnp.where(chosen, dot(high, spread), 0.0).astype(BF16)
    low_ref[...] = jnp.where(chosen, dot(low, spread), 0.0).astype(BF16)


def collect_kernel(high_ref, low_ref, back_ref, out_ref):
    back = back_ref[...]
    out_ref[...] = (dot(high_ref[...], back) + dot(low_ref[...], back)).astype(BF16)


def hidden_kernel(
    x_ref, g0_ref, g1_ref, g2_ref, g3_ref, u0_ref, u1_ref, u2_ref, u3_ref,
    out_ref, gate_acc, up_acc, squares,
):
    step = pl.program_id(0)
    _, _, columns = x_ref.shape
    senders = g0_ref.shape[1] // columns
    order = [step * senders + i for i in range(senders)]
    pieces = [x_ref[lax.rem(t, 4) * 4 + t // 4] for t in order]
    x = jnp.concatenate(pieces, axis=1)
    gate = jnp.concatenate([w[...] for w in (g0_ref, g1_ref, g2_ref, g3_ref)], axis=0)
    up = jnp.concatenate([w[...] for w in (u0_ref, u1_ref, u2_ref, u3_ref)], axis=0)
    gate_part, up_part = dot_t(x, gate), dot_t(x, up)
    square = jnp.zeros(squares.shape, F32)
    for piece in pieces:
        wide = piece.astype(F32)
        square = square + wide * wide

    @pl.when(step == 0)
    def _():
        gate_acc[...] = gate_part
        up_acc[...] = up_part
        squares[...] = square

    @pl.when(step > 0)
    def _():
        gate_acc[...] += gate_part
        up_acc[...] += up_part
        squares[...] += square

    @pl.when(step == pl.num_programs(0) - 1)
    def _():
        total = jnp.sum(squares[...], axis=1, keepdims=True)
        inverse = lax.rsqrt(total * (1.0 / (columns * x_ref.shape[0])) + EPSILON)
        gate = gate_acc[...] * inverse
        hidden = gate * (1.0 / (1.0 + jnp.exp(-gate))) * (up_acc[...] * inverse)
        hidden = hidden.astype(BF16)
        for copy in range(out_ref.shape[0]):
            out_ref[copy] = hidden


def down_kernel(at_ref, h_ref, w0_ref, w1_ref, w2_ref, w3_ref, out_ref):
    part = h_ref.shape[2] // 4
    y = at_ref[1]
    hidden = jnp.concatenate([h_ref[xs] for xs in range(4)], axis=1)
    for k, w_ref in enumerate((w0_ref, w1_ref, w2_ref, w3_ref)):
        weight = []
        for xs in range(4):
            for j in range(4):
                start = (lax.rem(y + j, 4) * 4 + xs) * part
                weight.append(w_ref[pl.ds(pl.multiple_of(start, part), part), :])
        out_ref[lax.rem(y + k, 4)] = dot(hidden, jnp.concatenate(weight, axis=0)).astype(BF16)


def mix_kernel(h_ref, w_ref, out_ref, acc):
    step = pl.program_id(0)
    width = h_ref.shape[2]
    total = jnp.zeros(acc.shape, F32)
    for i in range(h_ref.shape[0]):
        total = total + dot(h_ref[i], w_ref[i * width : (i + 1) * width, :])

    @pl.when(step == 0)
    def _():
        acc[...] = total

    @pl.when(step > 0)
    def _():
        acc[...] += total

    @pl.when(step == pl.num_programs(0) - 1)
    def _():
        out_ref[...] = acc[...].astype(BF16)


def from_next(x, axis, k):
    n = lax.axis_size(axis)
    return lax.ppermute(x, axis, [((i + k) % n, i) for i in range(n)])


def exchange(x, axis):
    return lax.all_to_all(x, axis, split_axis=0, concat_axis=0, tiled=True)


def body(
    query_rows,
    key_rows,
    value_rows,
    in_gate,
    forget_gate,
    out_gate,
    head_gain,
    mix_weight,
    expert_input,
    routes,
    route_weight,
    gate_weight,
    up_weight,
    down_weight,
):
    sds = jax.ShapeDtypeStruct
    rows_a, dk = query_rows.shape
    dv = value_rows.shape[1]
    tokens, columns = expert_input.shape
    ep, tp = lax.axis_size(EP), lax.axis_size(TP)
    gate_local, up_local, down_local = gate_weight[0], up_weight[0], down_weight[0]
    width = gate_local.shape[0]
    slots = ep * 32
    at = jnp.stack([lax.axis_index(EP), lax.axis_index("y")]).astype(jnp.int32)

    mine = call(
        summary_kernel, sds((dk + 16, dv), BF16), (key_rows, value_rows, in_gate, forget_gate)
    )
    states = lax.all_gather(mine, EP, axis=0)
    table = call(dispatch_kernel, pltpu.VMEM((slots, columns), BF16), (routes.T, expert_input))
    arrived = exchange(table.reshape(4 * ep, 8, columns), (*EP, "y"))
    arrived = arrived.reshape(ep, 4, 8, columns).transpose(1, 0, 2, 3)

    gate_1 = from_next(gate_local, "y", 1)
    up_3 = from_next(up_local, "y", 3)
    gate_3 = from_next(gate_local, "y", 3)
    up_1 = from_next(up_local, "y", 1)
    gate_2 = from_next(gate_1, "y", 1)
    up_2 = from_next(up_3, "y", 3)
    down_far = []
    for k in (1, 3, 2):
        down_far.append(from_next(down_local, "y", k))
    down_1, down_3, down_2 = down_far

    heads = call(
        output_kernel,
        sds((rows_a, dv), BF16),
        (
            at, query_rows, key_rows, value_rows, in_gate, forget_gate, out_gate,
            head_gain[None, :], states,
        ),
    )

    sent = jnp.broadcast_to(arrived.reshape(1, slots, columns), (4, slots, columns))
    rows = exchange(sent, "x").reshape(tp, slots // 4, columns)
    grid = 2
    per = tp // grid
    weights_spec = lambda r: pl.BlockSpec((r, per * columns), lambda i: (0, i))
    hidden = call(
        hidden_kernel,
        sds((4, slots // 4, 4 * width), BF16),
        (rows, gate_local, gate_1, gate_2, gate_3, up_local, up_1, up_2, up_3),
        scratch=[pltpu.VMEM((slots // 4, 4 * width), F32)] * 2
        + [pltpu.VMEM((slots // 4, columns), F32)],
        grid=(grid,),
        in_specs=[
            pl.BlockSpec(memory_space=pltpu.VMEM),
        ]
        + [weights_spec(width)] * 8,
        out_specs=pl.BlockSpec(memory_space=pltpu.VMEM),
        near=(0,),
    )
    gathered = exchange(hidden, "x")
    results = call(
        down_kernel,
        pltpu.VMEM((4, slots // 4, columns), BF16),
        (at, gathered, down_local, down_1, down_2, down_3),
        near=(1,),
    )
    results = results.reshape(4, ep, 8, columns).transpose(1, 0, 2, 3)
    back = exchange(results.reshape(4 * ep, 8, columns), (*EP, "y")).reshape(slots, columns)

    all_heads = lax.all_gather(heads, TP, axis=0)
    steps = 2
    mixer_out = call(
        mix_kernel,
        sds((rows_a, columns), BF16),
        (all_heads, mix_weight),
        scratch=[pltpu.VMEM((rows_a, columns), F32)],
        grid=(steps,),
        in_specs=[
            pl.BlockSpec((tp // steps, rows_a, dv), lambda i: (i, 0, 0)),
            pl.BlockSpec((tp * dv // steps, columns), lambda i: (i, 0)),
        ],
        out_specs=pl.BlockSpec((rows_a, columns), lambda i: (0, 0)),
    )

    share = [pltpu.VMEM((tokens, slots), BF16)] * 2
    plan = call(plan_kernel, share, (routes, route_weight))
    expert_out = call(collect_kernel, sds((tokens, columns), BF16), (*plan, back), near=(0, 1, 2))
    return (mixer_out, expert_out)


def solution(mesh):
    split = Mesh(mesh.devices.reshape(16, 2, 4, 4), (*EP, *TP))
    in_specs = (
        P(EP, TP),
        P(EP, TP),
        P(EP, TP),
        P(TP, EP),
        P(TP, EP),
        P(EP, TP),
        P(TP),
        P(None, TP),
        P(EP, TP),
        P(EP, None),
        P(EP, None),
        P(EP, TP, None),
        P(EP, TP, None),
        P(EP, None, TP),
    )
    out_specs = (P(EP, TP), P(EP, TP))

    return jax.shard_map(body, mesh=split, in_specs=in_specs, out_specs=out_specs, check_vma=False)
```

```python
import jax
import jax.numpy as jnp
from jax import lax
from jax.experimental import pallas as pl
from jax.experimental.pallas import tpu as pltpu
from jax.sharding import Mesh
from jax.sharding import PartitionSpec as P


EP = ("z", "c")
TP = ("y", "x")
EPSILON = 1e-06
LOG_FLOOR = -1e30
MASKED = -1e38
HIGHEST = lax.Precision.HIGHEST
F32 = jnp.float32
BF16 = jnp.bfloat16


def dot(a, b):
    return jnp.dot(a, b, preferred_element_type=F32)


def dot_t(a, b):
    return lax.dot_general(a, b, (((1,), (1,)), ((), ())), preferred_element_type=F32)


def iota(shape, dim):
    return lax.broadcasted_iota(jnp.int32, shape, dim)


def call(kernel, out, args, scratch=(), grid=None, in_specs=None, out_specs=None, near=()):
    args = [
        pltpu.with_memory_space_constraint(a, pltpu.VMEM) if i in near else a
        for i, a in enumerate(args)
    ]
    vmem = pl.BlockSpec(memory_space=pltpu.VMEM)
    smem = pl.BlockSpec(memory_space=pltpu.SMEM)
    if in_specs is None:
        in_specs = [smem if a.dtype == jnp.int32 and a.ndim == 1 else vmem for a in args]
    kw = {} if grid is None else {"grid": grid}
    if out_specs is None:
        out_specs = jax.tree.map(lambda _: vmem, out)
    return pl.pallas_call(
        kernel,
        out_shape=out,
        in_specs=in_specs,
        out_specs=out_specs,
        scratch_shapes=list(scratch),
        compiler_params=pltpu.CompilerParams(vmem_limit_bytes=57 << 20),
        **kw,
    )(*args)


def log_sigmoid(f):
    return jnp.minimum(f, 0.0) - jnp.log1p(jnp.exp(-jnp.abs(f)))


def as_column(row, keep):
    n = row.shape[1]
    chosen = keep(iota((n, n), 1), iota((n, n), 0))
    return jnp.sum(jnp.where(chosen, jnp.broadcast_to(row, (n, n)), 0.0), axis=1, keepdims=True)


def column_of(row):
    pieces = [row[:, i : i + 128] for i in range(0, row.shape[1], 128)]
    return jnp.concatenate([as_column(p, lambda lane, at: lane == at) for p in pieces], axis=0)


def cumulative_forms(forget_row):
    logs = log_sigmoid(forget_row)
    before = jnp.zeros((1, 1), F32)
    columns, rows = [], []
    for start in range(0, forget_row.shape[1], 128):
        piece = logs[:, start : start + 128]
        n = piece.shape[1]
        column = as_column(piece, lambda lane, at: lane <= at)
        own = as_column(piece, lambda lane, at: lane == at)
        earlier = iota((n, n), 0) <= iota((n, n), 1)
        row = jnp.sum(jnp.where(earlier, own, 0.0), axis=0, keepdims=True)
        columns.append(column + before)
        rows.append(row + before)
        before = before + column[n - 1 :, :]
    return jnp.concatenate(columns, axis=0), jnp.concatenate(rows, axis=1)


def summary_kernel(k_ref, v_ref, in_ref, forget_ref, out_ref):
    n = k_ref.shape[0]
    dk = k_ref.shape[1]
    column, _ = cumulative_forms(forget_ref[...])
    log_in = column_of(in_ref[...])
    total = column[n - 1 :, :]
    weight_log = total - column + log_in
    top = jnp.max(weight_log, axis=0, keepdims=True)
    weighted = k_ref[...].astype(F32) * jnp.exp(weight_log - top)
    memory = lax.dot_general(
        weighted.astype(BF16), v_ref[...], (((0,), (0,)), ((), ())), preferred_element_type=F32
    )
    normal = jnp.sum(weighted, axis=0, keepdims=True)
    width = out_ref.shape[1]
    normal = jnp.concatenate([normal] * (width // dk), axis=1)
    pack(
        out_ref,
        memory,
        normal,
        jnp.broadcast_to(total, (1, width)),
        jnp.broadcast_to(top, (1, width)),
    )


def split3(x):
    high = x.astype(BF16)
    rest = x - high.astype(F32)
    middle = rest.astype(BF16)
    low = (rest - middle.astype(F32)).astype(BF16)
    return high, middle, low


def pack(out_ref, memory, normal, decay, top):
    dk, width = memory.shape
    out_ref[0:dk, :] = memory.astype(BF16)
    rows = []
    for value in (normal, decay, top):
        rows += [part.astype(F32) for part in split3(value)]
    rows.append(jnp.zeros((out_ref.shape[0] - dk - len(rows), width), F32))
    out_ref[dk:, :] = jnp.concatenate(rows, axis=0).astype(BF16)


def earlier_state(all_ref, here, dk):
    count, _, width = all_ref.shape
    decay = jnp.zeros((1, width), F32)
    logs, normals = [], []
    for k in reversed(range(count)):
        lines = all_ref[k, dk : dk + 16, :].astype(F32)
        normal, own_decay, top = [
            lines[i : i + 1] + lines[i + 1 : i + 2] + lines[i + 2 : i + 3] for i in (0, 3, 6)
        ]
        logs.append(jnp.where(k < here, top + decay, MASKED))
        normals.append(normal)
        decay = decay + jnp.where(k < here, own_decay, 0.0)
    top = jnp.full((1, width), LOG_FLOOR, F32)
    for log in logs:
        top = jnp.maximum(top, log)
    memory = jnp.zeros((dk, width), F32)
    normal = jnp.zeros((1, width), F32)
    for k, log, own in zip(reversed(range(count)), logs, normals):
        weight = jnp.exp(log - top)
        memory = memory + weight * all_ref[k, 0:dk, :].astype(F32)
        normal = normal + weight * own
    return memory, normal, top


def output_kernel(
    at_ref, q_ref, k_ref, v_ref, in_ref, forget_ref, gate_ref, gain_ref, all_ref, out_ref
):
    n, dk = q_ref.shape
    scale = dk ** (-0.5)
    column, row = cumulative_forms(forget_ref[...])
    memory, normal, top_before = earlier_state(all_ref, at_ref[0], dk)
    normal = normal[:, :dk]
    top_before = top_before[:, 0:1]
    log_in = in_ref[...]
    step = n // 4
    for start in range(0, n, step):
        rows, seen = slice(start, start + step), start + step
        q = q_ref[rows, :]
        at = column[rows, :]
        causal = iota((step, seen), 1) <= iota((step, seen), 0) + start
        log_decay = jnp.where(causal, at - row[:, :seen] + log_in[:, :seen], MASKED)
        log_inter = at + top_before
        top = jnp.maximum(log_inter, jnp.max(log_decay, axis=1, keepdims=True))
        scores = dot_t(q, k_ref[0:seen, :]) * scale * jnp.exp(log_decay - top)
        carried = jnp.exp(log_inter - top) * scale
        wide = q.astype(F32)
        numerator = carried * jnp.dot(
            wide, memory, precision=HIGHEST, preferred_element_type=F32
        ) + dot(scores.astype(BF16), v_ref[0:seen, :])
        denominator = carried * jnp.sum(wide * normal, axis=1, keepdims=True) + jnp.sum(
            scores, axis=1, keepdims=True
        )
        values = numerator / jnp.maximum(jnp.abs(denominator), jnp.exp(-top))
        values = values * lax.rsqrt(jnp.mean(values * values, axis=1, keepdims=True) + EPSILON)
        gate = gate_ref[rows, :].astype(F32)
        values = values * gain_ref[...] * (1.0 / (1.0 + jnp.exp(-gate)))
        out_ref[rows, :] = values.astype(BF16)


def dispatch_kernel(routes_ref, x_ref, out_ref):
    tokens = x_ref.shape[0]
    slots = out_ref.shape[0]
    experts, room = 32, slots // 32
    expert = iota((experts, tokens), 0)
    named = jnp.zeros((experts, tokens), F32)
    for r in range(routes_ref.shape[0]):
        named = named + (routes_ref[r : r + 1, :] == expert).astype(F32)
    earlier = (iota((tokens, tokens), 0) < iota((tokens, tokens), 1)).astype(F32).astype(BF16)
    place = dot(named.astype(BF16), earlier)
    key = jnp.where(named > 0.5, place, -1.0).astype(BF16)
    slot = iota((slots, experts), 0)
    spread = (slot // room == iota((slots, experts), 1)).astype(F32).astype(BF16)
    wanted = (iota((slots, tokens), 0) % room).astype(F32)
    chosen = (dot(spread, key) == wanted).astype(F32).astype(BF16)
    out_ref[...] = dot(chosen, x_ref[...]).astype(BF16)


def plan_kernel(routes_ref, weight_ref, high_ref, low_ref):
    tokens, slots = high_ref.shape
    experts, room = 32, slots // 32
    expert = iota((tokens, experts), 1)
    named = jnp.zeros((tokens, experts), F32)
    weight = jnp.zeros((tokens, experts), F32)
    for r in range(routes_ref.shape[1]):
        hit = routes_ref[:, r : r + 1] == expert
        named = named + hit.astype(F32)
        weight = weight + jnp.where(hit, weight_ref[:, r : r + 1], 0.0)
    earlier = (iota((tokens, tokens), 1) < iota((tokens, tokens), 0)).astype(F32).astype(BF16)
    place = dot(earlier, named.astype(BF16))
    key = jnp.where(named > 0.5, place, -1.0).astype(BF16)
    slot = iota((experts, slots), 1)
    spread = (slot // room == iota((experts, slots), 0)).astype(F32).astype(BF16)
    wanted = (iota((tokens, slots), 1) % room).astype(F32)
    chosen = dot(key, spread) == wanted
    high, low, _ = split3(weight)
    high_ref[...] = jnp.where(chosen, dot(high, spread), 0.0).astype(BF16)
    low_ref[...] = jnp.where(chosen, dot(low, spread), 0.0).astype(BF16)


def collect_kernel(high_ref, low_ref, back_ref, out_ref):
    back = back_ref[...]
    out_ref[...] = (dot(high_ref[...], back) + dot(low_ref[...], back)).astype(BF16)


def hidden_kernel(
    x_ref, g0_ref, g1_ref, g2_ref, g3_ref, u0_ref, u1_ref, u2_ref, u3_ref,
    out_ref, gate_acc, up_acc, squares,
):
    step = pl.program_id(0)
    _, _, columns = x_ref.shape
    senders = g0_ref.shape[1] // columns
    order = [step * senders + i for i in range(senders)]
    pieces = [x_ref[lax.rem(t, 4) * 4 + t // 4] for t in order]
    x = jnp.concatenate(pieces, axis=1)
    gate = jnp.concatenate([w[...] for w in (g0_ref, g1_ref, g2_ref, g3_ref)], axis=0)
    up = jnp.concatenate([w[...] for w in (u0_ref, u1_ref, u2_ref, u3_ref)], axis=0)
    gate_part, up_part = dot_t(x, gate), dot_t(x, up)
    square = jnp.zeros(squares.shape, F32)
    for piece in pieces:
        wide = piece.astype(F32)
        square = square + wide * wide

    @pl.when(step == 0)
    def _():
        gate_acc[...] = gate_part
        up_acc[...] = up_part
        squares[...] = square

    @pl.when(step > 0)
    def _():
        gate_acc[...] += gate_part
        up_acc[...] += up_part
        squares[...] += square

    @pl.when(step == pl.num_programs(0) - 1)
    def _():
        total = jnp.sum(squares[...], axis=1, keepdims=True)
        inverse = lax.rsqrt(total * (1.0 / (columns * x_ref.shape[0])) + EPSILON)
        gate = gate_acc[...] * inverse
        hidden = gate * (1.0 / (1.0 + jnp.exp(-gate))) * (up_acc[...] * inverse)
        hidden = hidden.astype(BF16)
        for copy in range(out_ref.shape[0]):
            out_ref[copy] = hidden


def down_kernel(at_ref, h_ref, w0_ref, w1_ref, w2_ref, w3_ref, out_ref):
    part = h_ref.shape[2] // 4
    y = at_ref[1]
    hidden = jnp.concatenate([h_ref[xs] for xs in range(4)], axis=1)
    for k, w_ref in enumerate((w0_ref, w1_ref, w2_ref, w3_ref)):
        weight = []
        for xs in range(4):
            for j in range(4):
                start = (lax.rem(y + j, 4) * 4 + xs) * part
                weight.append(w_ref[pl.ds(pl.multiple_of(start, part), part), :])
        out_ref[lax.rem(y + k, 4)] = dot(hidden, jnp.concatenate(weight, axis=0)).astype(BF16)


def mix_kernel(h_ref, w_ref, out_ref, acc):
    step = pl.program_id(0)
    width = h_ref.shape[2]
    total = jnp.zeros(acc.shape, F32)
    for i in range(h_ref.shape[0]):
        total = total + dot(h_ref[i], w_ref[i * width : (i + 1) * width, :])

    @pl.when(step == 0)
    def _():
        acc[...] = total

    @pl.when(step > 0)
    def _():
        acc[...] += total

    @pl.when(step == pl.num_programs(0) - 1)
    def _():
        out_ref[...] = acc[...].astype(BF16)


def from_next(x, axis, k):
    n = lax.axis_size(axis)
    return lax.ppermute(x, axis, [((i + k) % n, i) for i in range(n)])


def exchange(x, axis):
    return lax.all_to_all(x, axis, split_axis=0, concat_axis=0, tiled=True)


def body(
    query_rows,
    key_rows,
    value_rows,
    in_gate,
    forget_gate,
    out_gate,
    head_gain,
    mix_weight,
    expert_input,
    routes,
    route_weight,
    gate_weight,
    up_weight,
    down_weight,
):
    sds = jax.ShapeDtypeStruct
    rows_a, dk = query_rows.shape
    dv = value_rows.shape[1]
    tokens, columns = expert_input.shape
    ep, tp = lax.axis_size(EP), lax.axis_size(TP)
    gate_local, up_local, down_local = gate_weight[0], up_weight[0], down_weight[0]
    width = gate_local.shape[0]
    slots = ep * 32
    at = jnp.stack([lax.axis_index(EP), lax.axis_index("y")]).astype(jnp.int32)

    mine = call(
        summary_kernel, sds((dk + 16, dv), BF16), (key_rows, value_rows, in_gate, forget_gate)
    )
    states = lax.all_gather(mine, EP, axis=0)
    table = call(dispatch_kernel, pltpu.VMEM((slots, columns), BF16), (routes.T, expert_input))
    arrived = exchange(table.reshape(4 * ep, 8, columns), (*EP, "y"))
    arrived = arrived.reshape(ep, 4, 8, columns).transpose(1, 0, 2, 3)

    gate_1 = from_next(gate_local, "y", 1)
    up_3 = from_next(up_local, "y", 3)
    gate_3 = from_next(gate_local, "y", 3)
    up_1 = from_next(up_local, "y", 1)
    gate_2 = from_next(gate_1, "y", 1)
    up_2 = from_next(up_3, "y", 3)
    down_far = []
    for k in (1, 3, 2):
        down_far.append(from_next(down_local, "y", k))
    down_1, down_3, down_2 = down_far

    heads = call(
        output_kernel,
        sds((rows_a, dv), BF16),
        (
            at, query_rows, key_rows, value_rows, in_gate, forget_gate, out_gate,
            head_gain[None, :], states,
        ),
    )

    sent = jnp.broadcast_to(arrived.reshape(1, slots, columns), (4, slots, columns))
    rows = exchange(sent, "x").reshape(tp, slots // 4, columns)
    grid = 2
    per = tp // grid
    weights_spec = lambda r: pl.BlockSpec((r, per * columns), lambda i: (0, i))
    hidden = call(
        hidden_kernel,
        sds((4, slots // 4, 4 * width), BF16),
        (rows, gate_local, gate_1, gate_2, gate_3, up_local, up_1, up_2, up_3),
        scratch=[pltpu.VMEM((slots // 4, 4 * width), F32)] * 2
        + [pltpu.VMEM((slots // 4, columns), F32)],
        grid=(grid,),
        in_specs=[
            pl.BlockSpec(memory_space=pltpu.VMEM),
        ]
        + [weights_spec(width)] * 8,
        out_specs=pl.BlockSpec(memory_space=pltpu.VMEM),
        near=(0,),
    )
    gathered = exchange(hidden, "x")
    results = call(
        down_kernel,
        pltpu.VMEM((4, slots // 4, columns), BF16),
        (at, gathered, down_local, down_1, down_2, down_3),
        near=(1,),
    )
    results = results.reshape(4, ep, 8, columns).transpose(1, 0, 2, 3)
    back = exchange(results.reshape(4 * ep, 8, columns), (*EP, "y")).reshape(slots, columns)

    all_heads = lax.all_gather(heads, TP, axis=0)
    steps = 2
    mixer_out = call(
        mix_kernel,
        sds((rows_a, columns), BF16),
        (all_heads, mix_weight),
        scratch=[pltpu.VMEM((rows_a, columns), F32)],
        grid=(steps,),
        in_specs=[
            pl.BlockSpec((tp // steps, rows_a, dv), lambda i: (i, 0, 0)),
            pl.BlockSpec((tp * dv // steps, columns), lambda i: (i, 0)),
        ],
        out_specs=pl.BlockSpec((rows_a, columns), lambda i: (0, 0)),
    )

    share = [pltpu.VMEM((tokens, slots), BF16)] * 2
    plan = call(plan_kernel, share, (routes, route_weight))
    expert_out = call(collect_kernel, sds((tokens, columns), BF16), (*plan, back), near=(0, 1, 2))
    return (mixer_out, expert_out)


def solution(mesh):
    split = Mesh(mesh.devices.reshape(16, 2, 4, 4), (*EP, *TP))
    in_specs = (
        P(EP, TP),
        P(EP, TP),
        P(EP, TP),
        P(TP, EP),
        P(TP, EP),
        P(EP, TP),
        P(TP),
        P(None, TP),
        P(EP, TP),
        P(EP, None),
        P(EP, None),
        P(EP, TP, None),
        P(EP, TP, None),
        P(EP, None, TP),
    )
    out_specs = (P(EP, TP), P(EP, TP))

    return jax.shard_map(body, mesh=split, in_specs=in_specs, out_specs=out_specs, check_vma=False)
```

```python
import jax
import jax.numpy as jnp
from jax import lax
from jax.experimental import pallas as pl
from jax.experimental.pallas import tpu as pltpu
from jax.sharding import Mesh
from jax.sharding import PartitionSpec as P


EP = ("z", "c")
TP = ("y", "x")
EPSILON = 1e-06
LOG_FLOOR = -1e30
MASKED = -1e38
HIGHEST = lax.Precision.HIGHEST
F32 = jnp.float32
BF16 = jnp.bfloat16


def dot(a, b):
    return jnp.dot(a, b, preferred_element_type=F32)


def dot_t(a, b):
    return lax.dot_general(a, b, (((1,), (1,)), ((), ())), preferred_element_type=F32)


def iota(shape, dim):
    return lax.broadcasted_iota(jnp.int32, shape, dim)


def call(kernel, out, args, scratch=(), grid=None, in_specs=None, out_specs=None, near=()):
    args = [
        pltpu.with_memory_space_constraint(a, pltpu.VMEM) if i in near else a
        for i, a in enumerate(args)
    ]
    vmem = pl.BlockSpec(memory_space=pltpu.VMEM)
    smem = pl.BlockSpec(memory_space=pltpu.SMEM)
    if in_specs is None:
        in_specs = [smem if a.dtype == jnp.int32 and a.ndim == 1 else vmem for a in args]
    kw = {} if grid is None else {"grid": grid}
    if out_specs is None:
        out_specs = jax.tree.map(lambda _: vmem, out)
    return pl.pallas_call(
        kernel,
        out_shape=out,
        in_specs=in_specs,
        out_specs=out_specs,
        scratch_shapes=list(scratch),
        compiler_params=pltpu.CompilerParams(vmem_limit_bytes=57 << 20),
        **kw,
    )(*args)


def log_sigmoid(f):
    return jnp.minimum(f, 0.0) - jnp.log1p(jnp.exp(-jnp.abs(f)))


def cumulative_forms(forget_row):
    n = forget_row.shape[1]
    logs = jnp.broadcast_to(log_sigmoid(forget_row), (n, n))
    at_row, at_col = iota((n, n), 0), iota((n, n), 1)
    column = jnp.sum(jnp.where(at_col <= at_row, logs, 0.0), axis=1, keepdims=True)
    own = jnp.sum(jnp.where(at_col == at_row, logs, 0.0), axis=1, keepdims=True)
    row = jnp.sum(jnp.where(at_row <= at_col, own, 0.0), axis=0, keepdims=True)
    return column, row


def summary_kernel(k_ref, v_ref, in_ref, forget_ref, out_ref):
    n = k_ref.shape[0]
    dk = k_ref.shape[1]
    column, _ = cumulative_forms(forget_ref[...])
    diagonal = iota((n, n), 0) == iota((n, n), 1)
    log_in = jnp.sum(
        jnp.where(diagonal, jnp.broadcast_to(in_ref[...], (n, n)), 0.0), axis=1, keepdims=True
    )
    total = column[n - 1 :, :]
    weight_log = total - column + log_in
    top = jnp.max(weight_log, axis=0, keepdims=True)
    weighted = k_ref[...].astype(F32) * jnp.exp(weight_log - top)
    memory = lax.dot_general(
        weighted.astype(BF16), v_ref[...], (((0,), (0,)), ((), ())), preferred_element_type=F32
    )
    normal = jnp.sum(weighted, axis=0, keepdims=True)
    width = out_ref.shape[1]
    out_ref[0:dk, :] = memory
    rows = [
        jnp.concatenate([normal] * (width // dk), axis=1),
        jnp.broadcast_to(total, (1, width)),
        jnp.broadcast_to(top, (1, width)),
        jnp.zeros((out_ref.shape[0] - dk - 3, width), F32),
    ]
    out_ref[dk:, :] = jnp.concatenate(rows, axis=0)


def fold(first, second):
    memory_1, normal_1, decay_1, max_1 = first
    memory_2, normal_2, decay_2, max_2 = second
    top = jnp.maximum(decay_2 + max_1, max_2)
    keep_1 = jnp.exp(decay_2 + max_1 - top)
    keep_2 = jnp.exp(max_2 - top)
    return (
        keep_1 * memory_1 + keep_2 * memory_2,
        keep_1 * normal_1 + keep_2 * normal_2,
        decay_1 + decay_2,
        top,
    )


def split3(x):
    high = x.astype(BF16)
    rest = x - high.astype(F32)
    middle = rest.astype(BF16)
    low = (rest - middle.astype(F32)).astype(BF16)
    return high, middle, low


def unpack(item, dk):
    return (item[0:dk], item[dk : dk + 1], item[dk + 1 : dk + 2], item[dk + 2 : dk + 3])


def first_state(dk, width):
    return (
        jnp.zeros((dk, width), F32),
        jnp.zeros((1, width), F32),
        jnp.zeros((1, width), F32),
        jnp.full((1, width), LOG_FLOOR, F32),
    )


def output_kernel(
    at_ref, q_ref, k_ref, v_ref, in_ref, forget_ref, gate_ref, gain_ref, all_ref, out_ref
):
    n, dk = q_ref.shape
    scale = dk ** (-0.5)
    column, row = cumulative_forms(forget_ref[...])
    memory, normal, _, top_before = lax.fori_loop(
        0,
        at_ref[0],
        lambda k, state: fold(state, unpack(all_ref[k], dk)),
        first_state(dk, all_ref.shape[2]),
    )
    normal = normal[:, :dk]
    top_before = top_before[:, 0:1]
    log_in = in_ref[...]
    step = n // 4
    for start in range(0, n, step):
        rows, seen = slice(start, start + step), start + step
        q = q_ref[rows, :]
        at = column[rows, :]
        causal = iota((step, seen), 1) <= iota((step, seen), 0) + start
        log_decay = jnp.where(causal, at - row[:, :seen] + log_in[:, :seen], MASKED)
        log_inter = at + top_before
        top = jnp.maximum(log_inter, jnp.max(log_decay, axis=1, keepdims=True))
        scores = dot_t(q, k_ref[0:seen, :]) * scale * jnp.exp(log_decay - top)
        carried = jnp.exp(log_inter - top) * scale
        wide = q.astype(F32)
        numerator = carried * jnp.dot(
            wide, memory, precision=HIGHEST, preferred_element_type=F32
        ) + dot(scores.astype(BF16), v_ref[0:seen, :])
        denominator = carried * jnp.sum(wide * normal, axis=1, keepdims=True) + jnp.sum(
            scores, axis=1, keepdims=True
        )
        values = numerator / jnp.maximum(jnp.abs(denominator), jnp.exp(-top))
        values = values * lax.rsqrt(jnp.mean(values * values, axis=1, keepdims=True) + EPSILON)
        gate = gate_ref[rows, :].astype(F32)
        values = values * gain_ref[...] * (1.0 / (1.0 + jnp.exp(-gate)))
        out_ref[rows, :] = values.astype(BF16)


def dispatch_kernel(routes_ref, x_ref, out_ref):
    tokens = x_ref.shape[0]
    slots = out_ref.shape[0]
    experts, room = 32, slots // 32
    expert = iota((experts, tokens), 0)
    named = jnp.zeros((experts, tokens), F32)
    for r in range(routes_ref.shape[0]):
        named = named + (routes_ref[r : r + 1, :] == expert).astype(F32)
    earlier = (iota((tokens, tokens), 0) < iota((tokens, tokens), 1)).astype(F32).astype(BF16)
    place = dot(named.astype(BF16), earlier)
    key = jnp.where(named > 0.5, place, -1.0).astype(BF16)
    slot = iota((slots, experts), 0)
    spread = (slot // room == iota((slots, experts), 1)).astype(F32).astype(BF16)
    wanted = (iota((slots, tokens), 0) % room).astype(F32)
    chosen = (dot(spread, key) == wanted).astype(F32).astype(BF16)
    out_ref[...] = dot(chosen, x_ref[...]).astype(BF16)


def plan_kernel(routes_ref, weight_ref, high_ref, low_ref):
    tokens, slots = high_ref.shape
    experts, room = 32, slots // 32
    expert = iota((tokens, experts), 1)
    named = jnp.zeros((tokens, experts), F32)
    weight = jnp.zeros((tokens, experts), F32)
    for r in range(routes_ref.shape[1]):
        hit = routes_ref[:, r : r + 1] == expert
        named = named + hit.astype(F32)
        weight = weight + jnp.where(hit, weight_ref[:, r : r + 1], 0.0)
    earlier = (iota((tokens, tokens), 1) < iota((tokens, tokens), 0)).astype(F32).astype(BF16)
    place = dot(earlier, named.astype(BF16))
    key = jnp.where(named > 0.5, place, -1.0).astype(BF16)
    slot = iota((experts, slots), 1)
    spread = (slot // room == iota((experts, slots), 0)).astype(F32).astype(BF16)
    wanted = (iota((tokens, slots), 1) % room).astype(F32)
    chosen = dot(key, spread) == wanted
    high, low, _ = split3(weight)
    high_ref[...] = jnp.where(chosen, dot(high, spread), 0.0).astype(BF16)
    low_ref[...] = jnp.where(chosen, dot(low, spread), 0.0).astype(BF16)


def collect_kernel(high_ref, low_ref, back_ref, out_ref):
    back = back_ref[...]
    out_ref[...] = (dot(high_ref[...], back) + dot(low_ref[...], back)).astype(BF16)


def hidden_kernel(
    x_ref, g0_ref, g1_ref, g2_ref, g3_ref, u0_ref, u1_ref, u2_ref, u3_ref,
    out_ref, gate_acc, up_acc, squares,
):
    step = pl.program_id(0)
    _, _, columns = x_ref.shape
    senders = g0_ref.shape[1] // columns
    order = [step * senders + i for i in range(senders)]
    pieces = [x_ref[lax.rem(t, 4) * 4 + t // 4] for t in order]
    x = jnp.concatenate(pieces, axis=1)
    gate = jnp.concatenate([w[...] for w in (g0_ref, g1_ref, g2_ref, g3_ref)], axis=0)
    up = jnp.concatenate([w[...] for w in (u0_ref, u1_ref, u2_ref, u3_ref)], axis=0)
    gate_part, up_part = dot_t(x, gate), dot_t(x, up)
    square = jnp.zeros(squares.shape, F32)
    for piece in pieces:
        wide = piece.astype(F32)
        square = square + wide * wide

    @pl.when(step == 0)
    def _():
        gate_acc[...] = gate_part
        up_acc[...] = up_part
        squares[...] = square

    @pl.when(step > 0)
    def _():
        gate_acc[...] += gate_part
        up_acc[...] += up_part
        squares[...] += square

    @pl.when(step == pl.num_programs(0) - 1)
    def _():
        total = jnp.sum(squares[...], axis=1, keepdims=True)
        inverse = lax.rsqrt(total * (1.0 / (columns * x_ref.shape[0])) + EPSILON)
        gate = gate_acc[...] * inverse
        hidden = gate * (1.0 / (1.0 + jnp.exp(-gate))) * (up_acc[...] * inverse)
        hidden = hidden.astype(BF16)
        for copy in range(out_ref.shape[0]):
            out_ref[copy] = hidden


def down_kernel(at_ref, h_ref, w0_ref, w1_ref, w2_ref, w3_ref, out_ref):
    part = h_ref.shape[2] // 4
    y = at_ref[1]
    hidden = jnp.concatenate([h_ref[xs] for xs in range(4)], axis=1)
    for k, w_ref in enumerate((w0_ref, w1_ref, w2_ref, w3_ref)):
        weight = []
        for xs in range(4):
            for j in range(4):
                start = (lax.rem(y + j, 4) * 4 + xs) * part
                weight.append(w_ref[pl.ds(pl.multiple_of(start, part), part), :])
        out_ref[lax.rem(y + k, 4)] = dot(hidden, jnp.concatenate(weight, axis=0)).astype(BF16)


def mix_kernel(h_ref, w_ref, out_ref, acc):
    step = pl.program_id(0)
    width = h_ref.shape[2]
    total = jnp.zeros(acc.shape, F32)
    for i in range(h_ref.shape[0]):
        total = total + dot(h_ref[i], w_ref[i * width : (i + 1) * width, :])

    @pl.when(step == 0)
    def _():
        acc[...] = total

    @pl.when(step > 0)
    def _():
        acc[...] += total

    @pl.when(step == pl.num_programs(0) - 1)
    def _():
        out_ref[...] = acc[...].astype(BF16)


def from_next(x, axis, k):
    n = lax.axis_size(axis)
    return lax.ppermute(x, axis, [((i + k) % n, i) for i in range(n)])


def exchange(x, axis):
    return lax.all_to_all(x, axis, split_axis=0, concat_axis=0, tiled=True)


def body(
    query_rows,
    key_rows,
    value_rows,
    in_gate,
    forget_gate,
    out_gate,
    head_gain,
    mix_weight,
    expert_input,
    routes,
    route_weight,
    gate_weight,
    up_weight,
    down_weight,
):
    sds = jax.ShapeDtypeStruct
    rows_a, dk = query_rows.shape
    dv = value_rows.shape[1]
    tokens, columns = expert_input.shape
    ep, tp = lax.axis_size(EP), lax.axis_size(TP)
    gate_local, up_local, down_local = gate_weight[0], up_weight[0], down_weight[0]
    width = gate_local.shape[0]
    slots = ep * 32
    at = jnp.stack([lax.axis_index(EP), lax.axis_index("y")]).astype(jnp.int32)

    mine = call(
        summary_kernel, sds((dk + 8, dv), F32), (key_rows, value_rows, in_gate, forget_gate)
    )
    states = lax.all_gather(mine, EP, axis=0)
    table = call(dispatch_kernel, pltpu.VMEM((slots, columns), BF16), (routes.T, expert_input))
    arrived = exchange(table.reshape(4 * ep, 8, columns), (*EP, "y"))
    arrived = arrived.reshape(ep, 4, 8, columns).transpose(1, 0, 2, 3)

    gate_1 = from_next(gate_local, "y", 1)
    up_3 = from_next(up_local, "y", 3)
    gate_3 = from_next(gate_local, "y", 3)
    up_1 = from_next(up_local, "y", 1)
    gate_2 = from_next(gate_1, "y", 1)
    up_2 = from_next(up_3, "y", 3)
    down_far = []
    for k in (1, 3, 2):
        down_far.append(from_next(down_local, "y", k))
    down_1, down_3, down_2 = down_far

    heads = call(
        output_kernel,
        sds((rows_a, dv), BF16),
        (
            at, query_rows, key_rows, value_rows, in_gate, forget_gate, out_gate,
            head_gain[None, :], states,
        ),
    )

    sent = jnp.broadcast_to(arrived.reshape(1, slots, columns), (4, slots, columns))
    rows = exchange(sent, "x").reshape(tp, slots // 4, columns)
    grid = 2
    per = tp // grid
    weights_spec = lambda r: pl.BlockSpec((r, per * columns), lambda i: (0, i))
    hidden = call(
        hidden_kernel,
        sds((4, slots // 4, 4 * width), BF16),
        (rows, gate_local, gate_1, gate_2, gate_3, up_local, up_1, up_2, up_3),
        scratch=[pltpu.VMEM((slots // 4, 4 * width), F32)] * 2
        + [pltpu.VMEM((slots // 4, columns), F32)],
        grid=(grid,),
        in_specs=[
            pl.BlockSpec(memory_space=pltpu.VMEM),
        ]
        + [weights_spec(width)] * 8,
        out_specs=pl.BlockSpec(memory_space=pltpu.VMEM),
        near=(0,),
    )
    gathered = exchange(hidden, "x")
    results = call(
        down_kernel,
        pltpu.VMEM((4, slots // 4, columns), BF16),
        (at, gathered, down_local, down_1, down_2, down_3),
        near=(1,),
    )
    results = results.reshape(4, ep, 8, columns).transpose(1, 0, 2, 3)
    back = exchange(results.reshape(4 * ep, 8, columns), (*EP, "y")).reshape(slots, columns)

    all_heads = lax.all_gather(heads, TP, axis=0)
    steps = 2
    mixer_out = call(
        mix_kernel,
        sds((rows_a, columns), BF16),
        (all_heads, mix_weight),
        scratch=[pltpu.VMEM((rows_a, columns), F32)],
        grid=(steps,),
        in_specs=[
            pl.BlockSpec((tp // steps, rows_a, dv), lambda i: (i, 0, 0)),
            pl.BlockSpec((tp * dv // steps, columns), lambda i: (i, 0)),
        ],
        out_specs=pl.BlockSpec((rows_a, columns), lambda i: (0, 0)),
    )

    share = [pltpu.VMEM((tokens, slots), BF16)] * 2
    plan = call(plan_kernel, share, (routes, route_weight))
    expert_out = call(collect_kernel, sds((tokens, columns), BF16), (*plan, back), near=(0, 1, 2))
    return (mixer_out, expert_out)


def solution(mesh):
    split = Mesh(mesh.devices.reshape(16, 2, 4, 4), (*EP, *TP))
    in_specs = (
        P(EP, TP),
        P(EP, TP),
        P(EP, TP),
        P(TP, EP),
        P(TP, EP),
        P(EP, TP),
        P(TP),
        P(None, TP),
        P(EP, TP),
        P(EP, None),
        P(EP, None),
        P(EP, TP, None),
        P(EP, TP, None),
        P(EP, None, TP),
    )
    out_specs = (P(EP, TP), P(EP, TP))

    return jax.shard_map(body, mesh=split, in_specs=in_specs, out_specs=out_specs, check_vma=False)
```
